256 devices in a mesh: sp: 32 (over z, y), tp: 8 (over x, core).
Axes of the slice: x: 4, y: 4, z: 8, core: 2. Of those that a mesh axis runs over, the one named last changes fastest.
Arguments:
- latent: bfloat16 [8192, 2048], P(('sp', 'tp')), may hold values from -6 to 6
- log_decay: float32 [8192, 8], P('sp', 'tp'), may hold values from -2 to 0
- context: bfloat16 [512, 2048], P('sp'), may hold values from -6 to 6
- condition: bfloat16 [2, 2048], replicated, may hold values from -6 to 6
- w_modulate: bfloat16 [2048, 6144], P('sp', 'tp'), may hold values from -1 to 1
- norm_gain: bfloat16 [2048], replicated, may hold values from 0.099609375 to 1.8984375
- w_query: bfloat16 [2048, 2048], P(None, 'tp'), may hold values from -0.125 to 0.125
- w_key: bfloat16 [2048, 2048], P(None, 'tp'), may hold values from -0.125 to 0.125
- w_value: bfloat16 [2048, 4096], P(None, 'tp'), may hold values from -0.125 to 0.125
- w_gate: bfloat16 [2048, 4096], P(None, 'tp'), may hold values from -0.125 to 0.125
- group_gain: bfloat16 [4096], P('tp'), may hold values from 0.099609375 to 1.8984375
- w_output: bfloat16 [4096, 2048], P('tp'), may hold values from -0.125 to 0.125
Outputs:
- updated: bfloat16 [8192, 2048], P(('sp', 'tp'))
The draws below stay inside these ranges and needn't reach their ends.
All inputs are finite; a program needn't handle non-finite values.
Results may differ from the reference program's by a relative error of at most 0.014.
Values may be sent and summed in bfloat16 or wider, within the bound.
No kernel may reach another device: no remote copies, remote signals or barrier semaphores. Data moves between devices by JAX's collectives and lax.ppermute only.
A program may use at most 128 MiB of HBM per device.

```python
import math
import jax
import jax.numpy as jnp
from jax import lax

D = 2048
RETENTION_HEADS = 8
DK = 256
DV = 512
BLOCK = 128
GRID_W = 64
LATENT_TOKENS = 8192
CTX = 512
CTX_LIFT = 4
N_TP = 8


def draw_log_decay(key, part):
    random_keys = jax.random.split(key, 7)
    fast_count = max(1, RETENTION_HEADS // 4)
    head_order = jax.random.permutation(random_keys[0], RETENTION_HEADS)
    quick_decay_heads = head_order < fast_count
    slow_rate = jax.random.uniform(random_keys[1], (RETENTION_HEADS,), jnp.float32, 0.1, 0.4) * math.log(10.0) / LATENT_TOKENS
    fast_rate = jax.random.uniform(random_keys[2], (RETENTION_HEADS,), jnp.float32, 4.0, 8.0) / BLOCK
    base_rate = jnp.where(quick_decay_heads, fast_rate, slow_rate)
    block_count = LATENT_TOKENS // BLOCK
    block_factor = jnp.exp(jax.random.uniform(random_keys[3], (block_count, 1, RETENTION_HEADS), jnp.float32, math.log(0.4), math.log(1.6)))
    jitter = jax.random.uniform(random_keys[4], (block_count, BLOCK, RETENTION_HEADS), jnp.float32, 0.5, 1.5)
    decay_rates = (base_rate * block_factor * jitter).reshape(LATENT_TOKENS, RETENTION_HEADS)
    spike_positions = jax.random.randint(random_keys[5], (2,), 0, LATENT_TOKENS)
    spike_lengths = jax.random.uniform(random_keys[6], (2, RETENTION_HEADS), jnp.float32, 0.22, 0.51)
    spike_flags = (jnp.arange(LATENT_TOKENS)[:, None] == spike_positions[None, :]).astype(jnp.float32)
    spike_runs = jnp.dot(spike_flags, spike_lengths) * jnp.where(quick_decay_heads, 0.0, 1.0)
    return (-(decay_rates + spike_runs)).astype(jnp.float32)


def draw_latent(key, part):
    random_keys = jax.random.split(key, 1)
    drawn = jnp.clip(jax.random.normal(random_keys[0], (LATENT_TOKENS, D), jnp.float32), -6.0, 6.0)
    return drawn.astype(jnp.bfloat16)


def draw_w_modulate(key, part):
    column_scale = jnp.concatenate([jnp.full((D,), 0.12, jnp.float32), jnp.ones((2 * D,), jnp.float32)]) * math.sqrt(2.0 / D)
    base_values = jax.random.normal(key, (D, 3 * D), jnp.float32)
    return jnp.clip(base_values * column_scale[None, :], -1.0, 1.0).astype(jnp.bfloat16)


def level_of(rng, shape, pieces, least, top_value):
    factor_of = 1.0
    for axis_at, blocks in pieces:
        draws = jax.random.uniform(jax.random.fold_in(jax.random.fold_in(rng, 6), axis_at), (blocks,), jnp.float32, least / len(pieces), top_value / len(pieces))
        factor_of = factor_of * jnp.repeat(jnp.exp(draws), shape[axis_at] // blocks).reshape((-1,) + (1,) * (len(shape) - 1 - axis_at))
    return factor_of


def bell_draw(stream_key, shape, spread, reach, cuts=(), kind=jnp.bfloat16):
    result = spread * jax.random.normal(stream_key, shape, jnp.float32)
    if cuts:
        result = result * level_of(stream_key, shape, cuts, -0.22, 0.18)
    return jnp.clip(result, -reach, reach).astype(kind)


def setup_inputs(seed: int = 0) -> dict:
    splits = jax.random.split(jax.random.key(seed), 13)
    latent = draw_latent(jax.random.fold_in(splits[12], 71), 0)
    log_decay = draw_log_decay(jax.random.fold_in(splits[12], 71), 0)
    context = bell_draw(splits[2], (CTX, D), 1.0, 6.0, ((0, 32),))
    condition = bell_draw(splits[3], (2, D), 1.0, 6.0)
    w_modulate = draw_w_modulate(jax.random.fold_in(splits[12], 71), 0)
    norm_gain = jnp.clip(1.0 + 0.18 * jax.random.normal(splits[5], (D,), jnp.float32), 0.099609375, 1.8984375).astype(jnp.bfloat16)
    w_query = bell_draw(splits[6], (D, D), D ** -0.5, 0.125, ((1, 8),))
    w_key = bell_draw(splits[7], (D, D), D ** -0.5, 0.125, ((1, 8),))
    w_value = bell_draw(splits[8], (D, 2 * D), D ** -0.5, 0.125, ((1, 8),))
    w_gate = bell_draw(splits[9], (D, 2 * D), D ** -0.5, 0.125, ((1, 8),))
    group_gain = jnp.clip(1.0 + 0.18 * jax.random.normal(splits[10], (2 * D,), jnp.float32), 0.099609375, 1.8984375).astype(jnp.bfloat16)
    w_output = bell_draw(splits[11], (2 * D, D), D ** -0.5, 0.125, ((0, 8),))
    return dict(latent=latent, log_decay=log_decay, context=context, condition=condition, w_modulate=w_modulate, norm_gain=norm_gain, w_query=w_query, w_key=w_key, w_value=w_value, w_gate=w_gate, group_gain=group_gain, w_output=w_output)


epsilon = 1e-06
rotary_base = 10000.0

def modulate_rows(row_block, norm_gain, shift_vec, scale_vec):
    wide = row_block.astype(jnp.float32)
    normal = wide * lax.rsqrt(lax.optimization_barrier(jnp.mean(wide * wide, axis=-1, keepdims=True)) + epsilon)
    return (normal * norm_gain.astype(jnp.float32) * (1.0 + scale_vec) + shift_vec).astype(jnp.bfloat16)

def rotate(projected, positions):
    pairs = DK // 4
    inverse = rotary_base ** (-jnp.arange(pairs, dtype=jnp.float32) / pairs)
    grid_row = (positions // GRID_W).astype(jnp.float32)
    grid_column = (positions % GRID_W).astype(jnp.float32)
    angles = jnp.concatenate([grid_row[:, None] * inverse, grid_column[:, None] * inverse], axis=-1)
    cosine = jnp.cos(angles)[:, None, :]
    sine_part = jnp.sin(angles)[:, None, :]
    paired = projected.reshape(projected.shape[0], -1, DK // 2, 2)
    even_part = paired[..., 0]
    odd_part = paired[..., 1]
    turned = jnp.stack([even_part * cosine - odd_part * sine_part, even_part * sine_part + odd_part * cosine], axis=-1)
    return turned.reshape(projected.shape)

def narrowed(values):
    return lax.optimization_barrier(values.astype(jnp.bfloat16)).astype(jnp.float32)

def sweep_blocks(queries, key_rows, value_rows, decays, entry):
    block_count = queries.shape[0] // BLOCK
    head_count = queries.shape[1]

    def advance(states, element):
        query_block, key_block, value_block, decay_block = element
        cumulative = jnp.cumsum(decay_block, axis=0)
        by_head = cumulative.T
        within = jnp.arange(BLOCK, dtype=jnp.int32)
        lower_mask = within[:, None] >= within[None, :]
        log_gaps = by_head[:, :, None] - by_head[:, None, :]
        weights = jnp.where(lower_mask, jnp.exp(jnp.where(lower_mask, log_gaps, 0.0)), 0.0)
        query_wide = query_block.astype(jnp.float32)
        value_wide = value_block.astype(jnp.float32)
        scores = jnp.einsum('ihd,jhd->hij', query_wide, key_block.astype(jnp.float32))
        weighted = narrowed(scores * weights)
        inside = jnp.einsum('hij,jhv->ihv', weighted, value_wide)
        carried_in = jnp.exp(cumulative)[:, :, None] * jnp.einsum('ihd,hdv->ihv', query_wide, narrowed(states))
        totals = cumulative[-1]
        decayed = narrowed(key_block.astype(jnp.float32) * jnp.exp(totals[None, :] - cumulative)[:, :, None])
        updates = jnp.einsum('jhd,jhv->hdv', decayed, value_wide)
        return (jnp.exp(totals)[:, None, None] * states + updates, inside + carried_in)
    blocks = (queries.reshape(block_count, BLOCK, head_count, DK), key_rows.reshape(block_count, BLOCK, head_count, DK), value_rows.reshape(block_count, BLOCK, head_count, DV), decays.reshape(block_count, BLOCK, head_count))
    unused, outputs = lax.scan(advance, entry, blocks)
    return outputs.reshape(queries.shape[0], head_count, DV)

def reference(latent, log_decay, context, condition, w_modulate, norm_gain, w_query, w_key, w_value, w_gate, group_gain, w_output):
    activated = jax.nn.silu(condition.astype(jnp.float32)).astype(jnp.bfloat16)
    modulation = jnp.dot(activated, w_modulate, preferred_element_type=jnp.float32)
    normed = modulate_rows(latent, norm_gain, modulation[0, :D], modulation[0, D:2 * D])
    context_normed = modulate_rows(context, norm_gain, modulation[1, :D], modulation[1, D:2 * D])
    positions = jnp.arange(LATENT_TOKENS, dtype=jnp.int32)
    query_rows = rotate(jnp.dot(normed, w_query, preferred_element_type=jnp.float32), positions).astype(jnp.bfloat16)
    key_rows = (rotate(jnp.dot(normed, w_key, preferred_element_type=jnp.float32), positions) * DK ** (-0.5)).astype(jnp.bfloat16)
    value_rows = jnp.dot(normed, w_value, preferred_element_type=jnp.float32).astype(jnp.bfloat16)
    gate_rows = jnp.dot(normed, w_gate, preferred_element_type=jnp.float32).astype(jnp.bfloat16)
    context_keys = (jnp.dot(context_normed, w_key, preferred_element_type=jnp.float32) * DK ** (-0.5)).astype(jnp.bfloat16)
    context_values = jnp.dot(context_normed, w_value, preferred_element_type=jnp.float32).astype(jnp.bfloat16)
    context_state = jnp.einsum('jhd,jhv->hdv', context_keys.reshape(CTX, RETENTION_HEADS, DK).astype(jnp.float32), context_values.reshape(CTX, RETENTION_HEADS, DV).astype(jnp.float32)) * float(CTX_LIFT)
    queries = query_rows.reshape(LATENT_TOKENS, RETENTION_HEADS, DK)
    key_heads = key_rows.reshape(LATENT_TOKENS, RETENTION_HEADS, DK)
    value_heads = value_rows.reshape(LATENT_TOKENS, RETENTION_HEADS, DV)
    forward = sweep_blocks(queries, key_heads, value_heads, log_decay, context_state)
    backward = jnp.flip(sweep_blocks(jnp.flip(queries, 0), jnp.flip(key_heads, 0), jnp.flip(value_heads, 0), jnp.flip(log_decay, 0), context_state), 0)
    mixed_heads = forward + backward
    average = lax.optimization_barrier(jnp.mean(mixed_heads, axis=-1, keepdims=True))
    variance = lax.optimization_barrier(jnp.mean(jnp.square(mixed_heads - average), axis=-1, keepdims=True))
    normal_heads = ((mixed_heads - average) * lax.rsqrt(variance + epsilon)).reshape(LATENT_TOKENS, RETENTION_HEADS * DV)
    attended = (jax.nn.silu(gate_rows.astype(jnp.float32)) * normal_heads * group_gain.astype(jnp.float32)).astype(jnp.bfloat16)
    group_width = attended.shape[1] // N_TP
    projected = jnp.zeros((LATENT_TOKENS, D), jnp.float32)
    for group in range(N_TP):
        partial_sum = jnp.dot(attended[:, group * group_width:(group + 1) * group_width], w_output[group * group_width:(group + 1) * group_width], preferred_element_type=jnp.float32)
        projected = projected + narrowed(partial_sum)
    return (latent.astype(jnp.float32) + modulation[0, 2 * D:] * projected).astype(jnp.bfloat16)
```

```python
import jax
import jax.numpy as jnp
from jax import lax
from jax.experimental import pallas as pl
from jax.experimental.pallas import tpu as pltpu
from jax.sharding import Mesh
from jax.sharding import PartitionSpec as P

DK = 256
DV = 512
GRID_W = 64
CTX_LIFT = 4
SP = ("z", "y")
TP = ("x", "c")
ALL = ("z", "y", "x", "c")
f32 = jnp.float32
bf16 = jnp.bfloat16

epsilon = 1e-06
rotary_base = 10000.0
MIB = 1024 * 1024


def from_everyone(array, axis):
    size = lax.axis_size(axis)
    return lax.all_to_all(
        jnp.broadcast_to(array[None], (size, *array.shape)), axis, 0, 0, tiled=True
    )


def kernel_call(body, outs, vmem, flops, *args):
    moved = sum(a.size * a.dtype.itemsize for a in args)
    return pl.pallas_call(
        body,
        out_shape=outs,
        compiler_params=pltpu.CompilerParams(vmem_limit_bytes=vmem * MIB),
        cost_estimate=pl.CostEstimate(flops=flops, bytes_accessed=moved, transcendentals=0),
    )(*args)


def dot(a, b):
    return jnp.dot(a, b, preferred_element_type=f32)


def dot_t(a, b):
    return lax.dot_general(a, b, (((1,), (1,)), ((), ())), preferred_element_type=f32)


def turn(u, tab_ref):
    lanes = lax.broadcasted_iota(jnp.int32, u.shape, 1)
    swapped = jnp.where(lanes % 2 == 0, pltpu.roll(u, DK - 1, 1), pltpu.roll(u, 1, 1))
    return u * tab_ref[:, :DK] + swapped * tab_ref[:, DK:]


def keys_kernel(
    own_ref, other_ref, ctx_ref, mod_ref, gain_ref, wk_ref, wv_ref, tab_ref, col_ref,
    send_ref, normed_ref, k_ref, v_ref,
):
    width = own_ref.shape[1]
    gain = gain_ref[...].astype(f32)
    tp = mod_ref.shape[0]

    def modulated(rows, which):
        line = jnp.concatenate([mod_ref[t, which : which + 1, :] for t in range(tp)], axis=1)
        shift, scale = line[:, :width], line[:, width : 2 * width]
        wide = rows.astype(f32)
        normal = wide * lax.rsqrt(jnp.mean(wide * wide, axis=-1, keepdims=True) + epsilon)
        return (normal * gain * (1.0 + scale) + shift).astype(bf16)

    half = own_ref.shape[0]
    rows = 2 * half
    normed_ref[0:half, :] = modulated(own_ref[...], 0)
    normed_ref[half:rows, :] = modulated(other_ref[...], 0)
    normed_ref[rows:, :] = modulated(ctx_ref[...], 1)
    keys = dot(normed_ref[...], wk_ref[...])
    values = dot(normed_ref[...], wv_ref[...]).astype(bf16)
    key_rows = (turn(keys[:rows], tab_ref) * DK ** (-0.5)).astype(bf16)
    ctx_keys = (keys[rows:] * DK ** (-0.5)).astype(bf16)
    k_ref[...] = key_rows
    v_ref[...] = values[:rows]
    wide = key_rows.astype(f32)
    ahead = (wide * jnp.exp(col_ref[:, 0:1])).astype(bf16)
    behind = (wide * jnp.exp(col_ref[:, 1:2])).astype(bf16)
    turned = values.T
    send_ref[:, 0:DK] = dot(turned[:, :rows], ahead).astype(bf16)
    send_ref[:, DK : 2 * DK] = dot(turned[:, :rows], behind).astype(bf16)
    send_ref[:, 2 * DK :] = dot(turned[:, rows:], ctx_keys).astype(bf16)


def inside_kernel(
    normed_ref, k_ref, v_ref, wq_ref, wg_ref, tab_ref, col_ref, line_ref, q_ref, g_ref, y_ref
):
    rows = k_ref.shape[0]
    queries = turn(dot(normed_ref[0:rows, :], wq_ref[...]), tab_ref).astype(bf16)
    q_ref[...] = queries
    g_ref[...] = dot(normed_ref[0:rows, :], wg_ref[...]).astype(bf16)
    scores = dot_t(queries, k_ref[...])
    here, there = col_ref[:, 4:5], line_ref[2:3, :]
    gaps = jnp.where(
        here >= there,
        col_ref[:, 2:3] - line_ref[0:1, :],
        line_ref[1:2, :] - col_ref[:, 1:2],
    )
    weights = jnp.exp(gaps) * jnp.where(here == there, 2.0, 1.0)
    y_ref[...] = dot((scores * weights).astype(bf16), v_ref[...])


def scan_kernel(parts_ref, decay_ref, out_ref):
    count = parts_ref.shape[0]
    lift = jnp.zeros((parts_ref.shape[1], DK), f32)
    for r in range(count):
        lift = lift + parts_ref[r, :, 2 * DK :].astype(f32)
    ahead = behind = lift * float(CTX_LIFT)
    for r in range(count):
        s = count - 1 - r
        out_ref[r, :, 0:DK] = ahead.astype(bf16)
        out_ref[s, :, DK:] = behind.astype(bf16)
        ahead = decay_ref[r : r + 1, :] * ahead + parts_ref[r, :, 0:DK].astype(f32)
        behind = decay_ref[s : s + 1, :] * behind + parts_ref[s, :, DK : 2 * DK].astype(f32)


def output_kernel(y_ref, q_ref, g_ref, states_ref, col_ref, gain_ref, wo_ref, out_ref):
    queries = q_ref[...]
    mixed = (
        y_ref[...]
        + jnp.exp(col_ref[:, 2:3]) * dot_t(queries, states_ref[:, 0:DK])
        + jnp.exp(col_ref[:, 3:4]) * dot_t(queries, states_ref[:, DK:])
    )
    average = jnp.mean(mixed, axis=-1, keepdims=True)
    centred = mixed - average
    variance = jnp.mean(centred * centred, axis=-1, keepdims=True)
    gates = g_ref[...].astype(f32)
    attended = (
        gates * jax.nn.sigmoid(gates) * (centred * lax.rsqrt(variance + epsilon))
        * gain_ref[...].astype(f32)
    ).astype(bf16)
    out_ref[...] = dot(attended, wo_ref[...]).astype(bf16)


def shaped(*shape, dtype=bf16):
    return jax.ShapeDtypeStruct(shape, dtype)


def per_device(
    latent,
    log_decay,
    context,
    condition,
    w_modulate,
    norm_gain,
    w_query,
    w_key,
    w_value,
    w_gate,
    group_gain,
    w_output,
):
    seq_index = lax.axis_index(SP)
    core = lax.axis_index("c")
    lines, width = latent.shape
    x_size = lax.axis_size("x")
    half = lines * x_size
    rows = 2 * half
    swap = [(0, 1), (1, 0)]

    own_rows = from_everyone(latent, "x").reshape(half, width)
    other_rows = lax.ppermute(own_rows, "c", swap)

    activated = jax.nn.silu(condition.astype(f32)).astype(bf16)
    input_rows = w_modulate.shape[0]
    own_inputs = lax.dynamic_slice_in_dim(activated, seq_index * input_rows, input_rows, 1)
    partial_mod = jnp.dot(own_inputs, w_modulate, preferred_element_type=f32)
    total = jnp.sum(log_decay)
    packed = jnp.concatenate(
        [partial_mod, jnp.broadcast_to(total[None, None], (1, partial_mod.shape[1]))], axis=0
    )
    pieces = from_everyone(packed, SP)
    modulation = from_everyone(jnp.sum(pieces[:, :2], axis=0), TP)
    decays = jnp.exp(pieces[:, 2, :DK])

    local = jnp.arange(rows, dtype=jnp.int32)
    grid_row = (local // lines) % x_size
    grid_column = ((local // half + core) % 2) * lines + local % lines
    here = grid_row * GRID_W + grid_column
    slots = jnp.arange(rows, dtype=jnp.int32)
    flat = log_decay[:, 0]
    upto = jnp.sum(jnp.where(slots[None, :] <= here[:, None], flat[None, :], 0.0), axis=1)
    before = jnp.sum(jnp.where(slots[None, :] < here[:, None], flat[None, :], 0.0), axis=1)
    place = here.astype(f32)
    col = jnp.stack([total - upto, before, upto, total - before, place], axis=1)
    line = jnp.stack([upto, before, place], axis=0)

    pairs = DK // 4
    inverse = rotary_base ** (-jnp.arange(pairs, dtype=f32) / pairs)
    inverse = jnp.repeat(inverse, 2)
    first_row = seq_index * (rows // GRID_W)
    angles = jnp.concatenate(
        [
            (first_row + grid_row).astype(f32)[:, None] * inverse,
            grid_column.astype(f32)[:, None] * inverse,
        ],
        axis=1,
    )
    sign = jnp.where(jnp.arange(DK) % 2 == 0, -1.0, 1.0)
    table = jnp.concatenate([jnp.cos(angles), jnp.sin(angles) * sign], axis=1)

    ctx = context.shape[0]
    send, normed, key_rows, value_rows = kernel_call(
        keys_kernel,
        (shaped(DV, 3 * DK), shaped(rows + ctx, width), shaped(rows, DK), shaped(rows, DV)),
        32,
        2 * (rows + ctx) * width * (DK + DV),
        own_rows,
        other_rows,
        context,
        modulation,
        norm_gain[None],
        w_key,
        w_value,
        table,
        col,
    )
    count = lax.axis_size(SP)
    parts = lax.all_to_all(send.reshape(count, DV // count, 3 * DK), SP, 0, 0, tiled=True)
    queries, gates, inside = kernel_call(
        inside_kernel,
        (shaped(rows, DK), shaped(rows, DV), shaped(rows, DV, dtype=f32)),
        32,
        2 * rows * width * (DK + DV),
        normed,
        key_rows,
        value_rows,
        w_query,
        w_gate,
        table,
        col,
        line,
    )
    entering = kernel_call(
        scan_kernel, shaped(count, DV // count, 2 * DK), 16, 10 * parts.size, parts, decays
    )
    states = lax.all_to_all(entering, SP, 0, 0, tiled=True).reshape(DV, 2 * DK)
    partial = kernel_call(
        output_kernel,
        shaped(rows, width),
        32,
        2 * rows * DV * width,
        inside,
        queries,
        gates,
        states,
        col,
        group_gain[None],
        w_output,
    )
    crossed = lax.ppermute(partial[half:], "c", swap)
    paired = (partial[:half].astype(f32) + crossed.astype(f32)).astype(bf16)
    tiles = lax.all_to_all(paired.reshape(x_size, lines, width), "x", 0, 0, tiled=True)
    projected = jnp.sum(tiles.astype(f32), axis=0)
    gate = modulation[:, 0].reshape(-1)[2 * width :]
    return (latent.astype(f32) + gate * projected).astype(bf16)


def solution(mesh):
    torus = Mesh(mesh.devices.reshape(8, 4, 4, 2), ALL)
    in_specs = (
        P(ALL, None),
        P(SP, TP),
        P(SP, None),
        P(),
        P(SP, TP),
        P(),
        P(None, TP),
        P(None, TP),
        P(None, TP),
        P(None, TP),
        P(TP),
        P(TP, None),
    )
    return jax.shard_map(
        per_device, mesh=torus, in_specs=in_specs, out_specs=P(ALL, None), check_vma=False
    )
```

```python
import jax
import jax.numpy as jnp
from jax import lax
from jax.experimental import pallas as pl
from jax.experimental.pallas import tpu as pltpu
from jax.sharding import Mesh
from jax.sharding import PartitionSpec as P

DK = 256
DV = 512
GRID_W = 64
CTX_LIFT = 4
SP = ("z", "y")
TP = ("x", "c")
ALL = ("z", "y", "x", "c")
f32 = jnp.float32
bf16 = jnp.bfloat16

epsilon = 1e-06
rotary_base = 10000.0
MIB = 1024 * 1024


def kernel_call(body, outs, ins, scratch, vmem, flops, *args):
    spaces = {"h": pltpu.MemorySpace.HBM, "v": pltpu.MemorySpace.VMEM}
    moved = sum(a.size * a.dtype.itemsize for a in args)
    args = [
        pltpu.with_memory_space_constraint(a, pltpu.HBM) if k == "h" else a
        for k, a in zip(ins, args)
    ]
    return pl.pallas_call(
        body,
        out_shape=tuple(pltpu.HBM(a.shape, a.dtype) if k == "h" else a for k, a in outs),
        in_specs=[pl.BlockSpec(memory_space=spaces[k]) for k in ins],
        out_specs=tuple(pl.BlockSpec(memory_space=spaces[k]) for k, _ in outs),
        scratch_shapes=scratch,
        compiler_params=pltpu.CompilerParams(vmem_limit_bytes=vmem * MIB),
        cost_estimate=pl.CostEstimate(flops=flops, bytes_accessed=moved, transcendentals=0),
    )(*args)


def started(source, target, sems, slot):
    copy = pltpu.make_async_copy(source, target, sems.at[slot])
    copy.start()
    return copy


def dot(a, b):
    return jnp.dot(a, b, preferred_element_type=f32)


def dot_t(a, b):
    return lax.dot_general(a, b, (((1,), (1,)), ((), ())), preferred_element_type=f32)


def turn(u, tab_ref):
    lanes = lax.broadcasted_iota(jnp.int32, u.shape, 1)
    swapped = jnp.where(lanes % 2 == 0, pltpu.roll(u, DK - 1, 1), pltpu.roll(u, 1, 1))
    return u * tab_ref[:, :DK] + swapped * tab_ref[:, DK:]


def prepare_kernel(inputs_ref, weights_ref, decay_ref, out_ref):
    inputs = inputs_ref[...].astype(f32)
    activated = (inputs / (1.0 + jnp.exp(-inputs))).astype(bf16)
    part = dot(activated, weights_ref[...])
    total = jnp.sum(decay_ref[...], axis=0, keepdims=True)
    packed = jnp.concatenate([part, jnp.broadcast_to(total, (1, part.shape[1]))], axis=0)
    for r in range(out_ref.shape[0]):
        out_ref[r] = packed


def gather_kernel(pieces_ref, out_ref, decay_ref):
    summed = pieces_ref[0, 0:2, :]
    for r in range(1, pieces_ref.shape[0]):
        summed = summed + pieces_ref[r, 0:2, :]
    for t in range(out_ref.shape[0]):
        out_ref[t] = summed
    for r in range(pieces_ref.shape[0]):
        decay_ref[r : r + 1, :] = jnp.exp(pieces_ref[r, 2:3, 0:DK])


def keys_kernel(*refs):
    pieces, refs = refs[:8], refs[8:]
    (
        near_hbm, far_hbm, tab_hbm, wk_hbm, mod_ref, gain_ref, wv_ref, col_ref, line_ref,
        send_hbm, normed_hbm, k_hbm, v_hbm,
        raw_ref, ctx_ref, tab_ref, wk_ref, normed_ref, k_ref, v_ref, send_ref, sems,
    ) = refs
    lines, width = pieces[0].shape
    half = 4 * lines
    rows = 2 * half
    near = near_hbm.shape[0]
    raws = [
        started(piece, raw_ref.at[i * lines : (i + 1) * lines], sems, 10 + i)
        for i, piece in enumerate(pieces)
    ]
    loads = [
        started(near_hbm, ctx_ref.at[0:near], sems, 2),
        started(far_hbm, ctx_ref.at[near:], sems, 3),
        started(tab_hbm, tab_ref, sems, 4),
        started(wk_hbm, wk_ref, sems, 9),
    ]
    gain = gain_ref[...].astype(f32)
    tp = mod_ref.shape[0]

    def modulated(values, which):
        line = jnp.concatenate([mod_ref[t, which : which + 1, :] for t in range(tp)], axis=1)
        shift, scale = line[:, :width], line[:, width : 2 * width]
        wide = values.astype(f32)
        normal = wide * lax.rsqrt(jnp.mean(wide * wide, axis=-1, keepdims=True) + epsilon)
        return (normal * gain * (1.0 + scale) + shift).astype(bf16)

    for part in range(2):
        own = slice(part * half, (part + 1) * half)
        for copy in raws[part * 4 : part * 4 + 4]:
            copy.wait()
        normed_ref[own, :] = modulated(raw_ref[own, :], 0)
    stores = [started(normed_ref.at[0:rows], normed_hbm, sems, 5)]
    loads[0].wait()
    loads[1].wait()
    normed_ref[rows:, :] = modulated(ctx_ref[...], 1)
    values = dot(normed_ref[...], wv_ref[...]).astype(bf16)
    loads[2].wait()
    loads[3].wait()
    keys = dot(normed_ref[...], wk_ref[...])
    key_rows = (turn(keys[:rows], tab_ref) * DK ** (-0.5)).astype(bf16)
    ctx_keys = (keys[rows:] * DK ** (-0.5)).astype(bf16)
    k_ref[...] = key_rows
    v_ref[...] = values[:rows]
    stores.append(started(k_ref, k_hbm, sems, 6))
    stores.append(started(v_ref, v_hbm, sems, 7))
    wide = key_rows.astype(f32)
    ahead = (wide * jnp.exp(col_ref[:, 0:1])).astype(bf16)
    behind = (wide * jnp.exp(col_ref[:, 1:2])).astype(bf16)
    turned = values.T
    send_ref[:, 0:DK] = dot(turned[:, :rows], ahead).astype(bf16)
    send_ref[:, DK : 2 * DK] = dot(turned[:, :rows], behind).astype(bf16)
    odd = line_ref[3:4, 0 : DK // 2] > 0.5
    own_keys = jnp.where(
        odd, ctx_keys[:, DK // 2 :].astype(f32), ctx_keys[:, : DK // 2].astype(f32)
    ).astype(bf16)
    send_ref[:, 2 * DK :] = dot(turned[:, rows:], own_keys).astype(bf16)
    stores.append(started(send_ref, send_hbm, sems, 8))
    for copy in stores:
        copy.wait()


def inside_kernel(
    normed_hbm, k_hbm, v_hbm, wq_hbm, wg_hbm, tab_hbm, col_ref, line_ref,
    q_hbm, g_hbm, y_hbm,
    normed_ref, k_ref, v_ref, wq_ref, wg_ref, tab_ref, q_ref, g_ref, y_ref, sems,
):
    pairs = [
        (normed_hbm, normed_ref), (wq_hbm, wq_ref), (tab_hbm, tab_ref), (k_hbm, k_ref),
        (v_hbm, v_ref), (wg_hbm, wg_ref),
    ]
    loads = [started(a, b, sems, i) for i, (a, b) in enumerate(pairs)]
    for copy in loads[:4]:
        copy.wait()
    queries = turn(dot(normed_ref[...], wq_ref[...]), tab_ref).astype(bf16)
    q_ref[...] = queries
    stores = [started(q_ref, q_hbm, sems, 6)]
    scores = dot_t(queries, k_ref[...])
    here, there = col_ref[:, 4:5], line_ref[2:3, :]
    gaps = jnp.where(
        here >= there,
        col_ref[:, 2:3] - line_ref[0:1, :],
        line_ref[1:2, :] - col_ref[:, 1:2],
    )
    weights = jnp.exp(gaps) * jnp.where(here == there, 2.0, 1.0)
    loads[4].wait()
    y_ref[...] = dot((scores * weights).astype(bf16), v_ref[...])
    stores.append(started(y_ref, y_hbm, sems, 7))
    loads[5].wait()
    g_ref[...] = dot(normed_ref[...], wg_ref[...]).astype(bf16)
    stores.append(started(g_ref, g_hbm, sems, 8))
    for copy in stores:
        copy.wait()


def scan_kernel(parts_ref, decay_ref, out_ref):
    count = parts_ref.shape[0]
    lifts = []
    for parity in range(2):
        lift = parts_ref[parity, :, 2 * DK :].astype(f32)
        for r in range(parity + 2, count, 2):
            lift = lift + parts_ref[r, :, 2 * DK :].astype(f32)
        lifts.append(lift)
    ahead = behind = jnp.concatenate(lifts, axis=1) * float(CTX_LIFT)
    for r in range(count):
        s = count - 1 - r
        out_ref[r, :, 0:DK] = ahead.astype(bf16)
        out_ref[s, :, DK:] = behind.astype(bf16)
        ahead = decay_ref[r : r + 1, :] * ahead + parts_ref[r, :, 0:DK].astype(f32)
        behind = decay_ref[s : s + 1, :] * behind + parts_ref[s, :, DK : 2 * DK].astype(f32)


def output_kernel(
    q_hbm, y_hbm, g_hbm, states_ref, col_ref, gain_ref, wo_ref,
    out_hbm,
    q_ref, y_ref, g_ref, out_ref, sems,
):
    pairs = [(q_hbm, q_ref), (y_hbm, y_ref), (g_hbm, g_ref)]
    loads = [started(a, b, sems, i) for i, (a, b) in enumerate(pairs)]
    for copy in loads:
        copy.wait()
    queries = q_ref[...]
    mixed = (
        y_ref[...]
        + jnp.exp(col_ref[:, 2:3]) * dot_t(queries, states_ref[:, 0:DK])
        + jnp.exp(col_ref[:, 3:4]) * dot_t(queries, states_ref[:, DK:])
    )
    average = jnp.mean(mixed, axis=-1, keepdims=True)
    centred = mixed - average
    variance = jnp.mean(centred * centred, axis=-1, keepdims=True)
    gates = g_ref[...].astype(f32)
    attended = (
        gates * jax.nn.sigmoid(gates) * (centred * lax.rsqrt(variance + epsilon))
        * gain_ref[...].astype(f32)
    ).astype(bf16)
    half = out_hbm.shape[0] // 2
    stores = []
    for part in (1, 0):
        own = slice(part * half, (part + 1) * half)
        out_ref[own, :] = dot(attended[own], wo_ref[...]).astype(bf16)
        stores.append(started(out_ref.at[own], out_hbm.at[own], sems, 3 + part))
    for copy in stores:
        copy.wait()


def ring(size, step):
    return [(i, (i + step) % size) for i in range(size)]


def shaped(*shape, dtype=bf16):
    return jax.ShapeDtypeStruct(shape, dtype)


def per_device(
    latent,
    log_decay,
    context,
    condition,
    w_modulate,
    norm_gain,
    w_query,
    w_key,
    w_value,
    w_gate,
    group_gain,
    w_output,
):
    seq_index = lax.axis_index(SP)
    core = lax.axis_index("c")
    lines, width = latent.shape
    x_size = lax.axis_size("x")
    half = lines * x_size
    rows = 2 * half
    swap = [(0, 1), (1, 0)]

    input_rows, columns = w_modulate.shape
    own_inputs = lax.dynamic_slice_in_dim(condition, seq_index * input_rows, input_rows, 1)
    count, tp = lax.axis_size(SP), lax.axis_size(TP)
    (packed,) = kernel_call(
        prepare_kernel,
        [("v", shaped(count, 3, columns, dtype=f32))],
        "vvv",
        [],
        4,
        1000000,
        own_inputs,
        w_modulate,
        log_decay,
    )
    pieces = lax.all_to_all(packed, SP, 0, 0, tiled=True)
    spread, decays = kernel_call(
        gather_kernel,
        [("v", shaped(tp, 2, columns, dtype=f32)), ("v", shaped(count, DK, dtype=f32))],
        "v",
        [],
        4,
        1000000,
        pieces,
    )
    modulation = lax.all_to_all(spread, TP, 0, 0, tiled=True)

    later, spare_decay, place_index, _ = lax.optimization_barrier(
        (latent, log_decay, jnp.stack([seq_index, core, lax.axis_index("y") % 2, lax.axis_index("x")]), packed)
    )
    own_rows = [later] + [lax.ppermute(later, "x", ring(x_size, d)) for d in range(1, x_size)]
    other_rows = [lax.ppermute(piece, "c", swap) for piece in own_rows]
    far = lax.ppermute(context, "y", [(0, 1), (1, 0), (2, 3), (3, 2)])
    total = jnp.sum(spare_decay)

    local = jnp.arange(rows, dtype=jnp.int32)
    grid_row = (place_index[3] - local // lines) % x_size
    grid_column = ((local // half + place_index[1]) % 2) * lines + local % lines
    here = grid_row * GRID_W + grid_column
    slots = jnp.arange(rows, dtype=jnp.int32)
    flat = spare_decay[:, 0]
    upto = jnp.sum(jnp.where(slots[None, :] <= here[:, None], flat[None, :], 0.0), axis=1)
    before = jnp.sum(jnp.where(slots[None, :] < here[:, None], flat[None, :], 0.0), axis=1)
    place = here.astype(f32)
    col = jnp.stack([total - upto, before, upto, total - before, place], axis=1)
    odd = jnp.full((rows,), place_index[2], f32)
    line = jnp.stack([upto, before, place, odd], axis=0)

    pairs = DK // 4
    inverse = rotary_base ** (-jnp.arange(pairs, dtype=f32) / pairs)
    inverse = jnp.repeat(inverse, 2)
    first_row = place_index[0] * (rows // GRID_W)
    angles = jnp.concatenate(
        [
            (first_row + grid_row).astype(f32)[:, None] * inverse,
            grid_column.astype(f32)[:, None] * inverse,
        ],
        axis=1,
    )
    sign = jnp.where(jnp.arange(DK) % 2 == 0, -1.0, 1.0)
    table = jnp.concatenate([jnp.cos(angles), jnp.sin(angles) * sign], axis=1)

    ctx = 2 * context.shape[0]
    lanes = 2 * DK + DK // 2
    sems = pltpu.SemaphoreType.DMA
    send, normed, key_rows, value_rows = kernel_call(
        keys_kernel,
        [
            ("h", shaped(DV, lanes)),
            ("h", shaped(rows, width)),
            ("h", shaped(rows, DK)),
            ("h", shaped(rows, DV)),
        ],
        "hhhhhhhh" + "hhhhvvvvv",
        [
            pltpu.VMEM((rows, width), bf16),
            pltpu.VMEM((ctx, width), bf16),
            pltpu.VMEM((rows, 2 * DK), f32),
            pltpu.VMEM((width, DK), bf16),
            pltpu.VMEM((rows + ctx, width), bf16),
            pltpu.VMEM((rows, DK), bf16),
            pltpu.VMEM((rows, DV), bf16),
            pltpu.VMEM((DV, lanes), bf16),
            sems((18,)),
        ],
        32,
        2 * (rows + ctx) * width * (DK + DV),
        *own_rows,
        *other_rows,
        context,
        far,
        table,
        w_key,
        modulation,
        norm_gain[None],
        w_value,
        col,
        line,
    )
    parts = lax.all_to_all(send.reshape(count, DV // count, lanes), SP, 0, 0, tiled=True)
    queries, gates, inside = kernel_call(
        inside_kernel,
        [
            ("h", shaped(rows, DK)),
            ("h", shaped(rows, DV)),
            ("h", shaped(rows, DV, dtype=f32)),
        ],
        "hhhhhhvv",
        [
            pltpu.VMEM((rows, width), bf16),
            pltpu.VMEM((rows, DK), bf16),
            pltpu.VMEM((rows, DV), bf16),
            pltpu.VMEM((width, DK), bf16),
            pltpu.VMEM((width, DV), bf16),
            pltpu.VMEM((rows, 2 * DK), f32),
            pltpu.VMEM((rows, DK), bf16),
            pltpu.VMEM((rows, DV), bf16),
            pltpu.VMEM((rows, DV), f32),
            sems((9,)),
        ],
        32,
        2 * rows * width * (DK + DV),
        normed,
        key_rows,
        value_rows,
        w_query,
        w_gate,
        table,
        col,
        line,
    )
    (entering,) = kernel_call(
        scan_kernel,
        [("v", shaped(count, DV // count, 2 * DK))],
        "vv",
        [],
        16,
        10 * parts.size,
        parts,
        decays,
    )
    states = lax.all_to_all(entering, SP, 0, 0, tiled=True).reshape(DV, 2 * DK)
    (partial,) = kernel_call(
        output_kernel,
        [("h", shaped(rows, width))],
        "hhhvvvv",
        [
            pltpu.VMEM((rows, DK), bf16),
            pltpu.VMEM((rows, DV), f32),
            pltpu.VMEM((rows, DV), bf16),
            pltpu.VMEM((rows, width), bf16),
            sems((5,)),
        ],
        32,
        2 * rows * DV * width,
        queries,
        inside,
        gates,
        states,
        col,
        group_gain[None],
        w_output,
    )
    crossed = lax.ppermute(partial[half:], "c", swap)
    paired = (partial[:half].astype(f32) + crossed.astype(f32)).astype(bf16)
    tiles = paired.reshape(x_size, lines, width)
    projected = tiles[0].astype(f32)
    for d in range(1, x_size):
        arrived = lax.ppermute(tiles[d], "x", ring(x_size, -d))
        projected = projected + arrived.astype(f32)
    gate = modulation[:, 0].reshape(-1)[2 * width :]
    return (latent.astype(f32) + gate * projected).astype(bf16)


def solution(mesh):
    torus = Mesh(mesh.devices.reshape(8, 4, 4, 2), ALL)
    in_specs = (
        P(ALL, None),
        P(SP, TP),
        P(SP, None),
        P(),
        P(SP, TP),
        P(),
        P(None, TP),
        P(None, TP),
        P(None, TP),
        P(None, TP),
        P(TP),
        P(TP, None),
    )
    return jax.shard_map(
        per_device, mesh=torus, in_specs=in_specs, out_specs=P(ALL, None), check_vma=False
    )
```

```python
import functools

import jax
import jax.numpy as jnp
import numpy as np
from jax import lax
from jax.experimental import pallas as pl
from jax.experimental.pallas import tpu as pltpu
from jax.sharding import Mesh
from jax.sharding import PartitionSpec as P

DK = 256
DV = 512
GRID_W = 64
CTX_LIFT = 4
SP = ("z", "y")
TP = ("x", "c")
ALL = ("z", "y", "x", "c")
f32 = jnp.float32
bf16 = jnp.bfloat16

epsilon = 1e-06
rotary_base = 10000.0
MIB = 1024 * 1024


def kernel_call(body, outs, ins, scratch, vmem, flops, *args):
    spaces = {"h": pltpu.MemorySpace.HBM, "v": pltpu.MemorySpace.VMEM}
    moved = sum(a.size * a.dtype.itemsize for a in args)
    args = [
        pltpu.with_memory_space_constraint(a, pltpu.HBM) if k == "h" else a
        for k, a in zip(ins, args)
    ]
    return pl.pallas_call(
        body,
        out_shape=tuple(pltpu.HBM(a.shape, a.dtype) if k == "h" else a for k, a in outs),
        in_specs=[pl.BlockSpec(memory_space=spaces[k]) for k in ins],
        out_specs=tuple(pl.BlockSpec(memory_space=spaces[k]) for k, _ in outs),
        scratch_shapes=scratch,
        compiler_params=pltpu.CompilerParams(vmem_limit_bytes=vmem * MIB),
        cost_estimate=pl.CostEstimate(flops=flops, bytes_accessed=moved, transcendentals=0),
    )(*args)


def started(source, target, sems, slot):
    copy = pltpu.make_async_copy(source, target, sems.at[slot])
    copy.start()
    return copy


def dot(a, b):
    return jnp.dot(a, b, preferred_element_type=f32)


def dot_t(a, b):
    return lax.dot_general(a, b, (((1,), (1,)), ((), ())), preferred_element_type=f32)


def turn(u, tab_ref):
    lanes = lax.broadcasted_iota(jnp.int32, u.shape, 1)
    swapped = jnp.where(lanes % 2 == 0, pltpu.roll(u, DK - 1, 1), pltpu.roll(u, 1, 1))
    return u * tab_ref[:, :DK] + swapped * tab_ref[:, DK:]


def prepare_kernel(
    weights_hbm, condition_hbm, decay_hbm, out_ref, weights_ref, condition_ref, decay_ref, sems
):
    loads = [
        started(condition_hbm, condition_ref, sems, 0),
        started(decay_hbm, decay_ref, sems, 1),
        started(weights_hbm, weights_ref, sems, 2),
    ]
    size, width = weights_hbm.shape[0], condition_hbm.shape[1]
    seq = lax.axis_index("z") * lax.axis_size("y") + lax.axis_index("y")
    loads[0].wait()
    values = condition_ref[...].astype(f32)
    values = jnp.concatenate([values] * 4, axis=0)
    inputs = pltpu.roll(values, (width - seq * size) % width, 1)[0:2, 0:size]
    activated = (inputs / (1.0 + jnp.exp(-inputs))).astype(bf16)
    loads[1].wait()
    total = jnp.sum(decay_ref[...], axis=1, keepdims=True)
    loads[2].wait()
    part = dot(activated, weights_ref[...])
    packed = jnp.concatenate([part, jnp.broadcast_to(total, (1, part.shape[1]))], axis=0)
    for r in range(out_ref.shape[0]):
        out_ref[r] = packed


def rotary_tables(count):
    pairs = DK // 4
    exponents = -np.arange(pairs, dtype=np.float32) / np.float32(pairs)
    inverse = np.repeat(np.float32(rotary_base) ** exponents, 2).astype(np.float32)
    angles = np.arange(count, dtype=np.float32)[:, None] * inverse
    sign = np.where(np.arange(DK // 2) % 2 == 0, -1.0, 1.0).astype(np.float32)
    return np.concatenate([np.cos(angles), np.sin(angles) * sign], axis=1)


def tables_kernel(
    lines, chips, decay_hbm, row_hbm, column_hbm, col_ref, line_ref, tab_hbm,
    decay_ref, row_ref, column_ref, tab_ref, sems,
):
    loads = [
        started(row_hbm, row_ref, sems, 1),
        started(column_hbm, column_ref, sems, 2),
        started(decay_hbm, decay_ref, sems, 3),
    ]
    rows = 2 * chips * lines
    seq = lax.axis_index("z") * lax.axis_size("y") + lax.axis_index("y")
    chip, core = lax.axis_index("x"), lax.axis_index("c")
    pair = DK // 2
    loads[0].wait()
    loads[1].wait()
    for h in range(2):
        column = pl.multiple_of(((h + core) % 2) * lines, lines)
        for d in range(chips):
            own = slice((h * chips + d) * lines, (h * chips + d + 1) * lines)
            row = seq * chips + (chip - d + chips) % chips
            for k in range(2):
                part = slice(k * pair, (k + 1) * pair)
                tab_ref[own, k * DK : k * DK + pair] = jnp.broadcast_to(
                    row_ref[row, :, part], (lines, pair)
                )
                tab_ref[own, k * DK + pair : (k + 1) * DK] = column_ref[
                    pl.ds(column, lines), part
                ]
    store = started(tab_ref, tab_hbm, sems, 0)

    def position(local):
        origin = (chip - (local // lines) % chips + chips) % chips
        return origin * GRID_W + ((local // (chips * lines) + core) % 2) * lines + local % lines

    down = lax.broadcasted_iota(jnp.int32, (rows, rows), 0)
    across = lax.broadcasted_iota(jnp.int32, (rows, rows), 1)
    place_col = position(lax.broadcasted_iota(jnp.int32, (rows, 1), 0))
    place_line = position(lax.broadcasted_iota(jnp.int32, (1, rows), 1))
    loads[2].wait()
    flat = decay_ref[...]
    total = jnp.sum(flat, axis=1, keepdims=True)
    flat_col = jnp.sum(jnp.where(down == across, flat, 0.0), axis=1, keepdims=True)
    upto = jnp.sum(jnp.where(across <= place_col, flat, 0.0), axis=1, keepdims=True)
    before = jnp.sum(jnp.where(across < place_col, flat, 0.0), axis=1, keepdims=True)
    col_ref[:, 0:1] = total - upto
    col_ref[:, 1:2] = before
    col_ref[:, 2:3] = upto
    col_ref[:, 3:4] = total - before
    col_ref[:, 4:5] = place_col.astype(f32)
    line_ref[0:1, :] = jnp.sum(jnp.where(down <= place_line, flat_col, 0.0), axis=0, keepdims=True)
    line_ref[1:2, :] = jnp.sum(jnp.where(down < place_line, flat_col, 0.0), axis=0, keepdims=True)
    line_ref[2:3, :] = place_line.astype(f32)
    odd = lax.axis_index("y") % 2
    line_ref[3:4, :] = jnp.full((1, rows), odd, jnp.int32).astype(f32)
    store.wait()


def gather_kernel(pieces_ref, out_ref, decay_ref):
    summed = pieces_ref[0, 0:2, :]
    for r in range(1, pieces_ref.shape[0]):
        summed = summed + pieces_ref[r, 0:2, :]
    for t in range(out_ref.shape[0]):
        out_ref[t] = summed
    for r in range(pieces_ref.shape[0]):
        decay_ref[r : r + 1, :] = jnp.exp(pieces_ref[r, 2:3, 0:DK])


def keys_kernel(*refs):
    pieces, refs = refs[:8], refs[8:]
    (
        near_hbm, far_ref, tab_hbm, wk_hbm, wv_hbm, mod_ref, gain_ref, col_ref, line_ref,
        send_hbm, normed_hbm, k_hbm, v_hbm,
        own_ref, near_ref, tab_ref, wk_ref, wv_ref, normed_ref, k_ref, v_ref, send_ref, sems,
    ) = refs
    lines, width = pieces[0].shape
    rows = 8 * lines
    near = near_ref.shape[0]
    own = [started(pieces[0], own_ref, sems, 7), started(near_hbm, near_ref, sems, 8)]
    loads = [
        started(wv_hbm, wv_ref, sems, 0),
        started(wk_hbm, wk_ref, sems, 1),
        started(tab_hbm, tab_ref, sems, 2),
    ]
    gain = gain_ref[...].astype(f32)
    tp = mod_ref.shape[0]

    def modulated(values, which):
        line = jnp.concatenate([mod_ref[t, which : which + 1, :] for t in range(tp)], axis=1)
        shift, scale = line[:, :width], line[:, width : 2 * width]
        wide = values.astype(f32)
        normal = wide * lax.rsqrt(jnp.mean(wide * wide, axis=-1, keepdims=True) + epsilon)
        return (normal * gain * (1.0 + scale) + shift).astype(bf16)

    for i, piece in enumerate(pieces[1:]):
        normed_ref[(i + 1) * lines : (i + 2) * lines, :] = modulated(piece[...], 0)
    normed_ref[rows + near :, :] = modulated(far_ref[...], 1)
    for copy in own:
        copy.wait()
    normed_ref[0:lines, :] = modulated(own_ref[...], 0)
    normed_ref[rows : rows + near, :] = modulated(near_ref[...], 1)
    loads[0].wait()
    values = dot(normed_ref[...], wv_ref[...]).astype(bf16)
    loads[1].wait()
    keys = dot(normed_ref[...], wk_ref[...])
    loads[2].wait()
    key_rows = (turn(keys[:rows], tab_ref) * DK ** (-0.5)).astype(bf16)
    ctx_keys = (keys[rows:] * DK ** (-0.5)).astype(bf16)
    k_ref[...] = key_rows
    v_ref[...] = values[:rows]
    wide = key_rows.astype(f32)
    ahead = (wide * jnp.exp(col_ref[:, 0:1])).astype(bf16)
    behind = (wide * jnp.exp(col_ref[:, 1:2])).astype(bf16)
    turned = values.T
    send_ref[:, 0:DK] = dot(turned[:, :rows], ahead).astype(bf16)
    send_ref[:, DK : 2 * DK] = dot(turned[:, :rows], behind).astype(bf16)
    odd = line_ref[3:4, 0 : DK // 2] > 0.5
    own_keys = jnp.where(
        odd, ctx_keys[:, DK // 2 :].astype(f32), ctx_keys[:, : DK // 2].astype(f32)
    ).astype(bf16)
    send_ref[:, 2 * DK :] = dot(turned[:, rows:], own_keys).astype(bf16)
    stores = [
        started(send_ref, send_hbm, sems, 3),
        started(normed_ref.at[0:rows], normed_hbm, sems, 4),
        started(k_ref, k_hbm, sems, 5),
        started(v_ref, v_hbm, sems, 6),
    ]
    for copy in stores:
        copy.wait()


def inside_kernel(
    normed_hbm, k_hbm, v_hbm, wq_hbm, wg_hbm, tab_hbm, col_ref, line_ref,
    q_ref, g_hbm, y_hbm,
    normed_ref, k_ref, v_ref, wq_ref, wg_ref, tab_ref, g_ref, y_ref, sems,
):
    pairs = [
        (normed_hbm, normed_ref), (wq_hbm, wq_ref), (tab_hbm, tab_ref), (k_hbm, k_ref),
        (v_hbm, v_ref), (wg_hbm, wg_ref),
    ]
    loads = [started(a, b, sems, i) for i, (a, b) in enumerate(pairs)]
    for copy in loads[:4]:
        copy.wait()
    queries = turn(dot(normed_ref[...], wq_ref[...]), tab_ref).astype(bf16)
    q_ref[...] = queries
    scores = dot_t(queries, k_ref[...])
    here, there = col_ref[:, 4:5], line_ref[2:3, :]
    gaps = jnp.where(
        here >= there,
        col_ref[:, 2:3] - line_ref[0:1, :],
        line_ref[1:2, :] - col_ref[:, 1:2],
    )
    weights = jnp.exp(gaps) * jnp.where(here == there, 2.0, 1.0)
    loads[4].wait()
    y_ref[...] = dot((scores * weights).astype(bf16), v_ref[...])
    stores = [started(y_ref, y_hbm, sems, 7)]
    loads[5].wait()
    g_ref[...] = dot(normed_ref[...], wg_ref[...]).astype(bf16)
    stores.append(started(g_ref, g_hbm, sems, 8))
    for copy in stores:
        copy.wait()


def scan_kernel(parts_ref, decay_ref, out_ref):
    count = parts_ref.shape[0]
    lifts = []
    for parity in range(2):
        lift = parts_ref[parity, :, 2 * DK :].astype(f32)
        for r in range(parity + 2, count, 2):
            lift = lift + parts_ref[r, :, 2 * DK :].astype(f32)
        lifts.append(lift)
    ahead = behind = jnp.concatenate(lifts, axis=1) * float(CTX_LIFT)
    for r in range(count):
        s = count - 1 - r
        out_ref[r, :, 0:DK] = ahead.astype(bf16)
        out_ref[s, :, DK:] = behind.astype(bf16)
        ahead = decay_ref[r : r + 1, :] * ahead + parts_ref[r, :, 0:DK].astype(f32)
        behind = decay_ref[s : s + 1, :] * behind + parts_ref[s, :, DK : 2 * DK].astype(f32)


def output_kernel(
    part, y_hbm, g_hbm, q_ref, states_ref, col_ref, gain_ref, wo_ref, out_ref, y_ref, g_ref, sems
):
    half = out_ref.shape[0]
    own = slice(part * half, (part + 1) * half)
    loads = [started(y_hbm.at[own], y_ref, sems, 0), started(g_hbm.at[own], g_ref, sems, 1)]
    queries = q_ref[own, :]
    mixed = jnp.exp(col_ref[own, 2:3]) * dot_t(queries, states_ref[:, 0:DK]) + jnp.exp(
        col_ref[own, 3:4]
    ) * dot_t(queries, states_ref[:, DK:])
    loads[0].wait()
    mixed = mixed + y_ref[...]
    average = jnp.mean(mixed, axis=-1, keepdims=True)
    centred = mixed - average
    variance = jnp.mean(centred * centred, axis=-1, keepdims=True)
    loads[1].wait()
    gates = g_ref[...].astype(f32)
    attended = (
        gates * jax.nn.sigmoid(gates) * (centred * lax.rsqrt(variance + epsilon))
        * gain_ref[...].astype(f32)
    ).astype(bf16)
    out_ref[...] = dot(attended, wo_ref[...]).astype(bf16)


def pair_kernel(own_ref, crossed_ref, *out_refs):
    lines = out_refs[0].shape[0]
    for d, out_ref in enumerate(out_refs):
        own = slice(d * lines, (d + 1) * lines)
        out_ref[...] = (own_ref[own, :].astype(f32) + crossed_ref[own, :].astype(f32)).astype(bf16)


def ring(size, step):
    return [(i, (i + step) % size) for i in range(size)]


def shaped(*shape, dtype=bf16):
    return jax.ShapeDtypeStruct(shape, dtype)


def per_device(
    latent,
    log_decay,
    context,
    condition,
    w_modulate,
    norm_gain,
    w_query,
    w_key,
    w_value,
    w_gate,
    group_gain,
    w_output,
):
    lines, width = latent.shape
    x_size = lax.axis_size("x")
    half = lines * x_size
    rows = 2 * half
    swap = [(0, 1), (1, 0)]

    columns = w_modulate.shape[1]
    sems = pltpu.SemaphoreType.DMA
    count, tp = lax.axis_size(SP), lax.axis_size(TP)
    (packed,) = kernel_call(
        prepare_kernel,
        [("v", shaped(count, 3, columns, dtype=f32))],
        "hhh",
        [
            pltpu.VMEM(w_modulate.shape, bf16),
            pltpu.VMEM(condition.shape, bf16),
            pltpu.VMEM((1, rows), f32),
            sems((3,)),
        ],
        4,
        1000000,
        w_modulate,
        condition,
        log_decay.T,
    )
    pieces = lax.all_to_all(packed, SP, 0, 0, tiled=True)
    spread, decays = kernel_call(
        gather_kernel,
        [("v", shaped(tp, 2, columns, dtype=f32)), ("v", shaped(count, DK, dtype=f32))],
        "v",
        [],
        4,
        1000000,
        pieces,
    )
    modulation = lax.all_to_all(spread, TP, 0, 0, tiled=True)

    later, near, later_decay, _ = lax.optimization_barrier((latent, context, log_decay.T, packed))
    own_rows = [later] + [lax.ppermute(later, "x", ring(x_size, d)) for d in range(1, x_size)]
    other_rows = [lax.ppermute(piece, "c", swap) for piece in own_rows]
    far = lax.ppermute(near, "y", [(0, 1), (1, 0), (2, 3), (3, 2)])
    seq_rows = count * rows // GRID_W
    col, line, table = kernel_call(
        functools.partial(tables_kernel, lines, x_size),
        [
            ("v", shaped(rows, 8, dtype=f32)),
            ("v", shaped(4, rows, dtype=f32)),
            ("h", shaped(rows, 2 * DK, dtype=f32)),
        ],
        "hhh",
        [
            pltpu.VMEM((1, rows), f32),
            pltpu.VMEM((seq_rows, 1, DK), f32),
            pltpu.VMEM((GRID_W, DK), f32),
            pltpu.VMEM((rows, 2 * DK), f32),
            sems((4,)),
        ],
        8,
        1000000,
        later_decay,
        jnp.asarray(rotary_tables(seq_rows))[:, None],
        jnp.asarray(rotary_tables(GRID_W)),
    )

    ctx = 2 * context.shape[0]
    lanes = 2 * DK + DK // 2
    send, normed, key_rows, value_rows = kernel_call(
        keys_kernel,
        [
            ("h", shaped(DV, lanes)),
            ("h", shaped(rows, width)),
            ("h", shaped(rows, DK)),
            ("h", shaped(rows, DV)),
        ],
        "hvvvvvvv" + "hvhhhvvvv",
        [
            pltpu.VMEM((lines, width), bf16),
            pltpu.VMEM(context.shape, bf16),
            pltpu.VMEM((rows, 2 * DK), f32),
            pltpu.VMEM((width, DK), bf16),
            pltpu.VMEM((width, DV), bf16),
            pltpu.VMEM((rows + ctx, width), bf16),
            pltpu.VMEM((rows, DK), bf16),
            pltpu.VMEM((rows, DV), bf16),
            pltpu.VMEM((DV, lanes), bf16),
            sems((9,)),
        ],
        32,
        2 * (rows + ctx) * width * (DK + DV),
        *own_rows,
        *other_rows,
        near,
        far,
        table,
        w_key,
        w_value,
        modulation,
        norm_gain[None],
        col,
        line,
    )
    parts = lax.all_to_all(send.reshape(count, DV // count, lanes), SP, 0, 0, tiled=True)
    queries, gates, inside = kernel_call(
        inside_kernel,
        [
            ("v", shaped(rows, DK)),
            ("h", shaped(rows, DV)),
            ("h", shaped(rows, DV, dtype=f32)),
        ],
        "hhhhhhvv",
        [
            pltpu.VMEM((rows, width), bf16),
            pltpu.VMEM((rows, DK), bf16),
            pltpu.VMEM((rows, DV), bf16),
            pltpu.VMEM((width, DK), bf16),
            pltpu.VMEM((width, DV), bf16),
            pltpu.VMEM((rows, 2 * DK), f32),
            pltpu.VMEM((rows, DV), bf16),
            pltpu.VMEM((rows, DV), f32),
            sems((9,)),
        ],
        32,
        2 * rows * width * (DK + DV),
        normed,
        key_rows,
        value_rows,
        w_query,
        w_gate,
        table,
        col,
        line,
    )
    (entering,) = kernel_call(
        scan_kernel,
        [("v", shaped(count, DV // count, 2 * DK))],
        "vv",
        [],
        16,
        10 * parts.size,
        parts,
        decays,
    )
    states = lax.all_to_all(entering, SP, 0, 0, tiled=True).reshape(DV, 2 * DK)
    partials = []
    for part in (1, 0):
        (partial,) = kernel_call(
            functools.partial(output_kernel, part),
            [("v", shaped(half, width))],
            "hhvvvvv",
            [pltpu.VMEM((half, DV), f32), pltpu.VMEM((half, DV), bf16), sems((2,))],
            32,
            2 * half * DV * width,
            inside,
            gates,
            queries,
            states,
            col,
            group_gain[None],
            w_output,
        )
        partials.append(partial)
    crossed = lax.ppermute(partials[0], "c", swap)
    tiles = kernel_call(
        pair_kernel,
        [("v", shaped(lines, width))] * x_size,
        "vv",
        [],
        8,
        half * width,
        partials[1],
        crossed,
    )
    projected = tiles[0].astype(f32)
    for d in (2, 1, 3):
        arrived = lax.ppermute(tiles[d], "x", ring(x_size, -d))
        projected = projected + arrived.astype(f32)
    gate = modulation[:, 0].reshape(-1)[2 * width :]
    return (latent.astype(f32) + gate * projected).astype(bf16)


def solution(mesh):
    torus = Mesh(mesh.devices.reshape(8, 4, 4, 2), ALL)
    in_specs = (
        P(ALL, None),
        P(SP, TP),
        P(SP, None),
        P(),
        P(SP, TP),
        P(),
        P(None, TP),
        P(None, TP),
        P(None, TP),
        P(None, TP),
        P(TP),
        P(TP, None),
    )
    return jax.shard_map(
        per_device, mesh=torus, in_specs=in_specs, out_specs=P(ALL, None), check_vma=False
    )
```

```python
import functools

import jax
import jax.numpy as jnp
import numpy as np
from jax import lax
from jax.experimental import pallas as pl
from jax.experimental.pallas import tpu as pltpu
from jax.sharding import Mesh
from jax.sharding import PartitionSpec as P

DK = 256
DV = 512
GRID_W = 64
CTX_LIFT = 4
SP = ("z", "y")
YZ = ("y", "z")
TP = ("x", "c")
ALL = ("z", "y", "x", "c")
f32 = jnp.float32
bf16 = jnp.bfloat16

epsilon = 1e-06
rotary_base = 10000.0
MIB = 1024 * 1024


def kernel_call(body, outs, ins, scratch, vmem, flops, *args):
    spaces = {"h": pltpu.MemorySpace.HBM, "v": pltpu.MemorySpace.VMEM}
    moved = sum(a.size * a.dtype.itemsize for a in args)
    args = [
        pltpu.with_memory_space_constraint(a, pltpu.HBM) if k == "h" else a
        for k, a in zip(ins, args)
    ]
    return pl.pallas_call(
        body,
        out_shape=tuple(pltpu.HBM(a.shape, a.dtype) if k == "h" else a for k, a in outs),
        in_specs=[pl.BlockSpec(memory_space=spaces[k]) for k in ins],
        out_specs=tuple(pl.BlockSpec(memory_space=spaces[k]) for k, _ in outs),
        scratch_shapes=scratch,
        compiler_params=pltpu.CompilerParams(vmem_limit_bytes=vmem * MIB),
        cost_estimate=pl.CostEstimate(flops=flops, bytes_accessed=moved, transcendentals=0),
    )(*args)


def started(source, target, sems, slot):
    copy = pltpu.make_async_copy(source, target, sems.at[slot])
    copy.start()
    return copy


def dot(a, b):
    return jnp.dot(a, b, preferred_element_type=f32)


def dot_t(a, b):
    return lax.dot_general(a, b, (((1,), (1,)), ((), ())), preferred_element_type=f32)


def turn(u, row_ref, column_ref):
    lanes = lax.broadcasted_iota(jnp.int32, u.shape, 1)
    swapped = jnp.where(lanes % 2 == 0, pltpu.roll(u, DK - 1, 1), pltpu.roll(u, 1, 1))
    chips, lines, pair = row_ref.shape[0], column_ref.shape[0] // 2, DK // 2
    turned = []
    for i in range(2 * chips):
        own, half, d = slice(i * lines, (i + 1) * lines), i // chips, i % chips
        column = column_ref[half * lines : (half + 1) * lines, :]
        low = u[own, :pair] * row_ref[d, :, :pair] + swapped[own, :pair] * row_ref[d, :, pair:]
        high = u[own, pair:] * column[:, :pair] + swapped[own, pair:] * column[:, pair:]
        turned.append(jnp.concatenate([low, high], axis=1))
    return jnp.concatenate(turned, axis=0)


def prepare_kernel(
    weights_hbm, condition_hbm, decay_hbm, out_ref, weights_ref, condition_ref, decay_ref, sems
):
    loads = [
        started(condition_hbm, condition_ref, sems, 0),
        started(decay_hbm, decay_ref, sems, 1),
        started(weights_hbm, weights_ref, sems, 2),
    ]
    size, width = weights_hbm.shape[0], condition_hbm.shape[1]
    seq = lax.axis_index("z") * lax.axis_size("y") + lax.axis_index("y")
    loads[0].wait()
    values = condition_ref[...].astype(f32)
    values = jnp.concatenate([values] * 4, axis=0)
    inputs = pltpu.roll(values, (width - seq * size) % width, 1)[0:2, 0:size]
    activated = (inputs / (1.0 + jnp.exp(-inputs))).astype(bf16)
    loads[1].wait()
    total = jnp.sum(decay_ref[...], axis=1, keepdims=True)
    loads[2].wait()
    part = dot(activated, weights_ref[...])
    cuts = part.shape[1] // 128
    packed = [part[i : i + 1, k * 128 : (k + 1) * 128] for i in range(2) for k in range(cuts)]
    spare = out_ref.shape[1] - len(packed)
    packed = jnp.concatenate(packed + [jnp.broadcast_to(total, (spare, 128))], axis=0)
    for r in range(out_ref.shape[0]):
        out_ref[r] = packed


def rotary_tables(count):
    pairs = DK // 4
    exponents = -np.arange(pairs, dtype=np.float32) / np.float32(pairs)
    inverse = np.repeat(np.float32(rotary_base) ** exponents, 2).astype(np.float32)
    angles = np.arange(count, dtype=np.float32)[:, None] * inverse
    sign = np.where(np.arange(DK // 2) % 2 == 0, -1.0, 1.0).astype(np.float32)
    return np.concatenate([np.cos(angles), np.sin(angles) * sign], axis=1)


def tables_kernel(
    lines, chips, decay_hbm, row_hbm, column_hbm,
    col_ref, line_ref, row_ref, column_ref,
    decay_ref, sems,
):
    rows = 2 * chips * lines
    seq = lax.axis_index("z") * lax.axis_size("y") + lax.axis_index("y")
    chip, core = lax.axis_index("x"), lax.axis_index("c")
    started(decay_hbm, decay_ref, sems, 0).wait()
    loads = []
    for h in range(2):
        column = pl.multiple_of(((h + core) % 2) * lines, lines)
        target = column_ref.at[h * lines : (h + 1) * lines]
        loads.append(started(column_hbm.at[pl.ds(column, lines)], target, sems, 1 + h))
    for d in range(chips):
        row = seq * chips + (chip - d + chips) % chips
        loads.append(started(row_hbm.at[row], row_ref.at[d], sems, 3 + d))

    def position(local):
        origin = (chip - (local // lines) % chips + chips) % chips
        return origin * GRID_W + ((local // (chips * lines) + core) % 2) * lines + local % lines

    down = lax.broadcasted_iota(jnp.int32, (rows, rows), 0)
    across = lax.broadcasted_iota(jnp.int32, (rows, rows), 1)
    place_col = position(lax.broadcasted_iota(jnp.int32, (rows, 1), 0))
    place_line = position(lax.broadcasted_iota(jnp.int32, (1, rows), 1))
    flat = decay_ref[...]
    total = jnp.sum(flat, axis=1, keepdims=True)
    flat_col = jnp.sum(jnp.where(down == across, flat, 0.0), axis=1, keepdims=True)
    upto = jnp.sum(jnp.where(across <= place_col, flat, 0.0), axis=1, keepdims=True)
    before = jnp.sum(jnp.where(across < place_col, flat, 0.0), axis=1, keepdims=True)
    col_ref[:, 0:1] = total - upto
    col_ref[:, 1:2] = before
    col_ref[:, 2:3] = upto
    col_ref[:, 3:4] = total - before
    col_ref[:, 4:5] = place_col.astype(f32)
    line_ref[0:1, :] = jnp.sum(jnp.where(down <= place_line, flat_col, 0.0), axis=0, keepdims=True)
    line_ref[1:2, :] = jnp.sum(jnp.where(down < place_line, flat_col, 0.0), axis=0, keepdims=True)
    line_ref[2:3, :] = place_line.astype(f32)
    odd = lax.axis_index("y") % 2
    line_ref[3:4, :] = jnp.full((1, rows), odd, jnp.int32).astype(f32)
    for copy in loads:
        copy.wait()


def gather_kernel(pieces_ref, out_ref, decay_ref):
    cuts = out_ref.shape[2] // 128
    summed = pieces_ref[0]
    for r in range(1, pieces_ref.shape[0]):
        summed = summed + pieces_ref[r]
    rows = [
        jnp.concatenate([summed[i * cuts + k : i * cuts + k + 1, :] for k in range(cuts)], axis=1)
        for i in range(2)
    ]
    for t in range(out_ref.shape[0]):
        out_ref[t] = jnp.concatenate(rows, axis=0)
    for r in range(pieces_ref.shape[0]):
        decay = jnp.exp(pieces_ref[r, 2 * cuts : 2 * cuts + 1, :])
        decay_ref[r : r + 1, :] = jnp.concatenate([decay, decay], axis=1)


def keys_kernel(*refs):
    pieces, refs = refs[:8], refs[8:]
    (
        near_hbm, wk_hbm, wv_hbm, far_ref, mod_ref, gain_ref, col_ref, line_ref, row_ref,
        column_ref,
        send_ref, normed_hbm, k_hbm, v_hbm,
        own_ref, near_ref, wk_ref, wv_ref, normed_ref, k_ref, v_ref, sems,
    ) = refs
    lines, width = pieces[0].shape
    rows = 8 * lines
    near = near_ref.shape[0]
    own = [started(pieces[0], own_ref, sems, 7), started(near_hbm, near_ref, sems, 8)]
    loads = [
        started(wv_hbm, wv_ref, sems, 0),
        started(wk_hbm, wk_ref, sems, 1),
    ]
    gain = gain_ref[...].astype(f32)
    tp = mod_ref.shape[0]

    def modulated(values, which):
        line = jnp.concatenate([mod_ref[t, which : which + 1, :] for t in range(tp)], axis=1)
        shift, scale = line[:, :width], line[:, width : 2 * width]
        wide = values.astype(f32)
        normal = wide * lax.rsqrt(jnp.mean(wide * wide, axis=-1, keepdims=True) + epsilon)
        return (normal * gain * (1.0 + scale) + shift).astype(bf16)

    for i, piece in enumerate(pieces[1:]):
        normed_ref[(i + 1) * lines : (i + 2) * lines, :] = modulated(piece[...], 0)
    normed_ref[rows + near :, :] = modulated(far_ref[...], 1)
    for copy in own:
        copy.wait()
    normed_ref[0:lines, :] = modulated(own_ref[...], 0)
    normed_ref[rows : rows + near, :] = modulated(near_ref[...], 1)
    stores = [started(normed_ref.at[0:rows], normed_hbm, sems, 2)]
    loads[0].wait()
    values = dot(normed_ref[...], wv_ref[...]).astype(bf16)
    v_ref[...] = values[:rows]
    stores.append(started(v_ref, v_hbm, sems, 3))
    loads[1].wait()
    keys = dot(normed_ref[...], wk_ref[...])
    key_rows = (turn(keys[:rows], row_ref, column_ref) * DK ** (-0.5)).astype(bf16)
    ctx_keys = (keys[rows:] * DK ** (-0.5)).astype(bf16)
    k_ref[...] = key_rows
    stores.append(started(k_ref, k_hbm, sems, 4))
    wide = key_rows.astype(f32)
    ahead = (wide * jnp.exp(col_ref[:, 0:1])).astype(bf16)
    behind = (wide * jnp.exp(col_ref[:, 1:2])).astype(bf16)
    turned = values.T
    send_ref[:, 0:DK] = dot(turned[:, :rows], ahead).astype(bf16)
    send_ref[:, DK : 2 * DK] = dot(turned[:, :rows], behind).astype(bf16)
    odd = line_ref[3:4, 0 : DK // 2] > 0.5
    own_keys = jnp.where(
        odd, ctx_keys[:, DK // 2 :].astype(f32), ctx_keys[:, : DK // 2].astype(f32)
    ).astype(bf16)
    send_ref[:, 2 * DK :] = dot(turned[:, rows:], own_keys).astype(bf16)
    for copy in stores:
        copy.wait()


def inside_kernel(
    normed_hbm, k_hbm, v_hbm, wq_hbm, wg_hbm, col_ref, line_ref, row_ref, column_ref,
    q_ref, g_hbm, y_hbm,
    normed_ref, k_ref, v_ref, wq_ref, wg_ref, g_ref, y_ref, sems,
):
    pairs = [
        (normed_hbm, normed_ref), (wq_hbm, wq_ref), (k_hbm, k_ref), (v_hbm, v_ref),
        (wg_hbm, wg_ref),
    ]
    loads = [started(a, b, sems, i) for i, (a, b) in enumerate(pairs)]
    for copy in loads[:3]:
        copy.wait()
    queries = turn(dot(normed_ref[...], wq_ref[...]), row_ref, column_ref).astype(bf16)
    q_ref[...] = queries
    scores = dot_t(queries, k_ref[...])
    here, there = col_ref[:, 4:5], line_ref[2:3, :]
    gaps = jnp.where(
        here >= there,
        col_ref[:, 2:3] - line_ref[0:1, :],
        line_ref[1:2, :] - col_ref[:, 1:2],
    )
    weights = jnp.exp(gaps) * jnp.where(here == there, 2.0, 1.0)
    loads[3].wait()
    y_ref[...] = dot((scores * weights).astype(bf16), v_ref[...])
    stores = [started(y_ref, y_hbm, sems, 7)]
    loads[4].wait()
    g_ref[...] = dot(normed_ref[...], wg_ref[...]).astype(bf16)
    stores.append(started(g_ref, g_hbm, sems, 8))
    for copy in stores:
        copy.wait()


def scan_kernel(parts_ref, decay_ref, out_ref):
    count, z_size = parts_ref.shape[0], lax.axis_size("z")
    y_size = count // z_size
    spot = [(r % y_size) * z_size + r // y_size for r in range(count)]
    lifts = []
    for parity in range(2):
        lift = parts_ref[spot[parity], :, 2 * DK :].astype(f32)
        for r in range(parity + 2, count, 2):
            lift = lift + parts_ref[spot[r], :, 2 * DK :].astype(f32)
        lifts.append(lift)
    ahead = behind = jnp.concatenate(lifts, axis=1) * float(CTX_LIFT)
    for r in range(count):
        s = count - 1 - r
        out_ref[spot[r], :, 0:DK] = ahead.astype(bf16)
        out_ref[spot[s], :, DK:] = behind.astype(bf16)
        ahead = decay_ref[r : r + 1, :] * ahead + parts_ref[spot[r], :, 0:DK].astype(f32)
        behind = (
            decay_ref[s : s + 1, :] * behind + parts_ref[spot[s], :, DK : 2 * DK].astype(f32)
        )


def output_kernel(
    part, y_hbm, g_hbm, q_ref, states_ref, col_ref, gain_ref, wo_ref, out_ref, y_ref, g_ref, sems
):
    half = out_ref.shape[0]
    own = slice(part * half, (part + 1) * half)
    loads = [started(y_hbm.at[own], y_ref, sems, 0), started(g_hbm.at[own], g_ref, sems, 1)]
    queries = q_ref[own, :]
    mixed = jnp.exp(col_ref[own, 2:3]) * dot_t(queries, states_ref[:, 0:DK]) + jnp.exp(
        col_ref[own, 3:4]
    ) * dot_t(queries, states_ref[:, DK:])
    loads[0].wait()
    mixed = mixed + y_ref[...]
    average = jnp.mean(mixed, axis=-1, keepdims=True)
    centred = mixed - average
    variance = jnp.mean(centred * centred, axis=-1, keepdims=True)
    loads[1].wait()
    gates = g_ref[...].astype(f32)
    attended = (
        gates * jax.nn.sigmoid(gates) * (centred * lax.rsqrt(variance + epsilon))
        * gain_ref[...].astype(f32)
    ).astype(bf16)
    out_ref[...] = dot(attended, wo_ref[...]).astype(bf16)


def pair_kernel(own_ref, crossed_ref, *out_refs):
    lines = out_refs[0].shape[0]
    for d, out_ref in enumerate(out_refs):
        own = slice(d * lines, (d + 1) * lines)
        out_ref[...] = (own_ref[own, :].astype(f32) + crossed_ref[own, :].astype(f32)).astype(bf16)


def ring(size, step):
    return [(i, (i + step) % size) for i in range(size)]


def shaped(*shape, dtype=bf16):
    return jax.ShapeDtypeStruct(shape, dtype)


def per_device(
    latent,
    log_decay,
    context,
    condition,
    w_modulate,
    norm_gain,
    w_query,
    w_key,
    w_value,
    w_gate,
    group_gain,
    w_output,
):
    lines, width = latent.shape
    x_size = lax.axis_size("x")
    half = lines * x_size
    rows = 2 * half
    swap = [(0, 1), (1, 0)]

    columns = w_modulate.shape[1]
    sems = pltpu.SemaphoreType.DMA
    count, tp = lax.axis_size(SP), lax.axis_size(TP)
    (packed,) = kernel_call(
        prepare_kernel,
        [("v", shaped(count, 16, 128, dtype=f32))],
        "hhh",
        [
            pltpu.VMEM(w_modulate.shape, bf16),
            pltpu.VMEM(condition.shape, bf16),
            pltpu.VMEM((1, rows), f32),
            sems((3,)),
        ],
        4,
        1000000,
        w_modulate,
        condition,
        log_decay.T,
    )
    pieces = lax.all_to_all(packed, SP, 0, 0, tiled=True)
    spread, decays = kernel_call(
        gather_kernel,
        [("v", shaped(tp, 2, columns, dtype=f32)), ("v", shaped(count, DK, dtype=f32))],
        "v",
        [],
        4,
        1000000,
        pieces,
    )
    modulation = lax.all_to_all(spread, TP, 0, 0, tiled=True)

    later, near, later_decay, _ = lax.optimization_barrier((latent, context, log_decay.T, packed))
    own_rows = [later] + [lax.ppermute(later, "x", ring(x_size, d)) for d in range(1, x_size)]
    other_rows = [lax.ppermute(piece, "c", swap) for piece in own_rows]
    far = lax.ppermute(near, "y", [(0, 1), (1, 0), (2, 3), (3, 2)])
    seq_rows = count * rows // GRID_W
    col, line, row_table, column_table = kernel_call(
        functools.partial(tables_kernel, lines, x_size),
        [
            ("v", shaped(rows, 8, dtype=f32)),
            ("v", shaped(4, rows, dtype=f32)),
            ("v", shaped(x_size, 1, DK, dtype=f32)),
            ("v", shaped(2 * lines, DK, dtype=f32)),
        ],
        "hhh",
        [pltpu.VMEM((1, rows), f32), sems((3 + x_size,))],
        8,
        1000000,
        later_decay,
        jnp.asarray(rotary_tables(seq_rows))[:, None],
        jnp.asarray(rotary_tables(GRID_W)),
    )

    ctx = 2 * context.shape[0]
    lanes = 2 * DK + DK // 2
    send, normed, key_rows, value_rows = kernel_call(
        keys_kernel,
        [
            ("v", shaped(DV, lanes)),
            ("h", shaped(rows, width)),
            ("h", shaped(rows, DK)),
            ("h", shaped(rows, DV)),
        ],
        "hvvvvvvv" + "hhhvvvvvvv",
        [
            pltpu.VMEM((lines, width), bf16),
            pltpu.VMEM(context.shape, bf16),
            pltpu.VMEM((width, DK), bf16),
            pltpu.VMEM((width, DV), bf16),
            pltpu.VMEM((rows + ctx, width), bf16),
            pltpu.VMEM((rows, DK), bf16),
            pltpu.VMEM((rows, DV), bf16),
            sems((9,)),
        ],
        32,
        2 * (rows + ctx) * width * (DK + DV),
        *own_rows,
        *other_rows,
        near,
        w_key,
        w_value,
        far,
        modulation,
        norm_gain[None],
        col,
        line,
        row_table,
        column_table,
    )
    parts = lax.all_to_all(send.reshape(count, DV // count, lanes), YZ, 0, 0, tiled=True)
    queries, gates, inside = kernel_call(
        inside_kernel,
        [
            ("v", shaped(rows, DK)),
            ("h", shaped(rows, DV)),
            ("h", shaped(rows, DV, dtype=f32)),
        ],
        "hhhhhvvvv",
        [
            pltpu.VMEM((rows, width), bf16),
            pltpu.VMEM((rows, DK), bf16),
            pltpu.VMEM((rows, DV), bf16),
            pltpu.VMEM((width, DK), bf16),
            pltpu.VMEM((width, DV), bf16),
            pltpu.VMEM((rows, DV), bf16),
            pltpu.VMEM((rows, DV), f32),
            sems((9,)),
        ],
        32,
        2 * rows * width * (DK + DV),
        normed,
        key_rows,
        value_rows,
        w_query,
        w_gate,
        col,
        line,
        row_table,
        column_table,
    )
    (entering,) = kernel_call(
        scan_kernel,
        [("v", shaped(count, DV // count, 2 * DK))],
        "vv",
        [],
        16,
        10 * parts.size,
        parts,
        decays,
    )
    states = lax.all_to_all(entering, YZ, 0, 0, tiled=True).reshape(DV, 2 * DK)
    partials = []
    for part in (1, 0):
        (partial,) = kernel_call(
            functools.partial(output_kernel, part),
            [("v", shaped(half, width))],
            "hhvvvvv",
            [pltpu.VMEM((half, DV), f32), pltpu.VMEM((half, DV), bf16), sems((2,))],
            32,
            2 * half * DV * width,
            inside,
            gates,
            queries,
            states,
            col,
            group_gain[None],
            w_output,
        )
        partials.append(partial)
    crossed = lax.ppermute(partials[0], "c", swap)
    tiles = kernel_call(
        pair_kernel,
        [("v", shaped(lines, width))] * x_size,
        "vv",
        [],
        8,
        half * width,
        partials[1],
        crossed,
    )
    projected = tiles[0].astype(f32)
    for d in (2, 1, 3):
        arrived = lax.ppermute(tiles[d], "x", ring(x_size, -d))
        projected = projected + arrived.astype(f32)
    gate = modulation[:, 0].reshape(-1)[2 * width :]
    return (latent.astype(f32) + gate * projected).astype(bf16)


def solution(mesh):
    torus = Mesh(mesh.devices.reshape(8, 4, 4, 2), ALL)
    in_specs = (
        P(ALL, None),
        P(SP, TP),
        P(SP, None),
        P(),
        P(SP, TP),
        P(),
        P(None, TP),
        P(None, TP),
        P(None, TP),
        P(None, TP),
        P(TP),
        P(TP, None),
    )
    return jax.shard_map(
        per_device, mesh=torus, in_specs=in_specs, out_specs=P(ALL, None), check_vma=False
    )
```

```python
import functools

import jax
import jax.numpy as jnp
import numpy as np
from jax import lax
from jax.experimental import pallas as pl
from jax.experimental.pallas import tpu as pltpu
from jax.sharding import Mesh
from jax.sharding import PartitionSpec as P

DK = 256
DV = 512
GRID_W = 64
CTX_LIFT = 4
SP = ("z", "y")
YZ = ("y", "z")
TP = ("x", "c")
ALL = ("z", "y", "x", "c")
f32 = jnp.float32
bf16 = jnp.bfloat16

epsilon = 1e-06
rotary_base = 10000.0
MIB = 1024 * 1024


def kernel_call(body, outs, ins, scratch, vmem, flops, *args):
    spaces = {"h": pltpu.MemorySpace.HBM, "v": pltpu.MemorySpace.VMEM}
    moved = sum(a.size * a.dtype.itemsize for a in args)
    args = [
        pltpu.with_memory_space_constraint(a, pltpu.HBM) if k == "h" else a
        for k, a in zip(ins, args)
    ]
    return pl.pallas_call(
        body,
        out_shape=tuple(pltpu.HBM(a.shape, a.dtype) if k == "h" else a for k, a in outs),
        in_specs=[pl.BlockSpec(memory_space=spaces[k]) for k in ins],
        out_specs=tuple(pl.BlockSpec(memory_space=spaces[k]) for k, _ in outs),
        scratch_shapes=scratch,
        compiler_params=pltpu.CompilerParams(vmem_limit_bytes=vmem * MIB),
        cost_estimate=pl.CostEstimate(flops=flops, bytes_accessed=moved, transcendentals=0),
    )(*args)


def started(source, target, sems, slot):
    copy = pltpu.make_async_copy(source, target, sems.at[slot])
    copy.start()
    return copy


def flat_gain(gain_ref):
    wide = gain_ref[...].astype(f32)
    return jnp.concatenate([wide[i : i + 1, :] for i in range(wide.shape[0])], axis=1)


def dot(a, b):
    return jnp.dot(a, b, preferred_element_type=f32)


def dot_t(a, b):
    return lax.dot_general(a, b, (((1,), (1,)), ((), ())), preferred_element_type=f32)


def turn(u, row_ref, column_ref):
    lanes = lax.broadcasted_iota(jnp.int32, u.shape, 1)
    swapped = jnp.where(lanes % 2 == 0, pltpu.roll(u, DK - 1, 1), pltpu.roll(u, 1, 1))
    chips, lines, pair = row_ref.shape[0], column_ref.shape[0] // 2, DK // 2
    turned = []
    for i in range(2 * chips):
        own, half, d = slice(i * lines, (i + 1) * lines), i // chips, i % chips
        column = column_ref[half * lines : (half + 1) * lines, :]
        low = u[own, :pair] * row_ref[d, :, :pair] + swapped[own, :pair] * row_ref[d, :, pair:]
        high = u[own, pair:] * column[:, :pair] + swapped[own, pair:] * column[:, pair:]
        turned.append(jnp.concatenate([low, high], axis=1))
    return jnp.concatenate(turned, axis=0)


def prepare_kernel(
    weights_hbm, condition_hbm, decay_hbm, out_ref, weights_ref, condition_ref, decay_ref, sems
):
    loads = [
        started(condition_hbm, condition_ref, sems, 0),
        started(decay_hbm, decay_ref, sems, 1),
        started(weights_hbm, weights_ref, sems, 2),
    ]
    size, width = weights_hbm.shape[0], condition_hbm.shape[1]
    seq = lax.axis_index("z") * lax.axis_size("y") + lax.axis_index("y")
    loads[0].wait()
    values = condition_ref[...].astype(f32)
    values = jnp.concatenate([values] * 4, axis=0)
    inputs = pltpu.roll(values, (width - seq * size) % width, 1)[0:2, 0:size]
    activated = (inputs / (1.0 + jnp.exp(-inputs))).astype(bf16)
    loads[1].wait()
    total = jnp.sum(decay_ref[...], axis=1, keepdims=True)
    loads[2].wait()
    part = dot(activated, weights_ref[...])
    cuts = part.shape[1] // 128
    packed = [part[i : i + 1, k * 128 : (k + 1) * 128] for i in range(2) for k in range(cuts)]
    rest = total
    while len(packed) < out_ref.shape[1]:
        term = rest.astype(bf16).astype(f32)
        packed.append(jnp.broadcast_to(term, (1, 128)))
        rest = rest - term
    packed = jnp.concatenate(packed, axis=0).astype(bf16)
    for r in range(out_ref.shape[0]):
        out_ref[r] = packed


def rotary_tables(count):
    pairs = DK // 4
    exponents = -np.arange(pairs, dtype=np.float32) / np.float32(pairs)
    inverse = np.repeat(np.float32(rotary_base) ** exponents, 2).astype(np.float32)
    angles = np.arange(count, dtype=np.float32)[:, None] * inverse
    sign = np.where(np.arange(DK // 2) % 2 == 0, -1.0, 1.0).astype(np.float32)
    return np.concatenate([np.cos(angles), np.sin(angles) * sign], axis=1)


def tables_kernel(
    lines, chips, decay_hbm, row_hbm, column_hbm,
    col_ref, line_ref, row_ref, column_ref,
    decay_ref, sems,
):
    rows = 2 * chips * lines
    seq = lax.axis_index("z") * lax.axis_size("y") + lax.axis_index("y")
    chip, core = lax.axis_index("x"), lax.axis_index("c")
    started(decay_hbm, decay_ref, sems, 0).wait()
    loads = []
    for h in range(2):
        column = pl.multiple_of(((h + core) % 2) * lines, lines)
        target = column_ref.at[h * lines : (h + 1) * lines]
        loads.append(started(column_hbm.at[pl.ds(column, lines)], target, sems, 1 + h))
    for d in range(chips):
        row = seq * chips + (chip - d + chips) % chips
        loads.append(started(row_hbm.at[row], row_ref.at[d], sems, 3 + d))

    def position(local):
        origin = (chip - (local // lines) % chips + chips) % chips
        return origin * GRID_W + ((local // (chips * lines) + core) % 2) * lines + local % lines

    down = lax.broadcasted_iota(jnp.int32, (rows, rows), 0)
    across = lax.broadcasted_iota(jnp.int32, (rows, rows), 1)
    place_col = position(lax.broadcasted_iota(jnp.int32, (rows, 1), 0))
    place_line = position(lax.broadcasted_iota(jnp.int32, (1, rows), 1))
    flat = decay_ref[...]
    total = jnp.sum(flat, axis=1, keepdims=True)
    flat_col = jnp.sum(jnp.where(down == across, flat, 0.0), axis=1, keepdims=True)
    upto = jnp.sum(jnp.where(across <= place_col, flat, 0.0), axis=1, keepdims=True)
    before = jnp.sum(jnp.where(across < place_col, flat, 0.0), axis=1, keepdims=True)
    col_ref[:, 0:1] = total - upto
    col_ref[:, 1:2] = before
    col_ref[:, 2:3] = upto
    col_ref[:, 3:4] = total - before
    col_ref[:, 4:5] = place_col.astype(f32)
    line_ref[0:1, :] = jnp.sum(jnp.where(down <= place_line, flat_col, 0.0), axis=0, keepdims=True)
    line_ref[1:2, :] = jnp.sum(jnp.where(down < place_line, flat_col, 0.0), axis=0, keepdims=True)
    line_ref[2:3, :] = place_line.astype(f32)
    odd = lax.axis_index("y") % 2
    line_ref[3:4, :] = jnp.full((1, rows), odd, jnp.int32).astype(f32)
    for copy in loads:
        copy.wait()


def gather_kernel(pieces_ref, out_ref, decay_ref):
    cuts = out_ref.shape[2] // 128
    pieces = [pieces_ref[r].astype(f32) for r in range(pieces_ref.shape[0])]
    summed = functools.reduce(jnp.add, pieces)
    rows = [
        jnp.concatenate([summed[i * cuts + k : i * cuts + k + 1, :] for k in range(cuts)], axis=1)
        for i in range(2)
    ]
    for t in range(out_ref.shape[0]):
        out_ref[t] = jnp.concatenate(rows, axis=0)
    for r, piece in enumerate(pieces):
        decay = jnp.exp(jnp.sum(piece[2 * cuts :, :], axis=0, keepdims=True))
        decay_ref[r : r + 1, :] = jnp.concatenate([decay, decay], axis=1)


def keys_kernel(*refs):
    pieces, refs = refs[:8], refs[8:]
    (
        near_hbm, wk_hbm, wv_hbm, gain_hbm, far_ref, mod_ref, col_ref, line_ref, row_ref,
        column_ref,
        send_ref, normed_hbm, k_ref, v_ref,
        own_ref, near_ref, gain_ref, wk_ref, wv_ref, normed_ref, sems,
    ) = refs
    lines, width = pieces[0].shape
    rows = 8 * lines
    near = near_ref.shape[0]
    load_gain = started(gain_hbm, gain_ref, sems, 5)
    own = [started(pieces[0], own_ref, sems, 7), started(near_hbm, near_ref, sems, 8)]
    loads = [
        started(wk_hbm, wk_ref, sems, 0),
        started(wv_hbm, wv_ref, sems, 1),
    ]
    load_gain.wait()
    gain = flat_gain(gain_ref)
    tp = mod_ref.shape[0]

    def modulated(values, which):
        line = jnp.concatenate([mod_ref[t, which : which + 1, :] for t in range(tp)], axis=1)
        shift, scale = line[:, :width], line[:, width : 2 * width]
        wide = values.astype(f32)
        normal = wide * lax.rsqrt(jnp.mean(wide * wide, axis=-1, keepdims=True) + epsilon)
        return (normal * gain * (1.0 + scale) + shift).astype(bf16)

    for i, piece in enumerate(pieces[1:]):
        normed_ref[(i + 1) * lines : (i + 2) * lines, :] = modulated(piece[...], 0)
    normed_ref[rows + near :, :] = modulated(far_ref[...], 1)
    for copy in own:
        copy.wait()
    normed_ref[0:lines, :] = modulated(own_ref[...], 0)
    normed_ref[rows : rows + near, :] = modulated(near_ref[...], 1)
    stores = [started(normed_ref.at[0:rows], normed_hbm, sems, 2)]
    loads[0].wait()
    keys = dot(normed_ref[...], wk_ref[...])
    loads[1].wait()
    values = dot(normed_ref[...], wv_ref[...]).astype(bf16)
    v_ref[...] = values[:rows]
    key_rows = (turn(keys[:rows], row_ref, column_ref) * DK ** (-0.5)).astype(bf16)
    ctx_keys = (keys[rows:] * DK ** (-0.5)).astype(bf16)
    k_ref[...] = key_rows
    wide = key_rows.astype(f32)
    ahead = (wide * jnp.exp(col_ref[:, 0:1])).astype(bf16)
    behind = (wide * jnp.exp(col_ref[:, 1:2])).astype(bf16)
    turned = values.T
    send_ref[:, 0:DK] = dot(turned[:, :rows], ahead).astype(bf16)
    send_ref[:, DK : 2 * DK] = dot(turned[:, :rows], behind).astype(bf16)
    odd = line_ref[3:4, 0 : DK // 2] > 0.5
    own_keys = jnp.where(
        odd, ctx_keys[:, DK // 2 :].astype(f32), ctx_keys[:, : DK // 2].astype(f32)
    ).astype(bf16)
    send_ref[:, 2 * DK :] = dot(turned[:, rows:], own_keys).astype(bf16)
    for copy in stores:
        copy.wait()


def inside_kernel(
    normed_hbm, wq_hbm, wg_hbm, k_ref, v_ref, col_ref, line_ref, row_ref, column_ref,
    q_ref, g_hbm, y_hbm,
    normed_ref, wq_ref, wg_ref, g_ref, y_ref, sems,
):
    pairs = [(normed_hbm, normed_ref), (wq_hbm, wq_ref), (wg_hbm, wg_ref)]
    loads = [started(a, b, sems, i) for i, (a, b) in enumerate(pairs)]
    for copy in loads[:2]:
        copy.wait()
    queries = turn(dot(normed_ref[...], wq_ref[...]), row_ref, column_ref).astype(bf16)
    q_ref[...] = queries
    scores = dot_t(queries, k_ref[...])
    here, there = col_ref[:, 4:5], line_ref[2:3, :]
    gaps = jnp.where(
        here >= there,
        col_ref[:, 2:3] - line_ref[0:1, :],
        line_ref[1:2, :] - col_ref[:, 1:2],
    )
    weights = jnp.exp(gaps) * jnp.where(here == there, 2.0, 1.0)
    y_ref[...] = dot((scores * weights).astype(bf16), v_ref[...])
    stores = [started(y_ref, y_hbm, sems, 3)]
    loads[2].wait()
    g_ref[...] = dot(normed_ref[...], wg_ref[...]).astype(bf16)
    stores.append(started(g_ref, g_hbm, sems, 4))
    for copy in stores:
        copy.wait()


def scan_kernel(parts_ref, decay_ref, out_ref):
    count, z_size = parts_ref.shape[0], lax.axis_size("z")
    y_size = count // z_size
    spot = [(r % y_size) * z_size + r // y_size for r in range(count)]
    lifts = []
    for parity in range(2):
        lift = parts_ref[spot[parity], :, 2 * DK :].astype(f32)
        for r in range(parity + 2, count, 2):
            lift = lift + parts_ref[spot[r], :, 2 * DK :].astype(f32)
        lifts.append(lift)
    ahead = behind = jnp.concatenate(lifts, axis=1) * float(CTX_LIFT)
    for r in range(count):
        s = count - 1 - r
        out_ref[spot[r], :, 0:DK] = ahead.astype(bf16)
        out_ref[spot[s], :, DK:] = behind.astype(bf16)
        ahead = decay_ref[r : r + 1, :] * ahead + parts_ref[spot[r], :, 0:DK].astype(f32)
        behind = (
            decay_ref[s : s + 1, :] * behind + parts_ref[spot[s], :, DK : 2 * DK].astype(f32)
        )


def output_kernel(
    part, y_hbm, g_hbm, q_ref, states_ref, col_ref, gain_ref, wo_ref, out_ref, y_ref, g_ref, sems
):
    half = out_ref.shape[0]
    own = slice(part * half, (part + 1) * half)
    loads = [started(y_hbm.at[own], y_ref, sems, 0), started(g_hbm.at[own], g_ref, sems, 1)]
    queries = q_ref[own, :]
    mixed = jnp.exp(col_ref[own, 2:3]) * dot_t(queries, states_ref[:, 0:DK]) + jnp.exp(
        col_ref[own, 3:4]
    ) * dot_t(queries, states_ref[:, DK:])
    loads[0].wait()
    mixed = mixed + y_ref[...]
    average = jnp.mean(mixed, axis=-1, keepdims=True)
    centred = mixed - average
    variance = jnp.mean(centred * centred, axis=-1, keepdims=True)
    loads[1].wait()
    gates = g_ref[...].astype(f32)
    attended = (
        gates * jax.nn.sigmoid(gates) * (centred * lax.rsqrt(variance + epsilon))
        * flat_gain(gain_ref)
    ).astype(bf16)
    out_ref[...] = dot(attended, wo_ref[...]).astype(bf16)


def pair_kernel(own_ref, crossed_ref, *out_refs):
    lines = out_refs[0].shape[0]
    for d, out_ref in enumerate(out_refs):
        own = slice(d * lines, (d + 1) * lines)
        out_ref[...] = (own_ref[own, :].astype(f32) + crossed_ref[own, :].astype(f32)).astype(bf16)


def ring(size, step):
    return [(i, (i + step) % size) for i in range(size)]


def shaped(*shape, dtype=bf16):
    return jax.ShapeDtypeStruct(shape, dtype)


def per_device(
    latent,
    log_decay,
    context,
    condition,
    w_modulate,
    norm_gain,
    w_query,
    w_key,
    w_value,
    w_gate,
    group_gain,
    w_output,
):
    lines, width = latent.shape
    x_size = lax.axis_size("x")
    half = lines * x_size
    rows = 2 * half
    swap = [(0, 1), (1, 0)]

    columns = w_modulate.shape[1]
    sems = pltpu.SemaphoreType.DMA
    count, tp = lax.axis_size(SP), lax.axis_size(TP)
    (packed,) = kernel_call(
        prepare_kernel,
        [("v", shaped(count, 16, 128))],
        "hhh",
        [
            pltpu.VMEM(w_modulate.shape, bf16),
            pltpu.VMEM(condition.shape, bf16),
            pltpu.VMEM((1, rows), f32),
            sems((3,)),
        ],
        4,
        1000000,
        w_modulate,
        condition,
        log_decay.T,
    )
    pieces = lax.all_to_all(packed, SP, 0, 0, tiled=True)
    spread, decays = kernel_call(
        gather_kernel,
        [("v", shaped(tp, 2, columns, dtype=f32)), ("v", shaped(count, DK, dtype=f32))],
        "v",
        [],
        4,
        1000000,
        pieces,
    )
    modulation = lax.all_to_all(spread, TP, 0, 0, tiled=True)

    later, near, later_decay, _ = lax.optimization_barrier((latent, context, log_decay.T, packed))
    own_rows = [later] + [lax.ppermute(later, "x", ring(x_size, d)) for d in range(1, x_size)]
    other_rows = [lax.ppermute(piece, "c", swap) for piece in own_rows]
    far = lax.ppermute(near, "y", [(0, 1), (1, 0), (2, 3), (3, 2)])
    seq_rows = count * rows // GRID_W
    col, line, row_table, column_table = kernel_call(
        functools.partial(tables_kernel, lines, x_size),
        [
            ("v", shaped(rows, 8, dtype=f32)),
            ("v", shaped(4, rows, dtype=f32)),
            ("v", shaped(x_size, 1, DK, dtype=f32)),
            ("v", shaped(2 * lines, DK, dtype=f32)),
        ],
        "hhh",
        [pltpu.VMEM((1, rows), f32), sems((3 + x_size,))],
        8,
        1000000,
        later_decay,
        jnp.asarray(rotary_tables(seq_rows))[:, None],
        jnp.asarray(rotary_tables(GRID_W)),
    )

    ctx = 2 * context.shape[0]
    lanes = 2 * DK + DK // 2
    send, normed, key_rows, value_rows = kernel_call(
        keys_kernel,
        [
            ("v", shaped(DV, lanes)),
            ("h", shaped(rows, width)),
            ("v", shaped(rows, DK)),
            ("v", shaped(rows, DV)),
        ],
        "hvvvvvvv" + "hhhhvvvvvv",
        [
            pltpu.VMEM((lines, width), bf16),
            pltpu.VMEM(context.shape, bf16),
            pltpu.VMEM((width // 128, 128), bf16),
            pltpu.VMEM((width, DK), bf16),
            pltpu.VMEM((width, DV), bf16),
            pltpu.VMEM((rows + ctx, width), bf16),
            sems((9,)),
        ],
        32,
        2 * (rows + ctx) * width * (DK + DV),
        *own_rows,
        *other_rows,
        near,
        w_key,
        w_value,
        norm_gain.reshape(-1, 128),
        far,
        modulation,
        col,
        line,
        row_table,
        column_table,
    )
    parts = lax.all_to_all(send.reshape(count, DV // count, lanes), YZ, 0, 0, tiled=True)
    queries, gates, inside = kernel_call(
        inside_kernel,
        [
            ("v", shaped(rows, DK)),
            ("h", shaped(rows, DV)),
            ("h", shaped(rows, DV, dtype=f32)),
        ],
        "hhhvvvvvv",
        [
            pltpu.VMEM((rows, width), bf16),
            pltpu.VMEM((width, DK), bf16),
            pltpu.VMEM((width, DV), bf16),
            pltpu.VMEM((rows, DV), bf16),
            pltpu.VMEM((rows, DV), f32),
            sems((5,)),
        ],
        32,
        2 * rows * width * (DK + DV),
        normed,
        w_query,
        w_gate,
        key_rows,
        value_rows,
        col,
        line,
        row_table,
        column_table,
    )
    (entering,) = kernel_call(
        scan_kernel,
        [("v", shaped(count, DV // count, 2 * DK))],
        "vv",
        [],
        16,
        10 * parts.size,
        parts,
        decays,
    )
    states = lax.all_to_all(entering, YZ, 0, 0, tiled=True).reshape(DV, 2 * DK)
    partials = []
    for part in (1, 0):
        (partial,) = kernel_call(
            functools.partial(output_kernel, part),
            [("v", shaped(half, width))],
            "hhvvvvv",
            [pltpu.VMEM((half, DV), f32), pltpu.VMEM((half, DV), bf16), sems((2,))],
            32,
            2 * half * DV * width,
            inside,
            gates,
            queries,
            states,
            col,
            group_gain.reshape(-1, 128),
            w_output,
        )
        partials.append(partial)
    crossed = lax.ppermute(partials[0], "c", swap)
    tiles = kernel_call(
        pair_kernel,
        [("v", shaped(lines, width))] * x_size,
        "vv",
        [],
        8,
        half * width,
        partials[1],
        crossed,
    )
    projected = tiles[0].astype(f32)
    for d in (2, 1, 3):
        arrived = lax.ppermute(tiles[d], "x", ring(x_size, -d))
        projected = projected + arrived.astype(f32)
    gate = modulation[:, 0].reshape(-1)[2 * width :]
    return (latent.astype(f32) + gate * projected).astype(bf16)


def solution(mesh):
    torus = Mesh(mesh.devices.reshape(8, 4, 4, 2), ALL)
    in_specs = (
        P(ALL, None),
        P(SP, TP),
        P(SP, None),
        P(),
        P(SP, TP),
        P(),
        P(None, TP),
        P(None, TP),
        P(None, TP),
        P(None, TP),
        P(TP),
        P(TP, None),
    )
    return jax.shard_map(
        per_device, mesh=torus, in_specs=in_specs, out_specs=P(ALL, None), check_vma=False
    )
```

```python
import functools

import jax
import jax.numpy as jnp
import numpy as np
from jax import lax
from jax.experimental import pallas as pl
from jax.experimental.pallas import tpu as pltpu
from jax.sharding import Mesh
from jax.sharding import PartitionSpec as P

DK = 256
DV = 512
GRID_W = 64
CTX_LIFT = 4
SP = ("z", "y")
YZ = ("y", "z")
TP = ("x", "c")
ALL = ("z", "y", "x", "c")
f32 = jnp.float32
bf16 = jnp.bfloat16

epsilon = 1e-06
rotary_base = 10000.0
MIB = 1024 * 1024


def kernel_call(body, outs, ins, scratch, vmem, flops, *args):
    spaces = {"h": pltpu.MemorySpace.HBM, "v": pltpu.MemorySpace.VMEM}
    moved = sum(a.size * a.dtype.itemsize for a in args)
    args = [
        pltpu.with_memory_space_constraint(a, pltpu.HBM) if k == "h" else a
        for k, a in zip(ins, args)
    ]
    return pl.pallas_call(
        body,
        out_shape=tuple(pltpu.HBM(a.shape, a.dtype) if k == "h" else a for k, a in outs),
        in_specs=[pl.BlockSpec(memory_space=spaces[k]) for k in ins],
        out_specs=tuple(pl.BlockSpec(memory_space=spaces[k]) for k, _ in outs),
        scratch_shapes=scratch,
        compiler_params=pltpu.CompilerParams(vmem_limit_bytes=vmem * MIB),
        cost_estimate=pl.CostEstimate(flops=flops, bytes_accessed=moved, transcendentals=0),
    )(*args)


def started(source, target, sems, slot):
    copy = pltpu.make_async_copy(source, target, sems.at[slot])
    copy.start()
    return copy


def flat_gain(gain_ref):
    wide = gain_ref[...].astype(f32)
    return jnp.concatenate([wide[i : i + 1, :] for i in range(wide.shape[0])], axis=1)


def dot(a, b):
    return jnp.dot(a, b, preferred_element_type=f32)


def dot_t(a, b):
    return lax.dot_general(a, b, (((1,), (1,)), ((), ())), preferred_element_type=f32)


def turn(u, row_ref, column_ref):
    lanes = lax.broadcasted_iota(jnp.int32, u.shape, 1)
    swapped = jnp.where(lanes % 2 == 0, pltpu.roll(u, DK - 1, 1), pltpu.roll(u, 1, 1))
    chips, lines, pair = row_ref.shape[0], column_ref.shape[0] // 2, DK // 2
    turned = []
    for i in range(2 * chips):
        own, half, d = slice(i * lines, (i + 1) * lines), i // chips, i % chips
        column = column_ref[half * lines : (half + 1) * lines, :]
        low = u[own, :pair] * row_ref[d, :, :pair] + swapped[own, :pair] * row_ref[d, :, pair:]
        high = u[own, pair:] * column[:, :pair] + swapped[own, pair:] * column[:, pair:]
        turned.append(jnp.concatenate([low, high], axis=1))
    return jnp.concatenate(turned, axis=0)


def prepare_kernel(
    lines, weights_hbm, condition_hbm, decay_hbm, row_hbm, column_hbm,
    out_ref, decay_ref, row_ref, column_ref,
    weights_ref, condition_ref, sems,
):
    size, width = weights_hbm.shape[0], condition_hbm.shape[1]
    seq = lax.axis_index("z") * lax.axis_size("y") + lax.axis_index("y")
    chip, core = lax.axis_index("x"), lax.axis_index("c")
    chips = row_ref.shape[0]
    loads = [
        started(condition_hbm, condition_ref, sems, 0),
        started(decay_hbm, decay_ref, sems, 1),
        started(weights_hbm, weights_ref, sems, 2),
    ]
    for h in range(2):
        column = pl.multiple_of(((h + core) % 2) * lines, lines)
        target = column_ref.at[h * lines : (h + 1) * lines]
        loads.append(started(column_hbm.at[pl.ds(column, lines)], target, sems, 3 + h))
    for d in range(chips):
        row = seq * chips + (chip - d + chips) % chips
        loads.append(started(row_hbm.at[row], row_ref.at[d], sems, 5 + d))
    loads[0].wait()
    values = condition_ref[...].astype(f32)
    values = jnp.concatenate([values] * 4, axis=0)
    inputs = pltpu.roll(values, (width - seq * size) % width, 1)[0:2, 0:size]
    activated = (inputs / (1.0 + jnp.exp(-inputs))).astype(bf16)
    loads[1].wait()
    total = jnp.sum(decay_ref[...], axis=1, keepdims=True)
    loads[2].wait()
    part = dot(activated, weights_ref[...])
    cuts = part.shape[1] // 128
    packed = [part[i : i + 1, k * 128 : (k + 1) * 128] for i in range(2) for k in range(cuts)]
    rest = total
    while len(packed) < out_ref.shape[1]:
        term = rest.astype(bf16).astype(f32)
        packed.append(jnp.broadcast_to(term, (1, 128)))
        rest = rest - term
    packed = jnp.concatenate(packed, axis=0).astype(bf16)
    for r in range(out_ref.shape[0]):
        out_ref[r] = packed
    for copy in loads[3:]:
        copy.wait()


def rotary_tables(count):
    pairs = DK // 4
    exponents = -np.arange(pairs, dtype=np.float32) / np.float32(pairs)
    inverse = np.repeat(np.float32(rotary_base) ** exponents, 2).astype(np.float32)
    angles = np.arange(count, dtype=np.float32)[:, None] * inverse
    sign = np.where(np.arange(DK // 2) % 2 == 0, -1.0, 1.0).astype(np.float32)
    return np.concatenate([np.cos(angles), np.sin(angles) * sign], axis=1)


def tables_kernel(lines, chips, decay_ref, col_ref, line_ref):
    rows = 2 * chips * lines
    chip, core = lax.axis_index("x"), lax.axis_index("c")

    def position(local):
        origin = (chip - (local // lines) % chips + chips) % chips
        return origin * GRID_W + ((local // (chips * lines) + core) % 2) * lines + local % lines

    down = lax.broadcasted_iota(jnp.int32, (rows, rows), 0)
    across = lax.broadcasted_iota(jnp.int32, (rows, rows), 1)
    place_col = position(lax.broadcasted_iota(jnp.int32, (rows, 1), 0))
    place_line = position(lax.broadcasted_iota(jnp.int32, (1, rows), 1))
    flat = decay_ref[...]
    total = jnp.sum(flat, axis=1, keepdims=True)
    flat_col = jnp.sum(jnp.where(down == across, flat, 0.0), axis=1, keepdims=True)
    upto = jnp.sum(jnp.where(across <= place_col, flat, 0.0), axis=1, keepdims=True)
    before = jnp.sum(jnp.where(across < place_col, flat, 0.0), axis=1, keepdims=True)
    col_ref[:, 0:1] = total - upto
    col_ref[:, 1:2] = before
    col_ref[:, 2:3] = upto
    col_ref[:, 3:4] = total - before
    col_ref[:, 4:5] = place_col.astype(f32)
    line_ref[0:1, :] = jnp.sum(jnp.where(down <= place_line, flat_col, 0.0), axis=0, keepdims=True)
    line_ref[1:2, :] = jnp.sum(jnp.where(down < place_line, flat_col, 0.0), axis=0, keepdims=True)
    line_ref[2:3, :] = place_line.astype(f32)
    odd = lax.axis_index("y") % 2
    line_ref[3:4, :] = jnp.full((1, rows), odd, jnp.int32).astype(f32)


def gather_kernel(pieces_ref, out_ref, decay_ref):
    cuts = out_ref.shape[2] // 128
    pieces = [pieces_ref[r].astype(f32) for r in range(pieces_ref.shape[0])]
    summed = functools.reduce(jnp.add, pieces)
    rows = [
        jnp.concatenate([summed[i * cuts + k : i * cuts + k + 1, :] for k in range(cuts)], axis=1)
        for i in range(2)
    ]
    for t in range(out_ref.shape[0]):
        out_ref[t] = jnp.concatenate(rows, axis=0)
    for r, piece in enumerate(pieces):
        decay = jnp.exp(jnp.sum(piece[2 * cuts :, :], axis=0, keepdims=True))
        decay_ref[r : r + 1, :] = jnp.concatenate([decay, decay], axis=1)


def keys_kernel(*refs):
    pieces, refs = refs[:8], refs[8:]
    (
        near_hbm, wk_hbm, wv_hbm, gain_hbm, far_ref, mod_ref, col_ref, line_ref, row_ref,
        column_ref,
        send_ref, normed_hbm, k_ref, v_ref,
        own_ref, near_ref, gain_ref, wk_ref, wv_ref, normed_ref, sems,
    ) = refs
    lines, width = pieces[0].shape
    rows = 8 * lines
    near = near_ref.shape[0]
    load_gain = started(gain_hbm, gain_ref, sems, 5)
    own = [started(pieces[0], own_ref, sems, 7), started(near_hbm, near_ref, sems, 8)]
    loads = [started(wk_hbm, wk_ref, sems, 0), started(wv_hbm, wv_ref, sems, 1)]
    load_gain.wait()
    gain = flat_gain(gain_ref)
    tp = mod_ref.shape[0]

    def modulated(values, which):
        line = jnp.concatenate([mod_ref[t, which : which + 1, :] for t in range(tp)], axis=1)
        shift, scale = line[:, :width], line[:, width : 2 * width]
        wide = values.astype(f32)
        normal = wide * lax.rsqrt(jnp.mean(wide * wide, axis=-1, keepdims=True) + epsilon)
        return (normal * gain * (1.0 + scale) + shift).astype(bf16)

    for i, piece in enumerate(pieces[1:]):
        normed_ref[(i + 1) * lines : (i + 2) * lines, :] = modulated(piece[...], 0)
    normed_ref[rows + near :, :] = modulated(far_ref[...], 1)
    for copy in own:
        copy.wait()
    normed_ref[0:lines, :] = modulated(own_ref[...], 0)
    normed_ref[rows : rows + near, :] = modulated(near_ref[...], 1)
    stores = [started(normed_ref.at[0:rows], normed_hbm, sems, 2)]
    loads[0].wait()
    keys = dot(normed_ref[...], wk_ref[...])
    loads[1].wait()
    values = dot(normed_ref[...], wv_ref[...]).astype(bf16)
    v_ref[...] = values[:rows]
    key_rows = (turn(keys[:rows], row_ref, column_ref) * DK ** (-0.5)).astype(bf16)
    ctx_keys = (keys[rows:] * DK ** (-0.5)).astype(bf16)
    k_ref[...] = key_rows
    wide = key_rows.astype(f32)
    ahead = (wide * jnp.exp(col_ref[:, 0:1])).astype(bf16)
    behind = (wide * jnp.exp(col_ref[:, 1:2])).astype(bf16)
    turned = values.T
    send_ref[:, 0:DK] = dot(turned[:, :rows], ahead).astype(bf16)
    send_ref[:, DK : 2 * DK] = dot(turned[:, :rows], behind).astype(bf16)
    odd = line_ref[3:4, 0 : DK // 2] > 0.5
    own_keys = jnp.where(
        odd, ctx_keys[:, DK // 2 :].astype(f32), ctx_keys[:, : DK // 2].astype(f32)
    ).astype(bf16)
    send_ref[:, 2 * DK :] = dot(turned[:, rows:], own_keys).astype(bf16)
    for copy in stores:
        copy.wait()


def inside_kernel(
    normed_hbm, wq_hbm, wg_hbm, k_ref, v_ref, col_ref, line_ref, row_ref, column_ref,
    q_ref, g_ref, y_ref,
    normed_ref, wq_ref, wg_ref, sems,
):
    pairs = [(normed_hbm, normed_ref), (wq_hbm, wq_ref), (wg_hbm, wg_ref)]
    loads = [started(a, b, sems, i) for i, (a, b) in enumerate(pairs)]
    for copy in loads[:2]:
        copy.wait()
    queries = turn(dot(normed_ref[...], wq_ref[...]), row_ref, column_ref).astype(bf16)
    q_ref[...] = queries
    scores = dot_t(queries, k_ref[...])
    here, there = col_ref[:, 4:5], line_ref[2:3, :]
    gaps = jnp.where(
        here >= there,
        col_ref[:, 2:3] - line_ref[0:1, :],
        line_ref[1:2, :] - col_ref[:, 1:2],
    )
    weights = jnp.exp(gaps) * jnp.where(here == there, 2.0, 1.0)
    y_ref[...] = dot((scores * weights).astype(bf16), v_ref[...]).astype(bf16)
    loads[2].wait()
    g_ref[...] = dot(normed_ref[...], wg_ref[...]).astype(bf16)


def scan_kernel(parts_ref, decay_ref, out_ref):
    count, z_size = parts_ref.shape[0], lax.axis_size("z")
    y_size = count // z_size
    spot = [(r % y_size) * z_size + r // y_size for r in range(count)]
    lifts = []
    for parity in range(2):
        lift = parts_ref[spot[parity], :, 2 * DK :].astype(f32)
        for r in range(parity + 2, count, 2):
            lift = lift + parts_ref[spot[r], :, 2 * DK :].astype(f32)
        lifts.append(lift)
    ahead = behind = jnp.concatenate(lifts, axis=1) * float(CTX_LIFT)
    for r in range(count):
        s = count - 1 - r
        out_ref[spot[r], :, 0:DK] = ahead.astype(bf16)
        out_ref[spot[s], :, DK:] = behind.astype(bf16)
        ahead = decay_ref[r : r + 1, :] * ahead + parts_ref[spot[r], :, 0:DK].astype(f32)
        behind = (
            decay_ref[s : s + 1, :] * behind + parts_ref[spot[s], :, DK : 2 * DK].astype(f32)
        )


def output_kernel(
    part, y_ref, g_ref, q_ref, states_ref, col_ref, gain_ref, wo_ref, out_ref
):
    half = out_ref.shape[0]
    own = slice(part * half, (part + 1) * half)
    queries = q_ref[own, :]
    mixed = (
        y_ref[own, :].astype(f32)
        + jnp.exp(col_ref[own, 2:3]) * dot_t(queries, states_ref[:, 0:DK])
        + jnp.exp(col_ref[own, 3:4]) * dot_t(queries, states_ref[:, DK:])
    )
    average = jnp.mean(mixed, axis=-1, keepdims=True)
    centred = mixed - average
    variance = jnp.mean(centred * centred, axis=-1, keepdims=True)
    gates = g_ref[own, :].astype(f32)
    attended = (
        gates * jax.nn.sigmoid(gates) * (centred * lax.rsqrt(variance + epsilon))
        * flat_gain(gain_ref)
    ).astype(bf16)
    out_ref[...] = dot(attended, wo_ref[...]).astype(bf16)


def pair_kernel(own_ref, crossed_ref, *out_refs):
    lines = out_refs[0].shape[0]
    for d, out_ref in enumerate(out_refs):
        own = slice(d * lines, (d + 1) * lines)
        out_ref[...] = (own_ref[own, :].astype(f32) + crossed_ref[own, :].astype(f32)).astype(bf16)


def ring(size, step):
    return [(i, (i + step) % size) for i in range(size)]


def shaped(*shape, dtype=bf16):
    return jax.ShapeDtypeStruct(shape, dtype)


def per_device(
    latent,
    log_decay,
    context,
    condition,
    w_modulate,
    norm_gain,
    w_query,
    w_key,
    w_value,
    w_gate,
    group_gain,
    w_output,
):
    lines, width = latent.shape
    x_size = lax.axis_size("x")
    half = lines * x_size
    rows = 2 * half
    swap = [(0, 1), (1, 0)]

    columns = w_modulate.shape[1]
    sems = pltpu.SemaphoreType.DMA
    count, tp = lax.axis_size(SP), lax.axis_size(TP)
    packed, decay_row, row_table, column_table = kernel_call(
        functools.partial(prepare_kernel, lines),
        [
            ("v", shaped(count, 16, 128)),
            ("v", shaped(1, rows, dtype=f32)),
            ("v", shaped(x_size, 1, DK, dtype=f32)),
            ("v", shaped(2 * lines, DK, dtype=f32)),
        ],
        "hhhhh",
        [
            pltpu.VMEM(w_modulate.shape, bf16),
            pltpu.VMEM(condition.shape, bf16),
            sems((5 + x_size,)),
        ],
        4,
        1000000,
        w_modulate,
        condition,
        log_decay.T,
        jnp.asarray(rotary_tables(count * rows // GRID_W))[:, None],
        jnp.asarray(rotary_tables(GRID_W)),
    )
    pieces = lax.all_to_all(packed, SP, 0, 0, tiled=True)
    spread, decays = kernel_call(
        gather_kernel,
        [("v", shaped(tp, 2, columns, dtype=f32)), ("v", shaped(count, DK, dtype=f32))],
        "v",
        [],
        4,
        1000000,
        pieces,
    )
    modulation = lax.all_to_all(spread, TP, 0, 0, tiled=True)

    later, near, _ = lax.optimization_barrier((latent, context, packed))
    own_rows = [later] + [lax.ppermute(later, "x", ring(x_size, d)) for d in range(1, x_size)]
    other_rows = [lax.ppermute(piece, "c", swap) for piece in own_rows]
    far = lax.ppermute(near, "y", [(0, 1), (1, 0), (2, 3), (3, 2)])
    col, line = kernel_call(
        functools.partial(tables_kernel, lines, x_size),
        [("v", shaped(rows, 8, dtype=f32)), ("v", shaped(4, rows, dtype=f32))],
        "v",
        [],
        8,
        1000000,
        decay_row,
    )

    ctx = 2 * context.shape[0]
    lanes = 2 * DK + DK // 2
    send, normed, key_rows, value_rows = kernel_call(
        keys_kernel,
        [
            ("v", shaped(DV, lanes)),
            ("h", shaped(rows, width)),
            ("v", shaped(rows, DK)),
            ("v", shaped(rows, DV)),
        ],
        "hvvvvvvv" + "hhhhvvvvvv",
        [
            pltpu.VMEM((lines, width), bf16),
            pltpu.VMEM(context.shape, bf16),
            pltpu.VMEM((width // 128, 128), bf16),
            pltpu.VMEM((width, DK), bf16),
            pltpu.VMEM((width, DV), bf16),
            pltpu.VMEM((rows + ctx, width), bf16),
            sems((9,)),
        ],
        32,
        2 * (rows + ctx) * width * (DK + DV),
        *own_rows,
        *other_rows,
        near,
        w_key,
        w_value,
        norm_gain.reshape(-1, 128),
        far,
        modulation,
        col,
        line,
        row_table,
        column_table,
    )
    parts = lax.all_to_all(send.reshape(count, DV // count, lanes), YZ, 0, 0, tiled=True)
    queries, gates, inside = kernel_call(
        inside_kernel,
        [
            ("v", shaped(rows, DK)),
            ("v", shaped(rows, DV)),
            ("v", shaped(rows, DV)),
        ],
        "hhhvvvvvv",
        [
            pltpu.VMEM((rows, width), bf16),
            pltpu.VMEM((width, DK), bf16),
            pltpu.VMEM((width, DV), bf16),
            sems((3,)),
        ],
        32,
        2 * rows * width * (DK + DV),
        normed,
        w_query,
        w_gate,
        key_rows,
        value_rows,
        col,
        line,
        row_table,
        column_table,
    )
    (entering,) = kernel_call(
        scan_kernel,
        [("v", shaped(count, DV // count, 2 * DK))],
        "vv",
        [],
        16,
        10 * parts.size,
        parts,
        decays,
    )
    states = lax.all_to_all(entering, YZ, 0, 0, tiled=True).reshape(DV, 2 * DK)
    partials = []
    for part in (1, 0):
        (partial,) = kernel_call(
            functools.partial(output_kernel, part),
            [("v", shaped(half, width))],
            "vvvvvvv",
            [],
            32,
            2 * half * DV * width,
            inside,
            gates,
            queries,
            states,
            col,
            group_gain.reshape(-1, 128),
            w_output,
        )
        partials.append(partial)
    crossed = lax.ppermute(partials[0], "c", swap)
    tiles = kernel_call(
        pair_kernel,
        [("v", shaped(lines, width))] * x_size,
        "vv",
        [],
        8,
        half * width,
        partials[1],
        crossed,
    )
    projected = tiles[0].astype(f32)
    for d in (2, 1, 3):
        arrived = lax.ppermute(tiles[d], "x", ring(x_size, -d))
        projected = projected + arrived.astype(f32)
    gate = modulation[:, 0].reshape(-1)[2 * width :]
    return (latent.astype(f32) + gate * projected).astype(bf16)


def solution(mesh):
    torus = Mesh(mesh.devices.reshape(8, 4, 4, 2), ALL)
    in_specs = (
        P(ALL, None),
        P(SP, TP),
        P(SP, None),
        P(),
        P(SP, TP),
        P(),
        P(None, TP),
        P(None, TP),
        P(None, TP),
        P(None, TP),
        P(TP),
        P(TP, None),
    )
    return jax.shard_map(
        per_device, mesh=torus, in_specs=in_specs, out_specs=P(ALL, None), check_vma=False
    )
```

```python
import functools

import jax
import jax.numpy as jnp
import numpy as np
from jax import lax
from jax.experimental import pallas as pl
from jax.experimental.pallas import tpu as pltpu
from jax.sharding import Mesh
from jax.sharding import PartitionSpec as P

DK = 256
DV = 512
GRID_W = 64
CTX_LIFT = 4
SP = ("z", "y")
YZ = ("y", "z")
TP = ("x", "c")
ALL = ("z", "y", "x", "c")
f32 = jnp.float32
bf16 = jnp.bfloat16

epsilon = 1e-06
rotary_base = 10000.0
MIB = 1024 * 1024


def kernel_call(body, outs, ins, scratch, vmem, flops, *args):
    spaces = {"h": pltpu.MemorySpace.HBM, "v": pltpu.MemorySpace.VMEM}
    moved = sum(a.size * a.dtype.itemsize for a in args)
    args = [
        pltpu.with_memory_space_constraint(a, pltpu.HBM) if k == "h" else a
        for k, a in zip(ins, args)
    ]
    return pl.pallas_call(
        body,
        out_shape=tuple(pltpu.HBM(a.shape, a.dtype) if k == "h" else a for k, a in outs),
        in_specs=[pl.BlockSpec(memory_space=spaces[k]) for k in ins],
        out_specs=tuple(pl.BlockSpec(memory_space=spaces[k]) for k, _ in outs),
        scratch_shapes=scratch,
        compiler_params=pltpu.CompilerParams(vmem_limit_bytes=vmem * MIB),
        cost_estimate=pl.CostEstimate(flops=flops, bytes_accessed=moved, transcendentals=0),
    )(*args)


def started(source, target, sems, slot):
    copy = pltpu.make_async_copy(source, target, sems.at[slot])
    copy.start()
    return copy


def flat_gain(gain_ref):
    wide = gain_ref[...].astype(f32)
    return jnp.concatenate([wide[i : i + 1, :] for i in range(wide.shape[0])], axis=1)


def dot(a, b):
    return jnp.dot(a, b, preferred_element_type=f32)


def dot_t(a, b):
    return lax.dot_general(a, b, (((1,), (1,)), ((), ())), preferred_element_type=f32)


def turn(u, row_ref, column_ref):
    lanes = lax.broadcasted_iota(jnp.int32, u.shape, 1)
    swapped = jnp.where(lanes % 2 == 0, pltpu.roll(u, DK - 1, 1), pltpu.roll(u, 1, 1))
    chips, lines, pair = row_ref.shape[0], column_ref.shape[0] // 2, DK // 2
    turned = []
    for i in range(2 * chips):
        own, half, d = slice(i * lines, (i + 1) * lines), i // chips, i % chips
        column = column_ref[half * lines : (half + 1) * lines, :]
        low = u[own, :pair] * row_ref[d, :, :pair] + swapped[own, :pair] * row_ref[d, :, pair:]
        high = u[own, pair:] * column[:, :pair] + swapped[own, pair:] * column[:, pair:]
        turned.append(jnp.concatenate([low, high], axis=1))
    return jnp.concatenate(turned, axis=0)


def prepare_kernel(
    lines, weights_hbm, condition_hbm, decay_hbm, row_hbm, column_hbm, gain_hbm, wk_hbm, wv_hbm,
    out_ref, decay_ref, row_ref, column_ref, gain_ref, wk_ref, wv_ref,
    weights_ref, condition_ref, sems,
):
    size, width = weights_hbm.shape[0], condition_hbm.shape[1]
    seq = lax.axis_index("z") * lax.axis_size("y") + lax.axis_index("y")
    chip, core = lax.axis_index("x"), lax.axis_index("c")
    chips = row_ref.shape[0]
    loads = [
        started(condition_hbm, condition_ref, sems, 0),
        started(decay_hbm, decay_ref, sems, 1),
        started(weights_hbm, weights_ref, sems, 2),
    ]
    for h in range(2):
        column = pl.multiple_of(((h + core) % 2) * lines, lines)
        target = column_ref.at[h * lines : (h + 1) * lines]
        loads.append(started(column_hbm.at[pl.ds(column, lines)], target, sems, 3 + h))
    for d in range(chips):
        row = seq * chips + (chip - d + chips) % chips
        loads.append(started(row_hbm.at[row], row_ref.at[d], sems, 5 + d))
    loads.append(started(gain_hbm, gain_ref, sems, 5 + chips))
    loads.append(started(wk_hbm, wk_ref, sems, 6 + chips))
    loads.append(started(wv_hbm.at[:, : wv_ref.shape[1]], wv_ref, sems, 7 + chips))
    loads[0].wait()
    values = condition_ref[...].astype(f32)
    values = jnp.concatenate([values] * 4, axis=0)
    inputs = pltpu.roll(values, (width - seq * size) % width, 1)[0:2, 0:size]
    activated = (inputs / (1.0 + jnp.exp(-inputs))).astype(bf16)
    loads[1].wait()
    total = jnp.sum(decay_ref[...], axis=1, keepdims=True)
    loads[2].wait()
    part = dot(activated, weights_ref[...])
    cuts = part.shape[1] // 128
    packed = [part[i : i + 1, k * 128 : (k + 1) * 128] for i in range(2) for k in range(cuts)]
    rest = total
    while len(packed) < out_ref.shape[1]:
        term = rest.astype(bf16).astype(f32)
        packed.append(jnp.broadcast_to(term, (1, 128)))
        rest = rest - term
    packed = jnp.concatenate(packed, axis=0).astype(bf16)
    for r in range(out_ref.shape[0]):
        out_ref[r] = packed
    for copy in loads[3:]:
        copy.wait()


def rotary_tables(count):
    pairs = DK // 4
    exponents = -np.arange(pairs, dtype=np.float32) / np.float32(pairs)
    inverse = np.repeat(np.float32(rotary_base) ** exponents, 2).astype(np.float32)
    angles = np.arange(count, dtype=np.float32)[:, None] * inverse
    sign = np.where(np.arange(DK // 2) % 2 == 0, -1.0, 1.0).astype(np.float32)
    return np.concatenate([np.cos(angles), np.sin(angles) * sign], axis=1)


def tables_kernel(lines, chips, decay_ref, col_ref, line_ref):
    rows = 2 * chips * lines
    chip, core = lax.axis_index("x"), lax.axis_index("c")

    def position(local):
        origin = (chip - (local // lines) % chips + chips) % chips
        return origin * GRID_W + ((local // (chips * lines) + core) % 2) * lines + local % lines

    down = lax.broadcasted_iota(jnp.int32, (rows, rows), 0)
    across = lax.broadcasted_iota(jnp.int32, (rows, rows), 1)
    place_col = position(lax.broadcasted_iota(jnp.int32, (rows, 1), 0))
    place_line = position(lax.broadcasted_iota(jnp.int32, (1, rows), 1))
    flat = decay_ref[...]
    total = jnp.sum(flat, axis=1, keepdims=True)
    flat_col = jnp.sum(jnp.where(down == across, flat, 0.0), axis=1, keepdims=True)
    upto = jnp.sum(jnp.where(across <= place_col, flat, 0.0), axis=1, keepdims=True)
    before = jnp.sum(jnp.where(across < place_col, flat, 0.0), axis=1, keepdims=True)
    col_ref[:, 0:1] = total - upto
    col_ref[:, 1:2] = before
    col_ref[:, 2:3] = upto
    col_ref[:, 3:4] = total - before
    col_ref[:, 4:5] = place_col.astype(f32)
    line_ref[0:1, :] = jnp.sum(jnp.where(down <= place_line, flat_col, 0.0), axis=0, keepdims=True)
    line_ref[1:2, :] = jnp.sum(jnp.where(down < place_line, flat_col, 0.0), axis=0, keepdims=True)
    line_ref[2:3, :] = place_line.astype(f32)
    odd = lax.axis_index("y") % 2
    line_ref[3:4, :] = jnp.full((1, rows), odd, jnp.int32).astype(f32)


def gather_kernel(pieces_ref, out_ref, decay_ref):
    cuts = out_ref.shape[2] // 128
    pieces = [pieces_ref[r].astype(f32) for r in range(pieces_ref.shape[0])]
    summed = functools.reduce(jnp.add, pieces)
    rows = [
        jnp.concatenate([summed[i * cuts + k : i * cuts + k + 1, :] for k in range(cuts)], axis=1)
        for i in range(2)
    ]
    for t in range(out_ref.shape[0]):
        out_ref[t] = jnp.concatenate(rows, axis=0)
    for r, piece in enumerate(pieces):
        decay = jnp.exp(jnp.sum(piece[2 * cuts :, :], axis=0, keepdims=True))
        decay_ref[r : r + 1, :] = decay


def keys_kernel(*refs):
    pieces, refs = refs[:8], refs[8:]
    (
        near_hbm, wv_hbm, wk_ref, low_ref, gain_ref, far_ref, mod_ref, col_ref, line_ref, row_ref,
        column_ref,
        send_ref, normed_hbm, k_hbm, v_hbm,
        own_ref, near_ref, high_ref, normed_ref, k_ref, v_ref, sems,
    ) = refs
    lines, width = pieces[0].shape
    rows = 8 * lines
    near = near_ref.shape[0]
    own = [
        started(pieces[0], own_ref, sems, 3),
        started(near_hbm, near_ref, sems, 4),
    ]
    load = started(wv_hbm.at[:, low_ref.shape[1] :], high_ref, sems, 0)
    gain = flat_gain(gain_ref)
    tp = mod_ref.shape[0]

    def line_of(which):
        line = jnp.concatenate([mod_ref[t, which : which + 1, :] for t in range(tp)], axis=1)
        return line[:, :width], gain * (1.0 + line[:, width : 2 * width])

    lines_of = [line_of(which) for which in range(2)]

    def modulate(source_ref, base, which):
        shift, scale = lines_of[which]

        def block(i, carry):
            own = pl.ds(pl.multiple_of(i * 16, 16), 16)
            wide = source_ref[own, :].astype(f32)
            normal = wide * lax.rsqrt(jnp.mean(wide * wide, axis=-1, keepdims=True) + epsilon)
            target = pl.ds(pl.multiple_of(base + i * 16, 16), 16)
            normed_ref[target, :] = (normal * scale + shift).astype(bf16)
            return carry

        lax.fori_loop(0, source_ref.shape[0] // 16, block, 0)

    for i, piece in enumerate(pieces[1:]):
        modulate(piece, (i + 1) * lines, 0)
    modulate(far_ref, rows + near, 1)
    for copy in own:
        copy.wait()
    modulate(own_ref, 0, 0)
    modulate(near_ref, rows, 1)
    stores = [started(normed_ref.at[0:rows], normed_hbm, sems, 2)]
    load.wait()
    keys = dot(normed_ref[...], wk_ref[...])
    low = dot(normed_ref[...], low_ref[...]).astype(bf16)
    high = dot(normed_ref[...], high_ref[...]).astype(bf16)
    values = jnp.concatenate([low, high], axis=1)
    key_rows = (turn(keys[:rows], row_ref, column_ref) * DK ** (-0.5)).astype(bf16)
    ctx_keys = (keys[rows:] * DK ** (-0.5)).astype(bf16)
    k_ref[...] = key_rows
    stores.append(started(k_ref, k_hbm, sems, 1))
    wide = key_rows.astype(f32)
    ahead = (wide * jnp.exp(col_ref[:, 0:1])).astype(bf16)
    behind = (wide * jnp.exp(col_ref[:, 1:2])).astype(bf16)
    turned = jnp.concatenate([ahead.T, behind.T], axis=0)
    v_ref[...] = values[:rows]
    stores.append(started(v_ref, v_hbm, sems, 5))
    parts = dot(turned, values[:rows]).astype(bf16)
    send_ref[:, 0:DV] = parts[:DK]
    send_ref[:, DV : 2 * DV] = parts[DK:]
    ctx_values = values[rows:]
    odd = line_ref[3:4, 0 : DV // 2] > 0.5
    own_values = jnp.where(
        odd, ctx_values[:, DV // 2 :].astype(f32), ctx_values[:, : DV // 2].astype(f32)
    ).astype(bf16)
    send_ref[:, 2 * DV :] = dot(ctx_keys.T, own_values).astype(bf16)
    for copy in stores:
        copy.wait()


def inside_kernel(
    normed_hbm, wq_hbm, wg_hbm, k_hbm, v_hbm, col_ref, line_ref, row_ref, column_ref,
    q_ref, g_ref, y_ref,
    normed_ref, wq_ref, wg_ref, k_ref, v_ref, sems,
):
    pairs = [
        (normed_hbm, normed_ref), (wq_hbm, wq_ref), (k_hbm, k_ref), (v_hbm, v_ref),
        (wg_hbm, wg_ref),
    ]
    loads = [started(a, b, sems, i) for i, (a, b) in enumerate(pairs)]
    for copy in loads[:4]:
        copy.wait()
    queries = turn(dot(normed_ref[...], wq_ref[...]), row_ref, column_ref).astype(bf16)
    q_ref[...] = queries
    scores = dot_t(queries, k_ref[...])
    here, there = col_ref[:, 4:5], line_ref[2:3, :]
    gaps = jnp.where(
        here >= there,
        col_ref[:, 2:3] - line_ref[0:1, :],
        line_ref[1:2, :] - col_ref[:, 1:2],
    )
    weights = jnp.exp(gaps) * jnp.where(here == there, 2.0, 1.0)
    y_ref[...] = dot((scores * weights).astype(bf16), v_ref[...]).astype(bf16)
    loads[4].wait()
    g_ref[...] = dot(normed_ref[...], wg_ref[...]).astype(bf16)


def scan_kernel(parts_ref, decay_ref, out_ref):
    count, z_size = parts_ref.shape[0], lax.axis_size("z")
    y_size = count // z_size
    spot = [(r % y_size) * z_size + r // y_size for r in range(count)]
    lifts = []
    for parity in range(2):
        lift = parts_ref[spot[parity], :, 2 * DV :].astype(f32)
        for r in range(parity + 2, count, 2):
            lift = lift + parts_ref[spot[r], :, 2 * DV :].astype(f32)
        lifts.append(lift)
    ahead = behind = jnp.concatenate(lifts, axis=1) * float(CTX_LIFT)
    decays = [jnp.concatenate([decay_ref[r : r + 1, :]] * (DV // 128), axis=1) for r in range(count)]
    for r in range(count):
        s = count - 1 - r
        out_ref[spot[r], :, 0:DV] = ahead.astype(bf16)
        out_ref[spot[s], :, DV:] = behind.astype(bf16)
        ahead = decays[r] * ahead + parts_ref[spot[r], :, 0:DV].astype(f32)
        behind = (
            decays[s] * behind + parts_ref[spot[s], :, DV : 2 * DV].astype(f32)
        )


def output_kernel(
    part, y_ref, g_ref, q_ref, states_ref, col_ref, gain_ref, wo_ref, out_ref
):
    half = out_ref.shape[0]
    own = slice(part * half, (part + 1) * half)
    queries = q_ref[own, :]
    mixed = (
        y_ref[own, :].astype(f32)
        + jnp.exp(col_ref[own, 2:3]) * dot(queries, states_ref[:, 0:DV])
        + jnp.exp(col_ref[own, 3:4]) * dot(queries, states_ref[:, DV:])
    )
    average = jnp.mean(mixed, axis=-1, keepdims=True)
    centred = mixed - average
    variance = jnp.mean(centred * centred, axis=-1, keepdims=True)
    gates = g_ref[own, :].astype(f32)
    attended = (
        gates * jax.nn.sigmoid(gates) * (centred * lax.rsqrt(variance + epsilon))
        * flat_gain(gain_ref)
    ).astype(bf16)
    out_ref[...] = dot(attended, wo_ref[...]).astype(bf16)


def pair_kernel(own_ref, crossed_ref, *out_refs):
    lines = out_refs[0].shape[0]
    for d, out_ref in enumerate(out_refs):
        own = slice(d * lines, (d + 1) * lines)
        out_ref[...] = (own_ref[own, :].astype(f32) + crossed_ref[own, :].astype(f32)).astype(bf16)


def ring(size, step):
    return [(i, (i + step) % size) for i in range(size)]


def shaped(*shape, dtype=bf16):
    return jax.ShapeDtypeStruct(shape, dtype)


def per_device(
    latent,
    log_decay,
    context,
    condition,
    w_modulate,
    norm_gain,
    w_query,
    w_key,
    w_value,
    w_gate,
    group_gain,
    w_output,
):
    lines, width = latent.shape
    x_size = lax.axis_size("x")
    half = lines * x_size
    rows = 2 * half
    swap = [(0, 1), (1, 0)]

    columns = w_modulate.shape[1]
    sems = pltpu.SemaphoreType.DMA
    count, tp = lax.axis_size(SP), lax.axis_size(TP)
    packed, decay_row, row_table, column_table, gain, early_key, early_value = kernel_call(
        functools.partial(prepare_kernel, lines),
        [
            ("v", shaped(count, 16, 128)),
            ("v", shaped(1, rows, dtype=f32)),
            ("v", shaped(x_size, 1, DK, dtype=f32)),
            ("v", shaped(2 * lines, DK, dtype=f32)),
            ("v", shaped(width // 128, 128)),
            ("v", shaped(width, DK)),
            ("v", shaped(width, DV // 2)),
        ],
        "hhhhhhhh",
        [
            pltpu.VMEM(w_modulate.shape, bf16),
            pltpu.VMEM(condition.shape, bf16),
            sems((8 + x_size,)),
        ],
        8,
        1000000,
        w_modulate,
        condition,
        log_decay.T,
        jnp.asarray(rotary_tables(count * rows // GRID_W))[:, None],
        jnp.asarray(rotary_tables(GRID_W)),
        norm_gain.reshape(-1, 128),
        w_key,
        w_value,
    )
    pieces = lax.all_to_all(packed, SP, 0, 0, tiled=True)
    spread, decays = kernel_call(
        gather_kernel,
        [("v", shaped(tp, 2, columns, dtype=f32)), ("v", shaped(count, 128, dtype=f32))],
        "v",
        [],
        4,
        1000000,
        pieces,
    )
    modulation = lax.all_to_all(spread, TP, 0, 0, tiled=True)

    later, near, _ = lax.optimization_barrier((latent, context, packed))
    own_rows = [later] + [lax.ppermute(later, "x", ring(x_size, d)) for d in range(1, x_size)]
    other_rows = [lax.ppermute(piece, "c", swap) for piece in own_rows]
    far = lax.ppermute(near, "y", [(0, 1), (1, 0), (2, 3), (3, 2)])
    col, line = kernel_call(
        functools.partial(tables_kernel, lines, x_size),
        [("v", shaped(rows, 8, dtype=f32)), ("v", shaped(4, rows, dtype=f32))],
        "v",
        [],
        8,
        1000000,
        decay_row,
    )

    ctx = 2 * context.shape[0]
    lanes = 2 * DV + DV // 2
    send, normed, key_rows, value_rows = kernel_call(
        keys_kernel,
        [
            ("v", shaped(DK, lanes)),
            ("h", shaped(rows, width)),
            ("h", shaped(rows, DK)),
            ("h", shaped(rows, DV)),
        ],
        "hvvvvvvv" + "hhvvvvvvvvv",
        [
            pltpu.VMEM((lines, width), bf16),
            pltpu.VMEM(context.shape, bf16),
            pltpu.VMEM((width, DV // 2), bf16),
            pltpu.VMEM((rows + ctx, width), bf16),
            pltpu.VMEM((rows, DK), bf16),
            pltpu.VMEM((rows, DV), bf16),
            sems((6,)),
        ],
        32,
        2 * (rows + ctx) * width * (DK + DV),
        *own_rows,
        *other_rows,
        near,
        w_value,
        early_key,
        early_value,
        gain,
        far,
        modulation,
        col,
        line,
        row_table,
        column_table,
    )
    parts = lax.all_to_all(send.reshape(count, DK // count, lanes), YZ, 0, 0, tiled=True)
    queries, gates, inside = kernel_call(
        inside_kernel,
        [
            ("v", shaped(rows, DK)),
            ("v", shaped(rows, DV)),
            ("v", shaped(rows, DV)),
        ],
        "hhhhhvvvv",
        [
            pltpu.VMEM((rows, width), bf16),
            pltpu.VMEM((width, DK), bf16),
            pltpu.VMEM((width, DV), bf16),
            pltpu.VMEM((rows, DK), bf16),
            pltpu.VMEM((rows, DV), bf16),
            sems((5,)),
        ],
        32,
        2 * rows * width * (DK + DV),
        normed,
        w_query,
        w_gate,
        key_rows,
        value_rows,
        col,
        line,
        row_table,
        column_table,
    )
    (entering,) = kernel_call(
        scan_kernel,
        [("v", shaped(count, DK // count, 2 * DV))],
        "vv",
        [],
        16,
        10 * parts.size,
        parts,
        decays,
    )
    states = lax.all_to_all(entering, YZ, 0, 0, tiled=True).reshape(DK, 2 * DV)
    partials = []
    for part in (1, 0):
        (partial,) = kernel_call(
            functools.partial(output_kernel, part),
            [("v", shaped(half, width))],
            "vvvvvvv",
            [],
            32,
            2 * half * DV * width,
            inside,
            gates,
            queries,
            states,
            col,
            group_gain.reshape(-1, 128),
            w_output,
        )
        partials.append(partial)
    crossed = lax.ppermute(partials[0], "c", swap)
    tiles = kernel_call(
        pair_kernel,
        [("v", shaped(lines, width))] * x_size,
        "vv",
        [],
        8,
        half * width,
        partials[1],
        crossed,
    )
    projected = tiles[0].astype(f32)
    for d in (2, 1, 3):
        arrived = lax.ppermute(tiles[d], "x", ring(x_size, -d))
        projected = projected + arrived.astype(f32)
    gate = modulation[:, 0].reshape(-1)[2 * width :]
    return (latent.astype(f32) + gate * projected).astype(bf16)


def solution(mesh):
    torus = Mesh(mesh.devices.reshape(8, 4, 4, 2), ALL)
    in_specs = (
        P(ALL, None),
        P(SP, TP),
        P(SP, None),
        P(),
        P(SP, TP),
        P(),
        P(None, TP),
        P(None, TP),
        P(None, TP),
        P(None, TP),
        P(TP),
        P(TP, None),
    )
    return jax.shard_map(
        per_device, mesh=torus, in_specs=in_specs, out_specs=P(ALL, None), check_vma=False
    )
```

```python
import functools

import jax
import jax.numpy as jnp
import numpy as np
from jax import lax
from jax.experimental import pallas as pl
from jax.experimental.pallas import tpu as pltpu
from jax.sharding import Mesh
from jax.sharding import PartitionSpec as P

DK = 256
DV = 512
GRID_W = 64
CTX_LIFT = 4
SP = ("z", "y")
YZ = ("y", "z")
TP = ("x", "c")
ALL = ("z", "y", "x", "c")
f32 = jnp.float32
bf16 = jnp.bfloat16

epsilon = 1e-06
rotary_base = 10000.0
MIB = 1024 * 1024


def kernel_call(body, outs, ins, scratch, vmem, flops, *args):
    spaces = {"h": pltpu.MemorySpace.HBM, "v": pltpu.MemorySpace.VMEM}
    moved = sum(a.size * a.dtype.itemsize for a in args)
    args = [
        pltpu.with_memory_space_constraint(a, pltpu.HBM) if k == "h" else a
        for k, a in zip(ins, args)
    ]
    return pl.pallas_call(
        body,
        out_shape=tuple(pltpu.HBM(a.shape, a.dtype) if k == "h" else a for k, a in outs),
        in_specs=[pl.BlockSpec(memory_space=spaces[k]) for k in ins],
        out_specs=tuple(pl.BlockSpec(memory_space=spaces[k]) for k, _ in outs),
        scratch_shapes=scratch,
        compiler_params=pltpu.CompilerParams(vmem_limit_bytes=vmem * MIB),
        cost_estimate=pl.CostEstimate(flops=flops, bytes_accessed=moved, transcendentals=0),
    )(*args)


def started(source, target, sems, slot):
    copy = pltpu.make_async_copy(source, target, sems.at[slot])
    copy.start()
    return copy


def flat_gain(gain_ref):
    wide = gain_ref[...].astype(f32)
    return jnp.concatenate([wide[i : i + 1, :] for i in range(wide.shape[0])], axis=1)


def dot(a, b):
    return jnp.dot(a, b, preferred_element_type=f32)


def dot_t(a, b):
    return lax.dot_general(a, b, (((1,), (1,)), ((), ())), preferred_element_type=f32)


def turn(u, row_ref, column_ref):
    lanes = lax.broadcasted_iota(jnp.int32, u.shape, 1)
    swapped = jnp.where(lanes % 2 == 0, pltpu.roll(u, DK - 1, 1), pltpu.roll(u, 1, 1))
    chips, lines, pair = row_ref.shape[0], column_ref.shape[0] // 2, DK // 2
    turned = []
    for i in range(2 * chips):
        own, half, d = slice(i * lines, (i + 1) * lines), i // chips, i % chips
        column = column_ref[half * lines : (half + 1) * lines, :]
        low = u[own, :pair] * row_ref[d, :, :pair] + swapped[own, :pair] * row_ref[d, :, pair:]
        high = u[own, pair:] * column[:, :pair] + swapped[own, pair:] * column[:, pair:]
        turned.append(jnp.concatenate([low, high], axis=1))
    return jnp.concatenate(turned, axis=0)


def prepare_kernel(
    lines, weights_hbm, condition_hbm, decay_hbm, row_hbm, column_hbm, gain_hbm,
    out_ref, decay_ref, row_ref, column_ref, gain_ref,
    weights_ref, condition_ref, sems,
):
    size, width = weights_hbm.shape[0], condition_hbm.shape[1]
    seq = lax.axis_index("z") * lax.axis_size("y") + lax.axis_index("y")
    chip, core = lax.axis_index("x"), lax.axis_index("c")
    chips = row_ref.shape[0]
    loads = [
        started(condition_hbm, condition_ref, sems, 0),
        started(decay_hbm, decay_ref, sems, 1),
        started(weights_hbm, weights_ref, sems, 2),
    ]
    for h in range(2):
        column = pl.multiple_of(((h + core) % 2) * lines, lines)
        target = column_ref.at[h * lines : (h + 1) * lines]
        loads.append(started(column_hbm.at[pl.ds(column, lines)], target, sems, 3 + h))
    for d in range(chips):
        row = seq * chips + (chip - d + chips) % chips
        loads.append(started(row_hbm.at[row], row_ref.at[d], sems, 5 + d))
    loads.append(started(gain_hbm, gain_ref, sems, 5 + chips))
    loads[0].wait()
    values = condition_ref[...].astype(f32)
    values = jnp.concatenate([values] * 4, axis=0)
    inputs = pltpu.roll(values, (width - seq * size) % width, 1)[0:2, 0:size]
    activated = (inputs / (1.0 + jnp.exp(-inputs))).astype(bf16)
    loads[1].wait()
    total = jnp.sum(decay_ref[...], axis=1, keepdims=True)
    loads[2].wait()
    part = dot(activated, weights_ref[...])
    cuts = part.shape[1] // 128
    packed = [part[i : i + 1, k * 128 : (k + 1) * 128] for i in range(2) for k in range(cuts)]
    rest = total
    while len(packed) < out_ref.shape[1]:
        term = rest.astype(bf16).astype(f32)
        packed.append(jnp.broadcast_to(term, (1, 128)))
        rest = rest - term
    packed = jnp.concatenate(packed, axis=0).astype(bf16)
    for r in range(out_ref.shape[0]):
        out_ref[r] = packed
    for copy in loads[3:]:
        copy.wait()


def rotary_tables(count):
    pairs = DK // 4
    exponents = -np.arange(pairs, dtype=np.float32) / np.float32(pairs)
    inverse = np.repeat(np.float32(rotary_base) ** exponents, 2).astype(np.float32)
    angles = np.arange(count, dtype=np.float32)[:, None] * inverse
    sign = np.where(np.arange(DK // 2) % 2 == 0, -1.0, 1.0).astype(np.float32)
    return np.concatenate([np.cos(angles), np.sin(angles) * sign], axis=1)


def tables_kernel(lines, chips, decay_ref, col_ref, line_ref):
    rows = 2 * chips * lines
    chip, core = lax.axis_index("x"), lax.axis_index("c")

    def position(local):
        origin = (chip - (local // lines) % chips + chips) % chips
        return origin * GRID_W + ((local // (chips * lines) + core) % 2) * lines + local % lines

    down = lax.broadcasted_iota(jnp.int32, (rows, rows), 0)
    across = lax.broadcasted_iota(jnp.int32, (rows, rows), 1)
    place_col = position(lax.broadcasted_iota(jnp.int32, (rows, 1), 0))
    place_line = position(lax.broadcasted_iota(jnp.int32, (1, rows), 1))
    flat = decay_ref[...]
    total = jnp.sum(flat, axis=1, keepdims=True)
    flat_col = jnp.sum(jnp.where(down == across, flat, 0.0), axis=1, keepdims=True)
    upto = jnp.sum(jnp.where(across <= place_col, flat, 0.0), axis=1, keepdims=True)
    before = jnp.sum(jnp.where(across < place_col, flat, 0.0), axis=1, keepdims=True)
    col_ref[:, 0:1] = total - upto
    col_ref[:, 1:2] = before
    col_ref[:, 2:3] = upto
    col_ref[:, 3:4] = total - before
    col_ref[:, 4:5] = place_col.astype(f32)
    line_ref[0:1, :] = jnp.sum(jnp.where(down <= place_line, flat_col, 0.0), axis=0, keepdims=True)
    line_ref[1:2, :] = jnp.sum(jnp.where(down < place_line, flat_col, 0.0), axis=0, keepdims=True)
    line_ref[2:3, :] = place_line.astype(f32)
    odd = lax.axis_index("y") % 2
    line_ref[3:4, :] = jnp.full((1, rows), odd, jnp.int32).astype(f32)


def gather_kernel(pieces_ref, out_ref, decay_ref):
    cuts = out_ref.shape[2] // 128
    pieces = [pieces_ref[r].astype(f32) for r in range(pieces_ref.shape[0])]
    summed = functools.reduce(jnp.add, pieces)
    rows = [
        jnp.concatenate([summed[i * cuts + k : i * cuts + k + 1, :] for k in range(cuts)], axis=1)
        for i in range(2)
    ]
    for t in range(out_ref.shape[0]):
        out_ref[t] = jnp.concatenate(rows, axis=0)
    for r, piece in enumerate(pieces):
        decay = jnp.exp(jnp.sum(piece[2 * cuts :, :], axis=0, keepdims=True))
        decay_ref[r : r + 1, :] = decay


def keys_kernel(*refs):
    pieces, refs = refs[:8], refs[8:]
    (
        near_hbm, wk_hbm, wv_hbm, gain_ref, far_ref, mod_ref, col_ref, line_ref, row_ref,
        column_ref,
        send_ref, normed_hbm, k_ref, v_ref,
        own_ref, near_ref, wk_ref, wv_ref, normed_ref, sems,
    ) = refs
    lines, width = pieces[0].shape
    rows = 8 * lines
    near = near_ref.shape[0]
    loads = [started(wk_hbm, wk_ref, sems, 0)]
    own = [started(pieces[0], own_ref, sems, 7), started(near_hbm, near_ref, sems, 8)]
    gain = flat_gain(gain_ref)
    tp = mod_ref.shape[0]

    def line_of(which):
        line = jnp.concatenate([mod_ref[t, which : which + 1, :] for t in range(tp)], axis=1)
        return line[:, :width], gain * (1.0 + line[:, width : 2 * width])

    lines_of = [line_of(which) for which in range(2)]

    def modulated(values, which):
        shift, scale = lines_of[which]
        wide = values.astype(f32)
        normal = wide * lax.rsqrt(jnp.mean(wide * wide, axis=-1, keepdims=True) + epsilon)
        return (normal * scale + shift).astype(bf16)

    for i, piece in enumerate(pieces[1:]):
        normed_ref[(i + 1) * lines : (i + 2) * lines, :] = modulated(piece[...], 0)
        if i == 2:
            loads.append(started(wv_hbm, wv_ref, sems, 1))
    normed_ref[rows + near :, :] = modulated(far_ref[...], 1)
    for copy in own:
        copy.wait()
    normed_ref[0:lines, :] = modulated(own_ref[...], 0)
    normed_ref[rows : rows + near, :] = modulated(near_ref[...], 1)
    loads[0].wait()
    keys = dot(normed_ref[...], wk_ref[...])
    key_rows = (turn(keys[:rows], row_ref, column_ref) * DK ** (-0.5)).astype(bf16)
    ctx_keys = (keys[rows:] * DK ** (-0.5)).astype(bf16)
    k_ref[...] = key_rows
    wide = key_rows.astype(f32)
    ahead = (wide * jnp.exp(col_ref[:, 0:1])).astype(bf16)
    behind = (wide * jnp.exp(col_ref[:, 1:2])).astype(bf16)
    turned = jnp.concatenate([ahead.T, behind.T], axis=0)
    loads[1].wait()
    stores = [started(normed_ref.at[0:rows], normed_hbm, sems, 2)]
    values = dot(normed_ref[...], wv_ref[...]).astype(bf16)
    v_ref[...] = values[:rows]
    parts = dot(turned, values[:rows]).astype(bf16)
    send_ref[:, 0:DV] = parts[:DK]
    send_ref[:, DV : 2 * DV] = parts[DK:]
    ctx_values = values[rows:]
    odd = line_ref[3:4, 0 : DV // 2] > 0.5
    own_values = jnp.where(
        odd, ctx_values[:, DV // 2 :].astype(f32), ctx_values[:, : DV // 2].astype(f32)
    ).astype(bf16)
    send_ref[:, 2 * DV :] = dot(ctx_keys.T, own_values).astype(bf16)
    for copy in stores:
        copy.wait()


def inside_kernel(
    normed_hbm, wq_hbm, wg_hbm, k_ref, v_ref, col_ref, line_ref, row_ref, column_ref,
    q_ref, g_ref, y_ref,
    normed_ref, wq_ref, wg_ref, sems,
):
    pairs = [(normed_hbm, normed_ref), (wq_hbm, wq_ref), (wg_hbm, wg_ref)]
    loads = [started(a, b, sems, i) for i, (a, b) in enumerate(pairs)]
    for copy in loads[:2]:
        copy.wait()
    queries = turn(dot(normed_ref[...], wq_ref[...]), row_ref, column_ref).astype(bf16)
    q_ref[...] = queries
    scores = dot_t(queries, k_ref[...])
    here, there = col_ref[:, 4:5], line_ref[2:3, :]
    gaps = jnp.where(
        here >= there,
        col_ref[:, 2:3] - line_ref[0:1, :],
        line_ref[1:2, :] - col_ref[:, 1:2],
    )
    weights = jnp.exp(gaps) * jnp.where(here == there, 2.0, 1.0)
    y_ref[...] = dot((scores * weights).astype(bf16), v_ref[...]).astype(bf16)
    loads[2].wait()
    g_ref[...] = dot(normed_ref[...], wg_ref[...]).astype(bf16)


def scan_kernel(parts_ref, decay_ref, out_ref):
    count, z_size = parts_ref.shape[0], lax.axis_size("z")
    y_size = count // z_size
    spot = [(r % y_size) * z_size + r // y_size for r in range(count)]
    lifts = []
    for parity in range(2):
        lift = parts_ref[spot[parity], :, 2 * DV :].astype(f32)
        for r in range(parity + 2, count, 2):
            lift = lift + parts_ref[spot[r], :, 2 * DV :].astype(f32)
        lifts.append(lift)
    ahead = behind = jnp.concatenate(lifts, axis=1) * float(CTX_LIFT)
    decays = [jnp.concatenate([decay_ref[r : r + 1, :]] * (DV // 128), axis=1) for r in range(count)]
    for r in range(count):
        s = count - 1 - r
        out_ref[spot[r], :, 0:DV] = ahead.astype(bf16)
        out_ref[spot[s], :, DV:] = behind.astype(bf16)
        ahead = decays[r] * ahead + parts_ref[spot[r], :, 0:DV].astype(f32)
        behind = (
            decays[s] * behind + parts_ref[spot[s], :, DV : 2 * DV].astype(f32)
        )


def output_kernel(
    part, y_ref, g_ref, q_ref, states_ref, col_ref, gain_ref, wo_ref, out_ref
):
    half = out_ref.shape[0]
    own = slice(part * half, (part + 1) * half)
    queries = q_ref[own, :]
    mixed = (
        y_ref[own, :].astype(f32)
        + jnp.exp(col_ref[own, 2:3]) * dot(queries, states_ref[:, 0:DV])
        + jnp.exp(col_ref[own, 3:4]) * dot(queries, states_ref[:, DV:])
    )
    average = jnp.mean(mixed, axis=-1, keepdims=True)
    centred = mixed - average
    variance = jnp.mean(centred * centred, axis=-1, keepdims=True)
    gates = g_ref[own, :].astype(f32)
    attended = (
        gates * jax.nn.sigmoid(gates) * (centred * lax.rsqrt(variance + epsilon))
        * flat_gain(gain_ref)
    ).astype(bf16)
    out_ref[...] = dot(attended, wo_ref[...]).astype(bf16)


def pair_kernel(own_ref, crossed_ref, *out_refs):
    lines = out_refs[0].shape[0]
    for d, out_ref in enumerate(out_refs):
        own = slice(d * lines, (d + 1) * lines)
        out_ref[...] = (own_ref[own, :].astype(f32) + crossed_ref[own, :].astype(f32)).astype(bf16)


def ring(size, step):
    return [(i, (i + step) % size) for i in range(size)]


def shaped(*shape, dtype=bf16):
    return jax.ShapeDtypeStruct(shape, dtype)


def per_device(
    latent,
    log_decay,
    context,
    condition,
    w_modulate,
    norm_gain,
    w_query,
    w_key,
    w_value,
    w_gate,
    group_gain,
    w_output,
):
    lines, width = latent.shape
    x_size = lax.axis_size("x")
    half = lines * x_size
    rows = 2 * half
    swap = [(0, 1), (1, 0)]

    columns = w_modulate.shape[1]
    sems = pltpu.SemaphoreType.DMA
    count, tp = lax.axis_size(SP), lax.axis_size(TP)
    packed, decay_row, row_table, column_table, gain = kernel_call(
        functools.partial(prepare_kernel, lines),
        [
            ("v", shaped(count, 16, 128)),
            ("v", shaped(1, rows, dtype=f32)),
            ("v", shaped(x_size, 1, DK, dtype=f32)),
            ("v", shaped(2 * lines, DK, dtype=f32)),
            ("v", shaped(width // 128, 128)),
        ],
        "hhhhhh",
        [
            pltpu.VMEM(w_modulate.shape, bf16),
            pltpu.VMEM(condition.shape, bf16),
            sems((6 + x_size,)),
        ],
        4,
        1000000,
        w_modulate,
        condition,
        log_decay.T,
        jnp.asarray(rotary_tables(count * rows // GRID_W))[:, None],
        jnp.asarray(rotary_tables(GRID_W)),
        norm_gain.reshape(-1, 128),
    )
    pieces = lax.all_to_all(packed, SP, 0, 0, tiled=True)
    spread, decays = kernel_call(
        gather_kernel,
        [("v", shaped(tp, 2, columns, dtype=f32)), ("v", shaped(count, 128, dtype=f32))],
        "v",
        [],
        4,
        1000000,
        pieces,
    )
    modulation = lax.all_to_all(spread, TP, 0, 0, tiled=True)

    later, near, _ = lax.optimization_barrier((latent, context, packed))
    own_rows = [later] + [lax.ppermute(later, "x", ring(x_size, d)) for d in range(1, x_size)]
    other_rows = [lax.ppermute(piece, "c", swap) for piece in own_rows]
    far = lax.ppermute(near, "y", [(0, 1), (1, 0), (2, 3), (3, 2)])
    col, line = kernel_call(
        functools.partial(tables_kernel, lines, x_size),
        [("v", shaped(rows, 8, dtype=f32)), ("v", shaped(4, rows, dtype=f32))],
        "v",
        [],
        8,
        1000000,
        decay_row,
    )

    ctx = 2 * context.shape[0]
    lanes = 2 * DV + DV // 2
    send, normed, key_rows, value_rows = kernel_call(
        keys_kernel,
        [
            ("v", shaped(DK, lanes)),
            ("h", shaped(rows, width)),
            ("v", shaped(rows, DK)),
            ("v", shaped(rows, DV)),
        ],
        "hvvvvvvv" + "hhhvvvvvvv",
        [
            pltpu.VMEM((lines, width), bf16),
            pltpu.VMEM(context.shape, bf16),
            pltpu.VMEM((width, DK), bf16),
            pltpu.VMEM((width, DV), bf16),
            pltpu.VMEM((rows + ctx, width), bf16),
            sems((9,)),
        ],
        32,
        2 * (rows + ctx) * width * (DK + DV),
        *own_rows,
        *other_rows,
        near,
        w_key,
        w_value,
        gain,
        far,
        modulation,
        col,
        line,
        row_table,
        column_table,
    )
    parts = lax.all_to_all(send.reshape(count, DK // count, lanes), YZ, 0, 0, tiled=True)
    queries, gates, inside = kernel_call(
        inside_kernel,
        [
            ("v", shaped(rows, DK)),
            ("v", shaped(rows, DV)),
            ("v", shaped(rows, DV)),
        ],
        "hhhvvvvvv",
        [
            pltpu.VMEM((rows, width), bf16),
            pltpu.VMEM((width, DK), bf16),
            pltpu.VMEM((width, DV), bf16),
            sems((3,)),
        ],
        32,
        2 * rows * width * (DK + DV),
        normed,
        w_query,
        w_gate,
        key_rows,
        value_rows,
        col,
        line,
        row_table,
        column_table,
    )
    (entering,) = kernel_call(
        scan_kernel,
        [("v", shaped(count, DK // count, 2 * DV))],
        "vv",
        [],
        16,
        10 * parts.size,
        parts,
        decays,
    )
    states = lax.all_to_all(entering, YZ, 0, 0, tiled=True).reshape(DK, 2 * DV)
    partials = []
    for part in (1, 0):
        (partial,) = kernel_call(
            functools.partial(output_kernel, part),
            [("v", shaped(half, width))],
            "vvvvvvv",
            [],
            32,
            2 * half * DV * width,
            inside,
            gates,
            queries,
            states,
            col,
            group_gain.reshape(-1, 128),
            w_output,
        )
        partials.append(partial)
    crossed = lax.ppermute(partials[0], "c", swap)
    tiles = kernel_call(
        pair_kernel,
        [("v", shaped(lines, width))] * x_size,
        "vv",
        [],
        8,
        half * width,
        partials[1],
        crossed,
    )
    projected = tiles[0].astype(f32)
    for d in (2, 1, 3):
        arrived = lax.ppermute(tiles[d], "x", ring(x_size, -d))
        projected = projected + arrived.astype(f32)
    gate = modulation[:, 0].reshape(-1)[2 * width :]
    return (latent.astype(f32) + gate * projected).astype(bf16)


def solution(mesh):
    torus = Mesh(mesh.devices.reshape(8, 4, 4, 2), ALL)
    in_specs = (
        P(ALL, None),
        P(SP, TP),
        P(SP, None),
        P(),
        P(SP, TP),
        P(),
        P(None, TP),
        P(None, TP),
        P(None, TP),
        P(None, TP),
        P(TP),
        P(TP, None),
    )
    return jax.shard_map(
        per_device, mesh=torus, in_specs=in_specs, out_specs=P(ALL, None), check_vma=False
    )
```

```python
import functools

import jax
import jax.numpy as jnp
import numpy as np
from jax import lax
from jax.experimental import pallas as pl
from jax.experimental.pallas import tpu as pltpu
from jax.sharding import Mesh
from jax.sharding import PartitionSpec as P

DK = 256
DV = 512
GRID_W = 64
CTX_LIFT = 4
SP = ("z", "y")
YZ = ("y", "z")
TP = ("x", "c")
ALL = ("z", "y", "x", "c")
f32 = jnp.float32
bf16 = jnp.bfloat16

epsilon = 1e-06
rotary_base = 10000.0
MIB = 1024 * 1024


def kernel_call(body, outs, ins, scratch, vmem, flops, *args):
    spaces = {"h": pltpu.MemorySpace.HBM, "v": pltpu.MemorySpace.VMEM}
    moved = sum(a.size * a.dtype.itemsize for a in args)
    args = [
        pltpu.with_memory_space_constraint(a, pltpu.HBM) if k == "h" else a
        for k, a in zip(ins, args)
    ]
    return pl.pallas_call(
        body,
        out_shape=tuple(pltpu.HBM(a.shape, a.dtype) if k == "h" else a for k, a in outs),
        in_specs=[pl.BlockSpec(memory_space=spaces[k]) for k in ins],
        out_specs=tuple(pl.BlockSpec(memory_space=spaces[k]) for k, _ in outs),
        scratch_shapes=scratch,
        compiler_params=pltpu.CompilerParams(vmem_limit_bytes=vmem * MIB),
        cost_estimate=pl.CostEstimate(flops=flops, bytes_accessed=moved, transcendentals=0),
    )(*args)


def started(source, target, sems, slot):
    copy = pltpu.make_async_copy(source, target, sems.at[slot])
    copy.start()
    return copy


def flat_gain(gain_ref):
    wide = gain_ref[...].astype(f32)
    return jnp.concatenate([wide[i : i + 1, :] for i in range(wide.shape[0])], axis=1)


class Split:
    def __init__(self, source, target, sems, slot, cuts):
        size = source.shape[0] // cuts
        self.copies = [
            started(
                source.at[i * size : (i + 1) * size], target.at[i * size : (i + 1) * size], sems, slot + i
            )
            for i in range(cuts)
        ]

    def wait(self):
        for copy in self.copies:
            copy.wait()


def dot(a, b):
    return jnp.dot(a, b, preferred_element_type=f32)


def dot_t(a, b):
    return lax.dot_general(a, b, (((1,), (1,)), ((), ())), preferred_element_type=f32)


def turn(u, row_ref, column_ref):
    lanes = lax.broadcasted_iota(jnp.int32, u.shape, 1)
    swapped = jnp.where(lanes % 2 == 0, pltpu.roll(u, DK - 1, 1), pltpu.roll(u, 1, 1))
    chips, lines, pair = row_ref.shape[0], column_ref.shape[0] // 2, DK // 2
    turned = []
    for i in range(2 * chips):
        own, half, d = slice(i * lines, (i + 1) * lines), i // chips, i % chips
        column = column_ref[half * lines : (half + 1) * lines, :]
        low = u[own, :pair] * row_ref[d, :, :pair] + swapped[own, :pair] * row_ref[d, :, pair:]
        high = u[own, pair:] * column[:, :pair] + swapped[own, pair:] * column[:, pair:]
        turned.append(jnp.concatenate([low, high], axis=1))
    return jnp.concatenate(turned, axis=0)


def prepare_kernel(
    lines, weights_hbm, condition_hbm, decay_hbm, row_hbm, column_hbm, gain_hbm,
    out_ref, decay_ref, row_ref, column_ref, gain_ref,
    weights_ref, condition_ref, sems,
):
    size, width = weights_hbm.shape[0], condition_hbm.shape[1]
    seq = lax.axis_index("z") * lax.axis_size("y") + lax.axis_index("y")
    chip, core = lax.axis_index("x"), lax.axis_index("c")
    chips = row_ref.shape[0]
    loads = [
        started(condition_hbm, condition_ref, sems, 0),
        started(decay_hbm, decay_ref, sems, 1),
        started(weights_hbm, weights_ref, sems, 2),
    ]
    for h in range(2):
        column = pl.multiple_of(((h + core) % 2) * lines, lines)
        target = column_ref.at[h * lines : (h + 1) * lines]
        loads.append(started(column_hbm.at[pl.ds(column, lines)], target, sems, 3 + h))
    for d in range(chips):
        row = seq * chips + (chip - d + chips) % chips
        loads.append(started(row_hbm.at[row], row_ref.at[d], sems, 5 + d))
    loads.append(started(gain_hbm, gain_ref, sems, 5 + chips))
    loads[0].wait()
    values = condition_ref[...].astype(f32)
    values = jnp.concatenate([values] * 4, axis=0)
    inputs = pltpu.roll(values, (width - seq * size) % width, 1)[0:2, 0:size]
    activated = (inputs / (1.0 + jnp.exp(-inputs))).astype(bf16)
    loads[1].wait()
    total = jnp.sum(decay_ref[...], axis=1, keepdims=True)
    loads[2].wait()
    part = dot(activated, weights_ref[...])
    cuts = part.shape[1] // 128
    packed = [part[i : i + 1, k * 128 : (k + 1) * 128] for i in range(2) for k in range(cuts)]
    rest = total
    while len(packed) < out_ref.shape[1]:
        term = rest.astype(bf16).astype(f32)
        packed.append(jnp.broadcast_to(term, (1, 128)))
        rest = rest - term
    packed = jnp.concatenate(packed, axis=0).astype(bf16)
    for r in range(out_ref.shape[0]):
        out_ref[r] = packed
    for copy in loads[3:]:
        copy.wait()


def rotary_tables(count):
    pairs = DK // 4
    exponents = -np.arange(pairs, dtype=np.float32) / np.float32(pairs)
    inverse = np.repeat(np.float32(rotary_base) ** exponents, 2).astype(np.float32)
    angles = np.arange(count, dtype=np.float32)[:, None] * inverse
    sign = np.where(np.arange(DK // 2) % 2 == 0, -1.0, 1.0).astype(np.float32)
    return np.concatenate([np.cos(angles), np.sin(angles) * sign], axis=1)


def tables_kernel(lines, chips, decay_ref, col_ref, line_ref):
    rows = 2 * chips * lines
    chip, core = lax.axis_index("x"), lax.axis_index("c")

    def position(local):
        origin = (chip - (local // lines) % chips + chips) % chips
        return origin * GRID_W + ((local // (chips * lines) + core) % 2) * lines + local % lines

    down = lax.broadcasted_iota(jnp.int32, (rows, rows), 0)
    across = lax.broadcasted_iota(jnp.int32, (rows, rows), 1)
    place_col = position(lax.broadcasted_iota(jnp.int32, (rows, 1), 0))
    place_line = position(lax.broadcasted_iota(jnp.int32, (1, rows), 1))
    flat = decay_ref[...]
    total = jnp.sum(flat, axis=1, keepdims=True)
    flat_col = jnp.sum(jnp.where(down == across, flat, 0.0), axis=1, keepdims=True)
    upto = jnp.sum(jnp.where(across <= place_col, flat, 0.0), axis=1, keepdims=True)
    before = jnp.sum(jnp.where(across < place_col, flat, 0.0), axis=1, keepdims=True)
    col_ref[:, 0:1] = total - upto
    col_ref[:, 1:2] = before
    col_ref[:, 2:3] = upto
    col_ref[:, 3:4] = total - before
    col_ref[:, 4:5] = place_col.astype(f32)
    line_ref[0:1, :] = jnp.sum(jnp.where(down <= place_line, flat_col, 0.0), axis=0, keepdims=True)
    line_ref[1:2, :] = jnp.sum(jnp.where(down < place_line, flat_col, 0.0), axis=0, keepdims=True)
    line_ref[2:3, :] = place_line.astype(f32)
    odd = lax.axis_index("y") % 2
    line_ref[3:4, :] = jnp.full((1, rows), odd, jnp.int32).astype(f32)


def gather_kernel(pieces_ref, out_ref, decay_ref):
    cuts = out_ref.shape[2] // 128
    pieces = [pieces_ref[r].astype(f32) for r in range(pieces_ref.shape[0])]
    summed = functools.reduce(jnp.add, pieces)
    rows = [
        jnp.concatenate([summed[i * cuts + k : i * cuts + k + 1, :] for k in range(cuts)], axis=1)
        for i in range(2)
    ]
    for t in range(out_ref.shape[0]):
        out_ref[t] = jnp.concatenate(rows, axis=0)
    for r, piece in enumerate(pieces):
        decay = jnp.exp(jnp.sum(piece[2 * cuts :, :], axis=0, keepdims=True))
        decay_ref[r : r + 1, :] = decay


def keys_kernel(*refs):
    pieces, refs = refs[:8], refs[8:]
    (
        near_hbm, wk_hbm, wv_hbm, gain_ref, far_ref, mod_ref, col_ref, line_ref, row_ref,
        column_ref,
        send_ref, normed_hbm, k_ref, v_ref,
        own_ref, near_ref, wk_ref, wv_ref, normed_ref, sems,
    ) = refs
    lines, width = pieces[0].shape
    rows = 8 * lines
    near = near_ref.shape[0]
    loads = [Split(wk_hbm, wk_ref, sems, 9, 8), Split(wv_hbm, wv_ref, sems, 17, 8)]
    own = [started(pieces[0], own_ref, sems, 7), started(near_hbm, near_ref, sems, 8)]
    gain = flat_gain(gain_ref)
    tp = mod_ref.shape[0]

    def line_of(which):
        line = jnp.concatenate([mod_ref[t, which : which + 1, :] for t in range(tp)], axis=1)
        return line[:, :width], gain * (1.0 + line[:, width : 2 * width])

    lines_of = [line_of(which) for which in range(2)]

    def modulated(values, which):
        shift, scale = lines_of[which]
        wide = values.astype(f32)
        normal = wide * lax.rsqrt(jnp.mean(wide * wide, axis=-1, keepdims=True) + epsilon)
        return (normal * scale + shift).astype(bf16)

    for i, piece in enumerate(pieces[1:]):
        normed_ref[(i + 1) * lines : (i + 2) * lines, :] = modulated(piece[...], 0)
    normed_ref[rows + near :, :] = modulated(far_ref[...], 1)
    for copy in own:
        copy.wait()
    normed_ref[0:lines, :] = modulated(own_ref[...], 0)
    normed_ref[rows : rows + near, :] = modulated(near_ref[...], 1)
    loads[0].wait()
    keys = dot(normed_ref[...], wk_ref[...])
    key_rows = (turn(keys[:rows], row_ref, column_ref) * DK ** (-0.5)).astype(bf16)
    ctx_keys = (keys[rows:] * DK ** (-0.5)).astype(bf16)
    k_ref[...] = key_rows
    wide = key_rows.astype(f32)
    ahead = (wide * jnp.exp(col_ref[:, 0:1])).astype(bf16)
    behind = (wide * jnp.exp(col_ref[:, 1:2])).astype(bf16)
    turned = jnp.concatenate([ahead.T, behind.T], axis=0)
    loads[1].wait()
    stores = [Split(normed_ref.at[0:rows], normed_hbm, sems, 0, 4)]
    values = dot(normed_ref[...], wv_ref[...]).astype(bf16)
    v_ref[...] = values[:rows]
    parts = dot(turned, values[:rows]).astype(bf16)
    send_ref[:, 0:DV] = parts[:DK]
    send_ref[:, DV : 2 * DV] = parts[DK:]
    ctx_values = values[rows:]
    odd = line_ref[3:4, 0 : DV // 2] > 0.5
    own_values = jnp.where(
        odd, ctx_values[:, DV // 2 :].astype(f32), ctx_values[:, : DV // 2].astype(f32)
    ).astype(bf16)
    send_ref[:, 2 * DV :] = dot(ctx_keys.T, own_values).astype(bf16)
    for copy in stores:
        copy.wait()


def inside_kernel(
    normed_hbm, wq_hbm, wg_hbm, k_ref, v_ref, col_ref, line_ref, row_ref, column_ref,
    q_ref, g_ref, y_ref,
    normed_ref, wq_ref, wg_ref, sems,
):
    pairs = [(normed_hbm, normed_ref), (wq_hbm, wq_ref), (wg_hbm, wg_ref)]
    loads = [Split(a, b, sems, 8 * i, 8) for i, (a, b) in enumerate(pairs)]
    for copy in loads[:2]:
        copy.wait()
    queries = turn(dot(normed_ref[...], wq_ref[...]), row_ref, column_ref).astype(bf16)
    q_ref[...] = queries
    scores = dot_t(queries, k_ref[...])
    here, there = col_ref[:, 4:5], line_ref[2:3, :]
    gaps = jnp.where(
        here >= there,
        col_ref[:, 2:3] - line_ref[0:1, :],
        line_ref[1:2, :] - col_ref[:, 1:2],
    )
    weights = jnp.exp(gaps) * jnp.where(here == there, 2.0, 1.0)
    y_ref[...] = dot((scores * weights).astype(bf16), v_ref[...]).astype(bf16)
    loads[2].wait()
    g_ref[...] = dot(normed_ref[...], wg_ref[...]).astype(bf16)


def scan_kernel(parts_ref, decay_ref, out_ref):
    count, z_size = parts_ref.shape[0], lax.axis_size("z")
    y_size = count // z_size
    spot = [(r % y_size) * z_size + r // y_size for r in range(count)]
    lifts = []
    for parity in range(2):
        lift = parts_ref[spot[parity], :, 2 * DV :].astype(f32)
        for r in range(parity + 2, count, 2):
            lift = lift + parts_ref[spot[r], :, 2 * DV :].astype(f32)
        lifts.append(lift)
    ahead = behind = jnp.concatenate(lifts, axis=1) * float(CTX_LIFT)
    decays = [jnp.concatenate([decay_ref[r : r + 1, :]] * (DV // 128), axis=1) for r in range(count)]
    for r in range(count):
        s = count - 1 - r
        out_ref[spot[r], :, 0:DV] = ahead.astype(bf16)
        out_ref[spot[s], :, DV:] = behind.astype(bf16)
        ahead = decays[r] * ahead + parts_ref[spot[r], :, 0:DV].astype(f32)
        behind = (
            decays[s] * behind + parts_ref[spot[s], :, DV : 2 * DV].astype(f32)
        )


def output_kernel(
    part, y_ref, g_ref, q_ref, states_ref, col_ref, gain_ref, wo_ref, out_ref
):
    half = out_ref.shape[0]
    own = slice(part * half, (part + 1) * half)
    queries = q_ref[own, :]
    mixed = (
        y_ref[own, :].astype(f32)
        + jnp.exp(col_ref[own, 2:3]) * dot(queries, states_ref[:, 0:DV])
        + jnp.exp(col_ref[own, 3:4]) * dot(queries, states_ref[:, DV:])
    )
    average = jnp.mean(mixed, axis=-1, keepdims=True)
    centred = mixed - average
    variance = jnp.mean(centred * centred, axis=-1, keepdims=True)
    gates = g_ref[own, :].astype(f32)
    attended = (
        gates * jax.nn.sigmoid(gates) * (centred * lax.rsqrt(variance + epsilon))
        * flat_gain(gain_ref)
    ).astype(bf16)
    out_ref[...] = dot(attended, wo_ref[...]).astype(bf16)


def pair_kernel(own_ref, crossed_ref, *out_refs):
    lines = out_refs[0].shape[0]
    for d, out_ref in enumerate(out_refs):
        own = slice(d * lines, (d + 1) * lines)
        out_ref[...] = (own_ref[own, :].astype(f32) + crossed_ref[own, :].astype(f32)).astype(bf16)


def ring(size, step):
    return [(i, (i + step) % size) for i in range(size)]


def shaped(*shape, dtype=bf16):
    return jax.ShapeDtypeStruct(shape, dtype)


def per_device(
    latent,
    log_decay,
    context,
    condition,
    w_modulate,
    norm_gain,
    w_query,
    w_key,
    w_value,
    w_gate,
    group_gain,
    w_output,
):
    lines, width = latent.shape
    x_size = lax.axis_size("x")
    half = lines * x_size
    rows = 2 * half
    swap = [(0, 1), (1, 0)]

    columns = w_modulate.shape[1]
    sems = pltpu.SemaphoreType.DMA
    count, tp = lax.axis_size(SP), lax.axis_size(TP)
    packed, decay_row, row_table, column_table, gain = kernel_call(
        functools.partial(prepare_kernel, lines),
        [
            ("v", shaped(count, 16, 128)),
            ("v", shaped(1, rows, dtype=f32)),
            ("v", shaped(x_size, 1, DK, dtype=f32)),
            ("v", shaped(2 * lines, DK, dtype=f32)),
            ("v", shaped(width // 128, 128)),
        ],
        "hhhhhh",
        [
            pltpu.VMEM(w_modulate.shape, bf16),
            pltpu.VMEM(condition.shape, bf16),
            sems((6 + x_size,)),
        ],
        4,
        1000000,
        w_modulate,
        condition,
        log_decay.T,
        jnp.asarray(rotary_tables(count * rows // GRID_W))[:, None],
        jnp.asarray(rotary_tables(GRID_W)),
        norm_gain.reshape(-1, 128),
    )
    pieces = lax.all_to_all(packed, SP, 0, 0, tiled=True)
    spread, decays = kernel_call(
        gather_kernel,
        [("v", shaped(tp, 2, columns, dtype=f32)), ("v", shaped(count, 128, dtype=f32))],
        "v",
        [],
        4,
        1000000,
        pieces,
    )
    modulation = lax.all_to_all(spread, TP, 0, 0, tiled=True)

    later, near, _ = lax.optimization_barrier((latent, context, packed))
    own_rows = [later] + [lax.ppermute(later, "x", ring(x_size, d)) for d in range(1, x_size)]
    other_rows = [lax.ppermute(piece, "c", swap) for piece in own_rows]
    far = lax.ppermute(near, "y", [(0, 1), (1, 0), (2, 3), (3, 2)])
    col, line = kernel_call(
        functools.partial(tables_kernel, lines, x_size),
        [("v", shaped(rows, 8, dtype=f32)), ("v", shaped(4, rows, dtype=f32))],
        "v",
        [],
        8,
        1000000,
        decay_row,
    )

    ctx = 2 * context.shape[0]
    lanes = 2 * DV + DV // 2
    send, normed, key_rows, value_rows = kernel_call(
        keys_kernel,
        [
            ("v", shaped(DK, lanes)),
            ("h", shaped(rows, width)),
            ("v", shaped(rows, DK)),
            ("v", shaped(rows, DV)),
        ],
        "hvvvvvvv" + "hhhvvvvvvv",
        [
            pltpu.VMEM((lines, width), bf16),
            pltpu.VMEM(context.shape, bf16),
            pltpu.VMEM((width, DK), bf16),
            pltpu.VMEM((width, DV), bf16),
            pltpu.VMEM((rows + ctx, width), bf16),
            sems((25,)),
        ],
        32,
        2 * (rows + ctx) * width * (DK + DV),
        *own_rows,
        *other_rows,
        near,
        w_key,
        w_value,
        gain,
        far,
        modulation,
        col,
        line,
        row_table,
        column_table,
    )
    parts = lax.all_to_all(send.reshape(count, DK // count, lanes), YZ, 0, 0, tiled=True)
    queries, gates, inside = kernel_call(
        inside_kernel,
        [
            ("v", shaped(rows, DK)),
            ("v", shaped(rows, DV)),
            ("v", shaped(rows, DV)),
        ],
        "hhhvvvvvv",
        [
            pltpu.VMEM((rows, width), bf16),
            pltpu.VMEM((width, DK), bf16),
            pltpu.VMEM((width, DV), bf16),
            sems((24,)),
        ],
        32,
        2 * rows * width * (DK + DV),
        normed,
        w_query,
        w_gate,
        key_rows,
        value_rows,
        col,
        line,
        row_table,
        column_table,
    )
    (entering,) = kernel_call(
        scan_kernel,
        [("v", shaped(count, DK // count, 2 * DV))],
        "vv",
        [],
        16,
        10 * parts.size,
        parts,
        decays,
    )
    states = lax.all_to_all(entering, YZ, 0, 0, tiled=True).reshape(DK, 2 * DV)
    partials = []
    for part in (1, 0):
        (partial,) = kernel_call(
            functools.partial(output_kernel, part),
            [("v", shaped(half, width))],
            "vvvvvvv",
            [],
            32,
            2 * half * DV * width,
            inside,
            gates,
            queries,
            states,
            col,
            group_gain.reshape(-1, 128),
            w_output,
        )
        partials.append(partial)
    crossed = lax.ppermute(partials[0], "c", swap)
    tiles = kernel_call(
        pair_kernel,
        [("v", shaped(lines, width))] * x_size,
        "vv",
        [],
        8,
        half * width,
        partials[1],
        crossed,
    )
    projected = tiles[0].astype(f32)
    for d in (2, 1, 3):
        arrived = lax.ppermute(tiles[d], "x", ring(x_size, -d))
        projected = projected + arrived.astype(f32)
    gate = modulation[:, 0].reshape(-1)[2 * width :]
    return (latent.astype(f32) + gate * projected).astype(bf16)


def solution(mesh):
    torus = Mesh(mesh.devices.reshape(8, 4, 4, 2), ALL)
    in_specs = (
        P(ALL, None),
        P(SP, TP),
        P(SP, None),
        P(),
        P(SP, TP),
        P(),
        P(None, TP),
        P(None, TP),
        P(None, TP),
        P(None, TP),
        P(TP),
        P(TP, None),
    )
    return jax.shard_map(
        per_device, mesh=torus, in_specs=in_specs, out_specs=P(ALL, None), check_vma=False
    )
```

```python
import functools

import jax
import jax.numpy as jnp
import numpy as np
from jax import lax
from jax.experimental import pallas as pl
from jax.experimental.pallas import tpu as pltpu
from jax.sharding import Mesh
from jax.sharding import PartitionSpec as P

DK = 256
DV = 512
GRID_W = 64
CTX_LIFT = 4
SP = ("z", "y")
YZ = ("y", "z")
TP = ("x", "c")
ALL = ("z", "y", "x", "c")
f32 = jnp.float32
bf16 = jnp.bfloat16

epsilon = 1e-06
rotary_base = 10000.0
MIB = 1024 * 1024


def kernel_call(body, outs, ins, scratch, vmem, flops, *args):
    spaces = {"h": pltpu.MemorySpace.HBM, "v": pltpu.MemorySpace.VMEM}
    moved = sum(a.size * a.dtype.itemsize for a in args)
    args = [
        pltpu.with_memory_space_constraint(a, pltpu.HBM) if k == "h" else a
        for k, a in zip(ins, args)
    ]
    return pl.pallas_call(
        body,
        out_shape=tuple(pltpu.HBM(a.shape, a.dtype) if k == "h" else a for k, a in outs),
        in_specs=[pl.BlockSpec(memory_space=spaces[k]) for k in ins],
        out_specs=tuple(pl.BlockSpec(memory_space=spaces[k]) for k, _ in outs),
        scratch_shapes=scratch,
        compiler_params=pltpu.CompilerParams(vmem_limit_bytes=vmem * MIB),
        cost_estimate=pl.CostEstimate(flops=flops, bytes_accessed=moved, transcendentals=0),
    )(*args)


def started(source, target, sems, slot):
    copy = pltpu.make_async_copy(source, target, sems.at[slot])
    copy.start()
    return copy


def flat_gain(gain_ref):
    wide = gain_ref[...].astype(f32)
    return jnp.concatenate([wide[i : i + 1, :] for i in range(wide.shape[0])], axis=1)


def dot(a, b):
    return jnp.dot(a, b, preferred_element_type=f32)


def dot_t(a, b):
    return lax.dot_general(a, b, (((1,), (1,)), ((), ())), preferred_element_type=f32)


def turn(u, row_ref, column_ref):
    lanes = lax.broadcasted_iota(jnp.int32, u.shape, 1)
    swapped = jnp.where(lanes % 2 == 0, pltpu.roll(u, DK - 1, 1), pltpu.roll(u, 1, 1))
    chips, lines, pair = row_ref.shape[0], column_ref.shape[0] // 2, DK // 2
    turned = []
    for i in range(2 * chips):
        own, half, d = slice(i * lines, (i + 1) * lines), i // chips, i % chips
        column = column_ref[half * lines : (half + 1) * lines, :]
        low = u[own, :pair] * row_ref[d, :, :pair] + swapped[own, :pair] * row_ref[d, :, pair:]
        high = u[own, pair:] * column[:, :pair] + swapped[own, pair:] * column[:, pair:]
        turned.append(jnp.concatenate([low, high], axis=1))
    return jnp.concatenate(turned, axis=0)


def prepare_kernel(
    lines, weights_hbm, condition_hbm, decay_hbm, row_hbm, column_hbm, gain_hbm,
    out_ref, decay_ref, row_ref, column_ref, gain_ref,
    weights_ref, condition_ref, sems,
):
    size, width = weights_hbm.shape[0], condition_hbm.shape[1]
    seq = lax.axis_index("z") * lax.axis_size("y") + lax.axis_index("y")
    chip, core = lax.axis_index("x"), lax.axis_index("c")
    chips = row_ref.shape[0]
    loads = [
        started(condition_hbm, condition_ref, sems, 0),
        started(decay_hbm, decay_ref, sems, 1),
        started(weights_hbm, weights_ref, sems, 2),
    ]
    for h in range(2):
        column = pl.multiple_of(((h + core) % 2) * lines, lines)
        target = column_ref.at[h * lines : (h + 1) * lines]
        loads.append(started(column_hbm.at[pl.ds(column, lines)], target, sems, 3 + h))
    for d in range(chips):
        row = seq * chips + (chip - d + chips) % chips
        loads.append(started(row_hbm.at[row], row_ref.at[d], sems, 5 + d))
    loads.append(started(gain_hbm, gain_ref, sems, 5 + chips))
    loads[0].wait()
    values = condition_ref[...].astype(f32)
    values = jnp.concatenate([values] * 4, axis=0)
    inputs = pltpu.roll(values, (width - seq * size) % width, 1)[0:2, 0:size]
    activated = (inputs / (1.0 + jnp.exp(-inputs))).astype(bf16)
    loads[1].wait()
    total = jnp.sum(decay_ref[...], axis=1, keepdims=True)
    loads[2].wait()
    part = dot(activated, weights_ref[...])
    cuts = part.shape[1] // 128
    packed = [part[i : i + 1, k * 128 : (k + 1) * 128] for i in range(2) for k in range(cuts)]
    rest = total
    while len(packed) < out_ref.shape[1]:
        term = rest.astype(bf16).astype(f32)
        packed.append(jnp.broadcast_to(term, (1, 128)))
        rest = rest - term
    packed = jnp.concatenate(packed, axis=0).astype(bf16)
    for r in range(out_ref.shape[0]):
        out_ref[r] = packed
    for copy in loads[3:]:
        copy.wait()


def rotary_tables(count):
    pairs = DK // 4
    exponents = -np.arange(pairs, dtype=np.float32) / np.float32(pairs)
    inverse = np.repeat(np.float32(rotary_base) ** exponents, 2).astype(np.float32)
    angles = np.arange(count, dtype=np.float32)[:, None] * inverse
    sign = np.where(np.arange(DK // 2) % 2 == 0, -1.0, 1.0).astype(np.float32)
    return np.concatenate([np.cos(angles), np.sin(angles) * sign], axis=1)


def tables_kernel(
    lines, chips, wk_hbm, wv_hbm, decay_ref, col_ref, line_ref, wk_ref, wv_ref, sems
):
    loads = [
        started(wk_hbm, wk_ref, sems, 0),
        started(wv_hbm.at[:, : wv_ref.shape[1]], wv_ref, sems, 1),
    ]
    rows = 2 * chips * lines
    chip, core = lax.axis_index("x"), lax.axis_index("c")

    def position(local):
        origin = (chip - (local // lines) % chips + chips) % chips
        return origin * GRID_W + ((local // (chips * lines) + core) % 2) * lines + local % lines

    down = lax.broadcasted_iota(jnp.int32, (rows, rows), 0)
    across = lax.broadcasted_iota(jnp.int32, (rows, rows), 1)
    place_col = position(lax.broadcasted_iota(jnp.int32, (rows, 1), 0))
    place_line = position(lax.broadcasted_iota(jnp.int32, (1, rows), 1))
    flat = decay_ref[...]
    total = jnp.sum(flat, axis=1, keepdims=True)
    flat_col = jnp.sum(jnp.where(down == across, flat, 0.0), axis=1, keepdims=True)
    upto = jnp.sum(jnp.where(across <= place_col, flat, 0.0), axis=1, keepdims=True)
    before = jnp.sum(jnp.where(across < place_col, flat, 0.0), axis=1, keepdims=True)
    col_ref[:, 0:1] = total - upto
    col_ref[:, 1:2] = before
    col_ref[:, 2:3] = upto
    col_ref[:, 3:4] = total - before
    col_ref[:, 4:5] = place_col.astype(f32)
    line_ref[0:1, :] = jnp.sum(jnp.where(down <= place_line, flat_col, 0.0), axis=0, keepdims=True)
    line_ref[1:2, :] = jnp.sum(jnp.where(down < place_line, flat_col, 0.0), axis=0, keepdims=True)
    line_ref[2:3, :] = place_line.astype(f32)
    odd = lax.axis_index("y") % 2
    line_ref[3:4, :] = jnp.full((1, rows), odd, jnp.int32).astype(f32)
    for copy in loads:
        copy.wait()


def gather_kernel(pieces_ref, out_ref, decay_ref):
    cuts = out_ref.shape[2] // 128
    pieces = [pieces_ref[r].astype(f32) for r in range(pieces_ref.shape[0])]
    summed = functools.reduce(jnp.add, pieces)
    rows = [
        jnp.concatenate([summed[i * cuts + k : i * cuts + k + 1, :] for k in range(cuts)], axis=1)
        for i in range(2)
    ]
    for t in range(out_ref.shape[0]):
        out_ref[t] = jnp.concatenate(rows, axis=0)
    for r, piece in enumerate(pieces):
        decay = jnp.exp(jnp.sum(piece[2 * cuts :, :], axis=0, keepdims=True))
        decay_ref[r : r + 1, :] = decay


def keys_kernel(*refs):
    pieces, refs = refs[:8], refs[8:]
    (
        near_hbm, wv_hbm, wk_ref, low_ref, gain_ref, far_ref, mod_ref, col_ref, line_ref, row_ref,
        column_ref,
        send_ref, normed_hbm, k_hbm, v_hbm,
        own_ref, near_ref, high_ref, normed_ref, k_ref, v_ref, sems,
    ) = refs
    lines, width = pieces[0].shape
    rows = 8 * lines
    near = near_ref.shape[0]
    own = [
        started(pieces[0], own_ref, sems, 3),
        started(near_hbm, near_ref, sems, 4),
    ]
    load = started(wv_hbm.at[:, low_ref.shape[1] :], high_ref, sems, 0)
    gain = flat_gain(gain_ref)
    tp = mod_ref.shape[0]

    def line_of(which):
        line = jnp.concatenate([mod_ref[t, which : which + 1, :] for t in range(tp)], axis=1)
        return line[:, :width], gain * (1.0 + line[:, width : 2 * width])

    lines_of = [line_of(which) for which in range(2)]

    def modulated(source, which):
        shift, scale = lines_of[which]
        wide = source.astype(f32)
        normal = wide * lax.rsqrt(jnp.mean(wide * wide, axis=-1, keepdims=True) + epsilon)
        return (normal * scale + shift).astype(bf16)

    for i, piece in enumerate(pieces[1:]):
        normed_ref[(i + 1) * lines : (i + 2) * lines, :] = modulated(piece[...], 0)
    normed_ref[rows + near :, :] = modulated(far_ref[...], 1)
    for copy in own:
        copy.wait()
    normed_ref[0:lines, :] = modulated(own_ref[...], 0)
    normed_ref[rows : rows + near, :] = modulated(near_ref[...], 1)
    stores = [started(normed_ref.at[0:rows], normed_hbm, sems, 2)]
    load.wait()
    keys = dot(normed_ref[...], wk_ref[...])
    low = dot(normed_ref[...], low_ref[...]).astype(bf16)
    high = dot(normed_ref[...], high_ref[...]).astype(bf16)
    values = jnp.concatenate([low, high], axis=1)
    key_rows = (turn(keys[:rows], row_ref, column_ref) * DK ** (-0.5)).astype(bf16)
    ctx_keys = (keys[rows:] * DK ** (-0.5)).astype(bf16)
    k_ref[...] = key_rows
    stores.append(started(k_ref, k_hbm, sems, 1))
    wide = key_rows.astype(f32)
    ahead = (wide * jnp.exp(col_ref[:, 0:1])).astype(bf16)
    behind = (wide * jnp.exp(col_ref[:, 1:2])).astype(bf16)
    turned = jnp.concatenate([ahead.T, behind.T], axis=0)
    v_ref[...] = values[:rows]
    stores.append(started(v_ref, v_hbm, sems, 5))
    parts = dot(turned, values[:rows]).astype(bf16)
    send_ref[:, 0:DV] = parts[:DK]
    send_ref[:, DV : 2 * DV] = parts[DK:]
    ctx_values = values[rows:]
    odd = line_ref[3:4, 0 : DV // 2] > 0.5
    own_values = jnp.where(
        odd, ctx_values[:, DV // 2 :].astype(f32), ctx_values[:, : DV // 2].astype(f32)
    ).astype(bf16)
    send_ref[:, 2 * DV :] = dot(ctx_keys.T, own_values).astype(bf16)
    for copy in stores:
        copy.wait()


def inside_kernel(
    normed_hbm, wq_hbm, wg_hbm, k_hbm, v_hbm, col_ref, line_ref, row_ref, column_ref,
    q_ref, g_ref, y_ref,
    normed_ref, wq_ref, wg_ref, k_ref, v_ref, sems,
):
    pairs = [
        (normed_hbm, normed_ref), (wq_hbm, wq_ref), (k_hbm, k_ref), (v_hbm, v_ref),
        (wg_hbm, wg_ref),
    ]
    loads = [started(a, b, sems, i) for i, (a, b) in enumerate(pairs)]
    for copy in loads[:4]:
        copy.wait()
    queries = turn(dot(normed_ref[...], wq_ref[...]), row_ref, column_ref).astype(bf16)
    q_ref[...] = queries
    scores = dot_t(queries, k_ref[...])
    here, there = col_ref[:, 4:5], line_ref[2:3, :]
    gaps = jnp.where(
        here >= there,
        col_ref[:, 2:3] - line_ref[0:1, :],
        line_ref[1:2, :] - col_ref[:, 1:2],
    )
    weights = jnp.exp(gaps) * jnp.where(here == there, 2.0, 1.0)
    y_ref[...] = dot((scores * weights).astype(bf16), v_ref[...]).astype(bf16)
    loads[4].wait()
    g_ref[...] = dot(normed_ref[...], wg_ref[...]).astype(bf16)


def scan_kernel(parts_ref, decay_ref, out_ref):
    count, z_size = parts_ref.shape[0], lax.axis_size("z")
    y_size = count // z_size
    spot = [(r % y_size) * z_size + r // y_size for r in range(count)]
    lifts = []
    for parity in range(2):
        lift = parts_ref[spot[parity], :, 2 * DV :].astype(f32)
        for r in range(parity + 2, count, 2):
            lift = lift + parts_ref[spot[r], :, 2 * DV :].astype(f32)
        lifts.append(lift)
    ahead = behind = jnp.concatenate(lifts, axis=1) * float(CTX_LIFT)
    decays = [jnp.concatenate([decay_ref[r : r + 1, :]] * (DV // 128), axis=1) for r in range(count)]
    for r in range(count):
        s = count - 1 - r
        out_ref[spot[r], :, 0:DV] = ahead.astype(bf16)
        out_ref[spot[s], :, DV:] = behind.astype(bf16)
        ahead = decays[r] * ahead + parts_ref[spot[r], :, 0:DV].astype(f32)
        behind = (
            decays[s] * behind + parts_ref[spot[s], :, DV : 2 * DV].astype(f32)
        )


def output_kernel(
    part, y_ref, g_ref, q_ref, states_ref, col_ref, gain_ref, wo_ref, out_ref
):
    half = out_ref.shape[0]
    own = slice(part * half, (part + 1) * half)
    queries = q_ref[own, :]
    mixed = (
        y_ref[own, :].astype(f32)
        + jnp.exp(col_ref[own, 2:3]) * dot(queries, states_ref[:, 0:DV])
        + jnp.exp(col_ref[own, 3:4]) * dot(queries, states_ref[:, DV:])
    )
    average = jnp.mean(mixed, axis=-1, keepdims=True)
    centred = mixed - average
    variance = jnp.mean(centred * centred, axis=-1, keepdims=True)
    gates = g_ref[own, :].astype(f32)
    attended = (
        gates * jax.nn.sigmoid(gates) * (centred * lax.rsqrt(variance + epsilon))
        * flat_gain(gain_ref)
    ).astype(bf16)
    out_ref[...] = dot(attended, wo_ref[...]).astype(bf16)


def pair_kernel(own_ref, crossed_ref, *out_refs):
    lines = out_refs[0].shape[0]
    for d, out_ref in enumerate(out_refs):
        own = slice(d * lines, (d + 1) * lines)
        out_ref[...] = (own_ref[own, :].astype(f32) + crossed_ref[own, :].astype(f32)).astype(bf16)


def ring(size, step):
    return [(i, (i + step) % size) for i in range(size)]


def shaped(*shape, dtype=bf16):
    return jax.ShapeDtypeStruct(shape, dtype)


def per_device(
    latent,
    log_decay,
    context,
    condition,
    w_modulate,
    norm_gain,
    w_query,
    w_key,
    w_value,
    w_gate,
    group_gain,
    w_output,
):
    lines, width = latent.shape
    x_size = lax.axis_size("x")
    half = lines * x_size
    rows = 2 * half
    swap = [(0, 1), (1, 0)]

    columns = w_modulate.shape[1]
    sems = pltpu.SemaphoreType.DMA
    count, tp = lax.axis_size(SP), lax.axis_size(TP)
    packed, decay_row, row_table, column_table, gain = kernel_call(
        functools.partial(prepare_kernel, lines),
        [
            ("v", shaped(count, 16, 128)),
            ("v", shaped(1, rows, dtype=f32)),
            ("v", shaped(x_size, 1, DK, dtype=f32)),
            ("v", shaped(2 * lines, DK, dtype=f32)),
            ("v", shaped(width // 128, 128)),
        ],
        "hhhhhh",
        [
            pltpu.VMEM(w_modulate.shape, bf16),
            pltpu.VMEM(condition.shape, bf16),
            sems((6 + x_size,)),
        ],
        8,
        1000000,
        w_modulate,
        condition,
        log_decay.T,
        jnp.asarray(rotary_tables(count * rows // GRID_W))[:, None],
        jnp.asarray(rotary_tables(GRID_W)),
        norm_gain.reshape(-1, 128),
    )
    pieces = lax.all_to_all(packed, SP, 0, 0, tiled=True)
    spread, decays = kernel_call(
        gather_kernel,
        [("v", shaped(tp, 2, columns, dtype=f32)), ("v", shaped(count, 128, dtype=f32))],
        "v",
        [],
        4,
        1000000,
        pieces,
    )
    modulation = lax.all_to_all(spread, TP, 0, 0, tiled=True)

    later, near, _ = lax.optimization_barrier((latent, context, packed))
    own_rows = [later] + [lax.ppermute(later, "x", ring(x_size, d)) for d in range(1, x_size)]
    other_rows = [lax.ppermute(piece, "c", swap) for piece in own_rows]
    far = lax.ppermute(near, "y", [(0, 1), (1, 0), (2, 3), (3, 2)])
    col, line, early_key, early_value = kernel_call(
        functools.partial(tables_kernel, lines, x_size),
        [
            ("v", shaped(rows, 8, dtype=f32)),
            ("v", shaped(4, rows, dtype=f32)),
            ("v", shaped(width, DK)),
            ("v", shaped(width, DV // 2)),
        ],
        "hhv",
        [sems((2,))],
        8,
        1000000,
        w_key,
        w_value,
        decay_row,
    )

    ctx = 2 * context.shape[0]
    lanes = 2 * DV + DV // 2
    send, normed, key_rows, value_rows = kernel_call(
        keys_kernel,
        [
            ("v", shaped(DK, lanes)),
            ("h", shaped(rows, width)),
            ("h", shaped(rows, DK)),
            ("h", shaped(rows, DV)),
        ],
        "hvvvvvvv" + "hhvvvvvvvvv",
        [
            pltpu.VMEM((lines, width), bf16),
            pltpu.VMEM(context.shape, bf16),
            pltpu.VMEM((width, DV // 2), bf16),
            pltpu.VMEM((rows + ctx, width), bf16),
            pltpu.VMEM((rows, DK), bf16),
            pltpu.VMEM((rows, DV), bf16),
            sems((6,)),
        ],
        32,
        2 * (rows + ctx) * width * (DK + DV),
        *own_rows,
        *other_rows,
        near,
        w_value,
        early_key,
        early_value,
        gain,
        far,
        modulation,
        col,
        line,
        row_table,
        column_table,
    )
    parts = lax.all_to_all(send.reshape(count, DK // count, lanes), YZ, 0, 0, tiled=True)
    queries, gates, inside = kernel_call(
        inside_kernel,
        [
            ("v", shaped(rows, DK)),
            ("v", shaped(rows, DV)),
            ("v", shaped(rows, DV)),
        ],
        "hhhhhvvvv",
        [
            pltpu.VMEM((rows, width), bf16),
            pltpu.VMEM((width, DK), bf16),
            pltpu.VMEM((width, DV), bf16),
            pltpu.VMEM((rows, DK), bf16),
            pltpu.VMEM((rows, DV), bf16),
            sems((5,)),
        ],
        32,
        2 * rows * width * (DK + DV),
        normed,
        w_query,
        w_gate,
        key_rows,
        value_rows,
        col,
        line,
        row_table,
        column_table,
    )
    (entering,) = kernel_call(
        scan_kernel,
        [("v", shaped(count, DK // count, 2 * DV))],
        "vv",
        [],
        16,
        10 * parts.size,
        parts,
        decays,
    )
    states = lax.all_to_all(entering, YZ, 0, 0, tiled=True).reshape(DK, 2 * DV)
    partials = []
    for part in (1, 0):
        (partial,) = kernel_call(
            functools.partial(output_kernel, part),
            [("v", shaped(half, width))],
            "vvvvvvv",
            [],
            32,
            2 * half * DV * width,
            inside,
            gates,
            queries,
            states,
            col,
            group_gain.reshape(-1, 128),
            w_output,
        )
        partials.append(partial)
    crossed = lax.ppermute(partials[0], "c", swap)
    tiles = kernel_call(
        pair_kernel,
        [("v", shaped(lines, width))] * x_size,
        "vv",
        [],
        8,
        half * width,
        partials[1],
        crossed,
    )
    projected = tiles[0].astype(f32)
    for d in (2, 1, 3):
        arrived = lax.ppermute(tiles[d], "x", ring(x_size, -d))
        projected = projected + arrived.astype(f32)
    gate = modulation[:, 0].reshape(-1)[2 * width :]
    return (latent.astype(f32) + gate * projected).astype(bf16)


def solution(mesh):
    torus = Mesh(mesh.devices.reshape(8, 4, 4, 2), ALL)
    in_specs = (
        P(ALL, None),
        P(SP, TP),
        P(SP, None),
        P(),
        P(SP, TP),
        P(),
        P(None, TP),
        P(None, TP),
        P(None, TP),
        P(None, TP),
        P(TP),
        P(TP, None),
    )
    return jax.shard_map(
        per_device, mesh=torus, in_specs=in_specs, out_specs=P(ALL, None), check_vma=False
    )
```

```python
import functools

import jax
import jax.numpy as jnp
import numpy as np
from jax import lax
from jax.experimental import pallas as pl
from jax.experimental.pallas import tpu as pltpu
from jax.sharding import Mesh
from jax.sharding import PartitionSpec as P

DK = 256
DV = 512
GRID_W = 64
CTX_LIFT = 4
SP = ("z", "y")
YZ = ("y", "z")
TP = ("x", "c")
ALL = ("z", "y", "x", "c")
f32 = jnp.float32
bf16 = jnp.bfloat16

epsilon = 1e-06
rotary_base = 10000.0
MIB = 1024 * 1024


def kernel_call(body, outs, ins, scratch, vmem, flops, *args):
    spaces = {"h": pltpu.MemorySpace.HBM, "v": pltpu.MemorySpace.VMEM}
    moved = sum(a.size * a.dtype.itemsize for a in args)
    args = [
        pltpu.with_memory_space_constraint(a, pltpu.HBM) if k == "h" else a
        for k, a in zip(ins, args)
    ]
    return pl.pallas_call(
        body,
        out_shape=tuple(pltpu.HBM(a.shape, a.dtype) if k == "h" else a for k, a in outs),
        in_specs=[pl.BlockSpec(memory_space=spaces[k]) for k in ins],
        out_specs=tuple(pl.BlockSpec(memory_space=spaces[k]) for k, _ in outs),
        scratch_shapes=scratch,
        compiler_params=pltpu.CompilerParams(vmem_limit_bytes=vmem * MIB),
        cost_estimate=pl.CostEstimate(flops=flops, bytes_accessed=moved, transcendentals=0),
    )(*args)


def started(source, target, sems, slot):
    copy = pltpu.make_async_copy(source, target, sems.at[slot])
    copy.start()
    return copy


def flat_gain(gain_ref):
    wide = gain_ref[...].astype(f32)
    return jnp.concatenate([wide[i : i + 1, :] for i in range(wide.shape[0])], axis=1)


def dot(a, b):
    return jnp.dot(a, b, preferred_element_type=f32)


def dot_t(a, b):
    return lax.dot_general(a, b, (((1,), (1,)), ((), ())), preferred_element_type=f32)


def turn(u, row_ref, column_ref):
    lanes = lax.broadcasted_iota(jnp.int32, u.shape, 1)
    swapped = jnp.where(lanes % 2 == 0, pltpu.roll(u, DK - 1, 1), pltpu.roll(u, 1, 1))
    chips, lines, pair = row_ref.shape[0], column_ref.shape[0] // 2, DK // 2
    turned = []
    for i in range(2 * chips):
        own, half, d = slice(i * lines, (i + 1) * lines), i // chips, i % chips
        column = column_ref[half * lines : (half + 1) * lines, :]
        low = u[own, :pair] * row_ref[d, :, :pair] + swapped[own, :pair] * row_ref[d, :, pair:]
        high = u[own, pair:] * column[:, :pair] + swapped[own, pair:] * column[:, pair:]
        turned.append(jnp.concatenate([low, high], axis=1))
    return jnp.concatenate(turned, axis=0)


def prepare_kernel(
    lines, weights_hbm, condition_hbm, decay_hbm, row_hbm, column_hbm, gain_hbm,
    out_ref, decay_ref, row_ref, column_ref, gain_ref,
    weights_ref, condition_ref, sems,
):
    size, width = weights_hbm.shape[0], condition_hbm.shape[1]
    seq = lax.axis_index("z") * lax.axis_size("y") + lax.axis_index("y")
    chip, core = lax.axis_index("x"), lax.axis_index("c")
    chips = row_ref.shape[0]
    loads = [
        started(condition_hbm, condition_ref, sems, 0),
        started(decay_hbm, decay_ref, sems, 1),
        started(weights_hbm, weights_ref, sems, 2),
    ]
    for h in range(2):
        column = pl.multiple_of(((h + core) % 2) * lines, lines)
        target = column_ref.at[h * lines : (h + 1) * lines]
        loads.append(started(column_hbm.at[pl.ds(column, lines)], target, sems, 3 + h))
    for d in range(chips):
        row = seq * chips + (chip - d + chips) % chips
        loads.append(started(row_hbm.at[row], row_ref.at[d], sems, 5 + d))
    loads.append(started(gain_hbm, gain_ref, sems, 5 + chips))
    loads[0].wait()
    values = condition_ref[...].astype(f32)
    values = jnp.concatenate([values] * 4, axis=0)
    inputs = pltpu.roll(values, (width - seq * size) % width, 1)[0:2, 0:size]
    activated = (inputs / (1.0 + jnp.exp(-inputs))).astype(bf16)
    loads[1].wait()
    total = jnp.sum(decay_ref[...], axis=1, keepdims=True)
    loads[2].wait()
    part = dot(activated, weights_ref[...])
    cuts = part.shape[1] // 128
    packed = [part[i : i + 1, k * 128 : (k + 1) * 128] for i in range(2) for k in range(cuts)]
    rest = total
    while len(packed) < out_ref.shape[1]:
        term = rest.astype(bf16).astype(f32)
        packed.append(jnp.broadcast_to(term, (1, 128)))
        rest = rest - term
    packed = jnp.concatenate(packed, axis=0).astype(bf16)
    for r in range(out_ref.shape[0]):
        out_ref[r] = packed
    for copy in loads[3:]:
        copy.wait()


def rotary_tables(count):
    pairs = DK // 4
    exponents = -np.arange(pairs, dtype=np.float32) / np.float32(pairs)
    inverse = np.repeat(np.float32(rotary_base) ** exponents, 2).astype(np.float32)
    angles = np.arange(count, dtype=np.float32)[:, None] * inverse
    sign = np.where(np.arange(DK // 2) % 2 == 0, -1.0, 1.0).astype(np.float32)
    return np.concatenate([np.cos(angles), np.sin(angles) * sign], axis=1)


def tables_kernel(lines, chips, wk_hbm, decay_ref, col_ref, line_ref, wk_ref, sems):
    loads = [started(wk_hbm, wk_ref, sems, 0)]
    rows = 2 * chips * lines
    chip, core = lax.axis_index("x"), lax.axis_index("c")

    def position(local):
        origin = (chip - (local // lines) % chips + chips) % chips
        return origin * GRID_W + ((local // (chips * lines) + core) % 2) * lines + local % lines

    down = lax.broadcasted_iota(jnp.int32, (rows, rows), 0)
    across = lax.broadcasted_iota(jnp.int32, (rows, rows), 1)
    place_col = position(lax.broadcasted_iota(jnp.int32, (rows, 1), 0))
    place_line = position(lax.broadcasted_iota(jnp.int32, (1, rows), 1))
    flat = decay_ref[...]
    total = jnp.sum(flat, axis=1, keepdims=True)
    flat_col = jnp.sum(jnp.where(down == across, flat, 0.0), axis=1, keepdims=True)
    upto = jnp.sum(jnp.where(across <= place_col, flat, 0.0), axis=1, keepdims=True)
    before = jnp.sum(jnp.where(across < place_col, flat, 0.0), axis=1, keepdims=True)
    col_ref[:, 0:1] = total - upto
    col_ref[:, 1:2] = before
    col_ref[:, 2:3] = upto
    col_ref[:, 3:4] = total - before
    col_ref[:, 4:5] = place_col.astype(f32)
    line_ref[0:1, :] = jnp.sum(jnp.where(down <= place_line, flat_col, 0.0), axis=0, keepdims=True)
    line_ref[1:2, :] = jnp.sum(jnp.where(down < place_line, flat_col, 0.0), axis=0, keepdims=True)
    line_ref[2:3, :] = place_line.astype(f32)
    odd = lax.axis_index("y") % 2
    line_ref[3:4, :] = jnp.full((1, rows), odd, jnp.int32).astype(f32)
    for copy in loads:
        copy.wait()


def gather_kernel(pieces_ref, out_ref, decay_ref):
    cuts = out_ref.shape[2] // 128
    pieces = [pieces_ref[r].astype(f32) for r in range(pieces_ref.shape[0])]
    summed = functools.reduce(jnp.add, pieces)
    rows = [
        jnp.concatenate([summed[i * cuts + k : i * cuts + k + 1, :] for k in range(cuts)], axis=1)
        for i in range(2)
    ]
    for t in range(out_ref.shape[0]):
        out_ref[t] = jnp.concatenate(rows, axis=0)
    for r, piece in enumerate(pieces):
        decay = jnp.exp(jnp.sum(piece[2 * cuts :, :], axis=0, keepdims=True))
        decay_ref[r : r + 1, :] = decay


def keys_kernel(*refs):
    pieces, refs = refs[:8], refs[8:]
    (
        near_hbm, wv_hbm, wk_ref, gain_ref, far_ref, mod_ref, col_ref, line_ref, row_ref,
        column_ref,
        send_ref, normed_hbm, k_ref, v_ref,
        own_ref, near_ref, wv_ref, normed_ref, sems,
    ) = refs
    lines, width = pieces[0].shape
    rows = 8 * lines
    near = near_ref.shape[0]
    own = [
        started(pieces[0], own_ref, sems, 3),
        started(near_hbm, near_ref, sems, 4),
    ]
    load = started(wv_hbm, wv_ref, sems, 0)
    gain = flat_gain(gain_ref)
    tp = mod_ref.shape[0]

    def line_of(which):
        line = jnp.concatenate([mod_ref[t, which : which + 1, :] for t in range(tp)], axis=1)
        return line[:, :width], gain * (1.0 + line[:, width : 2 * width])

    lines_of = [line_of(which) for which in range(2)]

    def modulated(source, which):
        shift, scale = lines_of[which]
        wide = source.astype(f32)
        normal = wide * lax.rsqrt(jnp.mean(wide * wide, axis=-1, keepdims=True) + epsilon)
        return (normal * scale + shift).astype(bf16)

    for i, piece in enumerate(pieces[1:]):
        normed_ref[(i + 1) * lines : (i + 2) * lines, :] = modulated(piece[...], 0)
    normed_ref[rows + near :, :] = modulated(far_ref[...], 1)
    for copy in own:
        copy.wait()
    normed_ref[0:lines, :] = modulated(own_ref[...], 0)
    normed_ref[rows : rows + near, :] = modulated(near_ref[...], 1)
    stores = [started(normed_ref.at[0:rows], normed_hbm, sems, 2)]
    keys = dot(normed_ref[...], wk_ref[...])
    key_rows = (turn(keys[:rows], row_ref, column_ref) * DK ** (-0.5)).astype(bf16)
    ctx_keys = (keys[rows:] * DK ** (-0.5)).astype(bf16)
    k_ref[...] = key_rows
    wide = key_rows.astype(f32)
    ahead = (wide * jnp.exp(col_ref[:, 0:1])).astype(bf16)
    behind = (wide * jnp.exp(col_ref[:, 1:2])).astype(bf16)
    turned = jnp.concatenate([ahead.T, behind.T], axis=0)
    load.wait()
    values = dot(normed_ref[...], wv_ref[...]).astype(bf16)
    v_ref[...] = values[:rows]
    parts = dot(turned, values[:rows]).astype(bf16)
    send_ref[:, 0:DV] = parts[:DK]
    send_ref[:, DV : 2 * DV] = parts[DK:]
    ctx_values = values[rows:]
    odd = line_ref[3:4, 0 : DV // 2] > 0.5
    own_values = jnp.where(
        odd, ctx_values[:, DV // 2 :].astype(f32), ctx_values[:, : DV // 2].astype(f32)
    ).astype(bf16)
    send_ref[:, 2 * DV :] = dot(ctx_keys.T, own_values).astype(bf16)
    for copy in stores:
        copy.wait()


def inside_kernel(
    normed_hbm, wq_hbm, wg_hbm, k_hbm, v_hbm, col_ref, line_ref, row_ref, column_ref,
    q_ref, g_ref, y_ref,
    normed_ref, wq_ref, wg_ref, k_ref, v_ref, sems,
):
    pairs = [
        (normed_hbm, normed_ref), (wq_hbm, wq_ref), (k_hbm, k_ref), (v_hbm, v_ref),
        (wg_hbm, wg_ref),
    ]
    loads = [started(a, b, sems, i) for i, (a, b) in enumerate(pairs)]
    for copy in loads[:4]:
        copy.wait()
    queries = turn(dot(normed_ref[...], wq_ref[...]), row_ref, column_ref).astype(bf16)
    q_ref[...] = queries
    scores = dot_t(queries, k_ref[...])
    here, there = col_ref[:, 4:5], line_ref[2:3, :]
    gaps = jnp.where(
        here >= there,
        col_ref[:, 2:3] - line_ref[0:1, :],
        line_ref[1:2, :] - col_ref[:, 1:2],
    )
    weights = jnp.exp(gaps) * jnp.where(here == there, 2.0, 1.0)
    y_ref[...] = dot((scores * weights).astype(bf16), v_ref[...]).astype(bf16)
    loads[4].wait()
    g_ref[...] = dot(normed_ref[...], wg_ref[...]).astype(bf16)


def scan_kernel(parts_ref, decay_ref, out_ref):
    count, z_size = parts_ref.shape[0], lax.axis_size("z")
    y_size = count // z_size
    spot = [(r % y_size) * z_size + r // y_size for r in range(count)]
    lifts = []
    for parity in range(2):
        lift = parts_ref[spot[parity], :, 2 * DV :].astype(f32)
        for r in range(parity + 2, count, 2):
            lift = lift + parts_ref[spot[r], :, 2 * DV :].astype(f32)
        lifts.append(lift)
    ahead = behind = jnp.concatenate(lifts, axis=1) * float(CTX_LIFT)
    decays = [jnp.concatenate([decay_ref[r : r + 1, :]] * (DV // 128), axis=1) for r in range(count)]
    for r in range(count):
        s = count - 1 - r
        out_ref[spot[r], :, 0:DV] = ahead.astype(bf16)
        out_ref[spot[s], :, DV:] = behind.astype(bf16)
        ahead = decays[r] * ahead + parts_ref[spot[r], :, 0:DV].astype(f32)
        behind = (
            decays[s] * behind + parts_ref[spot[s], :, DV : 2 * DV].astype(f32)
        )


def output_kernel(
    part, y_ref, g_ref, q_ref, states_ref, col_ref, gain_ref, wo_ref, out_ref
):
    half = out_ref.shape[0]
    own = slice(part * half, (part + 1) * half)
    queries = q_ref[own, :]
    mixed = (
        y_ref[own, :].astype(f32)
        + jnp.exp(col_ref[own, 2:3]) * dot(queries, states_ref[:, 0:DV])
        + jnp.exp(col_ref[own, 3:4]) * dot(queries, states_ref[:, DV:])
    )
    average = jnp.mean(mixed, axis=-1, keepdims=True)
    centred = mixed - average
    variance = jnp.mean(centred * centred, axis=-1, keepdims=True)
    gates = g_ref[own, :].astype(f32)
    attended = (
        gates * jax.nn.sigmoid(gates) * (centred * lax.rsqrt(variance + epsilon))
        * flat_gain(gain_ref)
    ).astype(bf16)
    out_ref[...] = dot(attended, wo_ref[...]).astype(bf16)


def pair_kernel(own_ref, crossed_ref, *out_refs):
    lines = out_refs[0].shape[0]
    for d, out_ref in enumerate(out_refs):
        own = slice(d * lines, (d + 1) * lines)
        out_ref[...] = (own_ref[own, :].astype(f32) + crossed_ref[own, :].astype(f32)).astype(bf16)


def ring(size, step):
    return [(i, (i + step) % size) for i in range(size)]


def shaped(*shape, dtype=bf16):
    return jax.ShapeDtypeStruct(shape, dtype)


def per_device(
    latent,
    log_decay,
    context,
    condition,
    w_modulate,
    norm_gain,
    w_query,
    w_key,
    w_value,
    w_gate,
    group_gain,
    w_output,
):
    lines, width = latent.shape
    x_size = lax.axis_size("x")
    half = lines * x_size
    rows = 2 * half
    swap = [(0, 1), (1, 0)]

    columns = w_modulate.shape[1]
    sems = pltpu.SemaphoreType.DMA
    count, tp = lax.axis_size(SP), lax.axis_size(TP)
    packed, decay_row, row_table, column_table, gain = kernel_call(
        functools.partial(prepare_kernel, lines),
        [
            ("v", shaped(count, 16, 128)),
            ("v", shaped(1, rows, dtype=f32)),
            ("v", shaped(x_size, 1, DK, dtype=f32)),
            ("v", shaped(2 * lines, DK, dtype=f32)),
            ("v", shaped(width // 128, 128)),
        ],
        "hhhhhh",
        [
            pltpu.VMEM(w_modulate.shape, bf16),
            pltpu.VMEM(condition.shape, bf16),
            sems((6 + x_size,)),
        ],
        8,
        1000000,
        w_modulate,
        condition,
        log_decay.T,
        jnp.asarray(rotary_tables(count * rows // GRID_W))[:, None],
        jnp.asarray(rotary_tables(GRID_W)),
        norm_gain.reshape(-1, 128),
    )
    pieces = lax.all_to_all(packed, SP, 0, 0, tiled=True)
    spread, decays = kernel_call(
        gather_kernel,
        [("v", shaped(tp, 2, columns, dtype=f32)), ("v", shaped(count, 128, dtype=f32))],
        "v",
        [],
        4,
        1000000,
        pieces,
    )
    modulation = lax.all_to_all(spread, TP, 0, 0, tiled=True)

    later, near, _ = lax.optimization_barrier((latent, context, packed))
    own_rows = [later] + [lax.ppermute(later, "x", ring(x_size, d)) for d in range(1, x_size)]
    other_rows = [lax.ppermute(piece, "c", swap) for piece in own_rows]
    far = lax.ppermute(near, "y", [(0, 1), (1, 0), (2, 3), (3, 2)])
    col, line, early_key = kernel_call(
        functools.partial(tables_kernel, lines, x_size),
        [
            ("v", shaped(rows, 8, dtype=f32)),
            ("v", shaped(4, rows, dtype=f32)),
            ("v", shaped(width, DK)),
        ],
        "hv",
        [sems((1,))],
        8,
        1000000,
        w_key,
        decay_row,
    )

    ctx = 2 * context.shape[0]
    lanes = 2 * DV + DV // 2
    send, normed, key_rows, value_rows = kernel_call(
        keys_kernel,
        [
            ("v", shaped(DK, lanes)),
            ("h", shaped(rows, width)),
            ("v", shaped(rows, DK)),
            ("v", shaped(rows, DV)),
        ],
        "hvvvvvvv" + "hhvvvvvvvv",
        [
            pltpu.VMEM((lines, width), bf16),
            pltpu.VMEM(context.shape, bf16),
            pltpu.VMEM((width, DV), bf16),
            pltpu.VMEM((rows + ctx, width), bf16),
            sems((5,)),
        ],
        32,
        2 * (rows + ctx) * width * (DK + DV),
        *own_rows,
        *other_rows,
        near,
        w_value,
        early_key,
        gain,
        far,
        modulation,
        col,
        line,
        row_table,
        column_table,
    )
    parts = lax.all_to_all(send.reshape(count, DK // count, lanes), YZ, 0, 0, tiled=True)
    queries, gates, inside = kernel_call(
        inside_kernel,
        [
            ("v", shaped(rows, DK)),
            ("v", shaped(rows, DV)),
            ("v", shaped(rows, DV)),
        ],
        "hhhhhvvvv",
        [
            pltpu.VMEM((rows, width), bf16),
            pltpu.VMEM((width, DK), bf16),
            pltpu.VMEM((width, DV), bf16),
            pltpu.VMEM((rows, DK), bf16),
            pltpu.VMEM((rows, DV), bf16),
            sems((5,)),
        ],
        32,
        2 * rows * width * (DK + DV),
        normed,
        w_query,
        w_gate,
        key_rows,
        value_rows,
        col,
        line,
        row_table,
        column_table,
    )
    (entering,) = kernel_call(
        scan_kernel,
        [("v", shaped(count, DK // count, 2 * DV))],
        "vv",
        [],
        16,
        10 * parts.size,
        parts,
        decays,
    )
    states = lax.all_to_all(entering, YZ, 0, 0, tiled=True).reshape(DK, 2 * DV)
    partials = []
    for part in (1, 0):
        (partial,) = kernel_call(
            functools.partial(output_kernel, part),
            [("v", shaped(half, width))],
            "vvvvvvv",
            [],
            32,
            2 * half * DV * width,
            inside,
            gates,
            queries,
            states,
            col,
            group_gain.reshape(-1, 128),
            w_output,
        )
        partials.append(partial)
    crossed = lax.ppermute(partials[0], "c", swap)
    tiles = kernel_call(
        pair_kernel,
        [("v", shaped(lines, width))] * x_size,
        "vv",
        [],
        8,
        half * width,
        partials[1],
        crossed,
    )
    projected = tiles[0].astype(f32)
    for d in (1, 3, 2):
        arrived = lax.ppermute(tiles[d], "x", ring(x_size, -d))
        projected = projected + arrived.astype(f32)
    gate = modulation[:, 0].reshape(-1)[2 * width :]
    return (latent.astype(f32) + gate * projected).astype(bf16)


def solution(mesh):
    torus = Mesh(mesh.devices.reshape(8, 4, 4, 2), ALL)
    in_specs = (
        P(ALL, None),
        P(SP, TP),
        P(SP, None),
        P(),
        P(SP, TP),
        P(),
        P(None, TP),
        P(None, TP),
        P(None, TP),
        P(None, TP),
        P(TP),
        P(TP, None),
    )
    return jax.shard_map(
        per_device, mesh=torus, in_specs=in_specs, out_specs=P(ALL, None), check_vma=False
    )
```
